512 devices in a mesh: dp: 4 (over x), kv: 64 (over z, y), tp: 2 (over core).
Axes of the slice: x: 4, y: 4, z: 16, core: 2. Of those that a mesh axis runs over, the one named last changes fastest.
Arguments:
- tokens: bfloat16 [512, 4, 2048], P('dp', None, 'kv'), may hold values from -600 to 600
- input_norm_gain: float32 [2048], P('kv'), may hold values from 0.1 to 1.9
- query_projection: bfloat16 [2048, 1024], P('kv', 'tp'), may hold values from -0.125 to 0.125
- key_projection: bfloat16 [2048, 1024], P('kv', 'tp'), may hold values from -0.125 to 0.125
- value_projection: bfloat16 [2048, 1024], P('kv', 'tp'), may hold values from -0.125 to 0.125
- write_strength_weight: bfloat16 [2048, 16], P('kv', 'tp'), may hold values from -0.125 to 0.125
- decay_projection: bfloat16 [2048, 16], P('kv', 'tp'), may hold values from -0.125 to 0.125
- head_decay_rate: float32 [16], P('tp'), may hold values from 0.02 to 0.6
- token_extra_decay: float32 [512, 4, 16], P(('dp', 'kv'), None, 'tp'), may hold values from -0.7 to 0
- accepted: int32 [512], P(('dp', 'kv')), may hold values from 1 to 4
- prior_step_states: float32 [512, 4, 16, 4096], P(('dp', 'kv'), None, 'tp'), may hold values from -4 to 4
- output_norm_gain: float32 [64], replicated, may hold values from 0.1 to 1.9
- output_projection: bfloat16 [1024, 2048], P('tp', 'kv'), may hold values from -0.1875 to 0.1875
Outputs:
- mixed: bfloat16 [512, 4, 2048], P('dp', None, 'kv')
- updated_states: float32 [512, 4, 16, 4096], P(('dp', 'kv'), None, 'tp')
The draws below stay inside these ranges and needn't reach their ends.
Inputs may be any that keep to these rules, and one draw needn't show every extreme that they name: `accepted`: how many proposals of the previous step each sequence kept; its state after that many is taken up.
All inputs are finite; a program needn't handle non-finite values.
Results may differ from the reference program's by a relative error of at most 0.029.
Values may be sent and summed in bfloat16 or wider, within the bound.
No kernel may reach another device: no remote copies, remote signals or barrier semaphores. Data moves between devices by JAX's collectives and lax.ppermute only.
A program may use at most 64 MiB of HBM per device.

```python
import math
import jax
import jax.numpy as jnp
from jax import lax

D = 2048
HEAD_TOTAL = 16
HEAD = 64
DRAFT_TOKENS = 4
SEQ_DEV = 2
SEQUENCE_TOTAL = 512


def draw_tokens(key, part):
    base_key = jax.random.fold_in(key, 11)
    key_one = jax.random.fold_in(base_key, 0)
    column = jnp.arange(D, dtype=jnp.float32) / D
    sample_noise = jax.random.normal(key_one, (SEQUENCE_TOTAL, DRAFT_TOKENS, D), jnp.float32)
    values = sample_noise * 10.0 ** column
    return values.astype(jnp.bfloat16)


def place_ends(array, own_key, least, largest):
    place = [jax.random.randint(jax.random.fold_in(own_key, axis), (), 0, length) for axis, length in enumerate(array.shape)]
    longest = array.shape.index(max(array.shape))
    next_to = place[:longest] + [(place[longest] + 1) % array.shape[longest]] + place[longest + 1:]
    return array.at[tuple(place)].set(least).at[tuple(next_to)].set(largest)


def shard_levels(key, extent, pieces, smallest, largest):
    factor_of, own = 1.0, jax.random.fold_in(key, 6)
    for dim, parts in pieces:
        heights = jnp.exp(jax.random.uniform(jax.random.fold_in(own, dim), (parts,), jnp.float32, smallest / len(pieces), largest / len(pieces)))
        factor_of = factor_of * jnp.repeat(heights, extent[dim] // parts).reshape([-1 if axis == dim else 1 for axis in range(len(extent))])
    return factor_of


def scatter_about(own_key, extent, scale, bound, cuts=(), held_as=jnp.bfloat16):
    array = jax.random.normal(own_key, extent, jnp.float32) * scale
    if len(cuts) > 0:
        array = shard_levels(own_key, extent, cuts, -0.22, 0.18) * array
    return jnp.clip(array, min=-bound, max=bound).astype(held_as)


def setup_inputs(seed: int = 0) -> dict:
    key_list = jax.random.split(jax.random.key(seed), 14)
    tokens = draw_tokens(jax.random.fold_in(key_list[13], 71), 0)
    input_norm_gain = jnp.clip(1.0 + 0.18 * jax.random.normal(key_list[1], (D,), jnp.float32), 0.1, 1.9)
    query_projection = scatter_about(key_list[2], (D, HEAD_TOTAL * HEAD), D ** -0.5, 0.125, ((0, 64), (1, 2)))
    key_projection = scatter_about(key_list[3], (D, HEAD_TOTAL * HEAD), D ** -0.5, 0.125, ((0, 64), (1, 2)))
    value_projection = scatter_about(key_list[4], (D, HEAD_TOTAL * HEAD), D ** -0.5, 0.125, ((0, 64), (1, 2)))
    write_strength_weight = scatter_about(key_list[5], (D, HEAD_TOTAL), D ** -0.5, 0.125, ((0, 64), (1, 2)))
    decay_projection = scatter_about(key_list[6], (D, HEAD_TOTAL), D ** -0.5, 0.125, ((0, 64), (1, 2)))
    head_decay_rate = jnp.clip(jnp.exp(math.log(0.6) - 3.4011974 * jax.random.uniform(key_list[7], (HEAD_TOTAL,), jnp.float32) ** shard_levels(key_list[7], (HEAD_TOTAL,), ((0, 2),), -0.2, 0.2)), 0.02, 0.6)
    token_extra_decay = jnp.clip(-0.7 + 0.7 * jax.random.uniform(key_list[8], (SEQUENCE_TOTAL, DRAFT_TOKENS, HEAD_TOTAL), jnp.float32) ** shard_levels(key_list[8], (SEQUENCE_TOTAL, DRAFT_TOKENS, HEAD_TOTAL), ((0, 256), (2, 2)), -0.2, 0.2), -0.7, 0.0)
    accepted = place_ends(jax.random.randint(key_list[9], (SEQUENCE_TOTAL,), 1, DRAFT_TOKENS + 1), jax.random.fold_in(key_list[9], 1), 1, DRAFT_TOKENS).astype(jnp.int32)
    prior_step_states = scatter_about(key_list[10], (SEQUENCE_TOTAL, DRAFT_TOKENS, HEAD_TOTAL, HEAD * HEAD), 0.3, 4.0, ((0, 256), (2, 2)), jnp.float32)
    output_norm_gain = jnp.clip(1.0 + 0.18 * jax.random.normal(key_list[11], (HEAD,), jnp.float32), 0.1, 1.9)
    output_projection = scatter_about(key_list[12], (HEAD_TOTAL * HEAD, D), (HEAD_TOTAL * HEAD) ** -0.5, 0.1875, ((0, 2), (1, 64)))
    return {"tokens": tokens, "input_norm_gain": input_norm_gain, "query_projection": query_projection, "key_projection": key_projection, "value_projection": value_projection, "write_strength_weight": write_strength_weight, "decay_projection": decay_projection, "head_decay_rate": head_decay_rate, "token_extra_decay": token_extra_decay, "accepted": accepted, "prior_step_states": prior_step_states, "output_norm_gain": output_norm_gain, "output_projection": output_projection}


epsilon = 1e-06
highest = lax.Precision.HIGHEST

def unit_rows(values):
    return values * lax.rsqrt(lax.optimization_barrier(jnp.sum(values * values, axis=-1, keepdims=True)) + epsilon)

def delta_block(query_heads, key_heads, value_heads, beta_gate, decay_logarithm, start_state):
    proposal_len = query_heads.shape[2]
    cumulative = jnp.cumsum(decay_logarithm, axis=-1)
    spread = cumulative[..., :, None] - cumulative[..., None, :]
    strict = jnp.tril(jnp.ones((proposal_len, proposal_len), bool), -1)
    inclusive = jnp.tril(jnp.ones((proposal_len, proposal_len), bool))
    key_inner = jnp.einsum('nhid,nhjd->nhij', key_heads, key_heads, precision=highest)
    coupling = jnp.where(strict, beta_gate[..., :, None] * key_inner * jnp.exp(jnp.where(strict, spread, 0.0)), 0.0)
    growth = jnp.exp(cumulative)
    right_w = (beta_gate * growth)[..., None] * key_heads
    right_u = beta_gate[..., None] * value_heads
    solved_w = []
    solved_u = []
    for current in range(proposal_len):
        part_w = right_w[:, :, current]
        part_u = right_u[:, :, current]
        for earlier in range(current):
            factor = coupling[:, :, current, earlier][..., None]
            part_w = part_w - factor * solved_w[earlier]
            part_u = part_u - factor * solved_u[earlier]
        solved_w.append(part_w)
        solved_u.append(part_u)
    weights_w = jnp.stack(solved_w, axis=2)
    weights_u = jnp.stack(solved_u, axis=2)
    corrected = weights_u - jnp.einsum('nhpd,nhde->nhpe', weights_w, start_state, precision=highest)
    within = jnp.where(inclusive, jnp.exp(jnp.where(inclusive, spread, 0.0)), 0.0)
    scores = jnp.einsum('nhid,nhjd->nhij', query_heads, key_heads, precision=highest) * within
    attended = jnp.einsum('nhpd,nhde->nhpe', query_heads * growth[..., None], start_state, precision=highest) + jnp.einsum('nhij,nhje->nhie', scores, corrected, precision=highest)
    states = growth[..., None, None] * start_state[:, :, None] + jnp.einsum('nhtj,nhjd,nhje->nhtde', within, key_heads, corrected, precision=highest)
    return (attended, states)

def combine_heads(query_logits, key_logits, value_logits, beta_logits, decay_logits, head_decay_rate, token_extra_decay, accepted, prior_step_states, output_norm_gain):
    seq_count, proposal_len, head_count = beta_logits.shape
    head_size = query_logits.shape[-1] // head_count

    def by_heads(values):
        return jnp.transpose(values.reshape(seq_count, proposal_len, head_count, head_size), (0, 2, 1, 3))
    query_heads = unit_rows(by_heads(jax.nn.silu(query_logits))) * head_size ** (-0.5)
    key_heads = unit_rows(by_heads(jax.nn.silu(key_logits)))
    value_heads = by_heads(jax.nn.silu(value_logits))
    beta_gate = jnp.transpose(jax.nn.sigmoid(beta_logits), (0, 2, 1))
    decay_logarithm = jnp.transpose(-head_decay_rate[None, None, :] * jax.nn.softplus(decay_logits) + token_extra_decay, (0, 2, 1))
    chosen = jnp.arange(proposal_len, dtype=jnp.int32)[None, :] == (accepted - 1)[:, None]
    picked = lax.optimization_barrier(jnp.sum(jnp.where(chosen[:, :, None, None], prior_step_states, 0.0), axis=1))
    start_state = picked.reshape(seq_count, head_count, head_size, head_size)
    attended, states = delta_block(query_heads, key_heads, value_heads, beta_gate, decay_logarithm, start_state)
    inverse_rms = lax.rsqrt(lax.optimization_barrier(jnp.mean(attended * attended, axis=-1, keepdims=True)) + epsilon)
    normalized_rows = (attended * inverse_rms * output_norm_gain).astype(jnp.bfloat16)
    normalized_rows = jnp.transpose(normalized_rows, (0, 2, 1, 3)).reshape(seq_count, proposal_len, head_count * head_size)
    updated_states = jnp.transpose(states, (0, 2, 1, 3, 4)).reshape(seq_count, proposal_len, head_count, head_size * head_size)
    return (normalized_rows, updated_states)

def reference(tokens, input_norm_gain, query_projection, key_projection, value_projection, write_strength_weight, decay_projection, head_decay_rate, token_extra_decay, accepted, prior_step_states, output_norm_gain, output_projection):
    seq_total, proposal_len, feature_count = tokens.shape
    token_rows = tokens.reshape(seq_total * proposal_len, feature_count).astype(jnp.float32)
    inverse = lax.rsqrt(lax.optimization_barrier(jnp.sum(token_rows * token_rows, axis=1)) / feature_count + epsilon)[:, None]
    scaled = (token_rows * input_norm_gain[None, :]).astype(jnp.bfloat16)

    def apply_projection(weight):
        result = jnp.dot(scaled, weight, preferred_element_type=jnp.float32) * inverse
        return result.reshape(seq_total, proposal_len, weight.shape[1])
    block_count = seq_total // SEQ_DEV

    def divide_blocks(values):
        return values.reshape((block_count, SEQ_DEV) + values.shape[1:])

    def single_block(input_rows):
        query_logits, key_logits, value_logits, beta_logits, decay_logits, extra_decay_slice, accepted_slice, saved_slice = input_rows
        return combine_heads(query_logits, key_logits, value_logits, beta_logits, decay_logits, head_decay_rate, extra_decay_slice, accepted_slice, saved_slice, output_norm_gain)
    normalized_rows, updated_states = lax.map(single_block, (divide_blocks(apply_projection(query_projection)), divide_blocks(apply_projection(key_projection)), divide_blocks(apply_projection(value_projection)), divide_blocks(apply_projection(write_strength_weight)), divide_blocks(apply_projection(decay_projection)), divide_blocks(token_extra_decay), divide_blocks(accepted), divide_blocks(prior_step_states)))
    normed_rows = normalized_rows.reshape(seq_total * proposal_len, output_projection.shape[0])
    mixed = jnp.dot(normed_rows, output_projection, preferred_element_type=jnp.float32).astype(jnp.bfloat16)
    return (mixed.reshape(seq_total, proposal_len, feature_count), updated_states.reshape(prior_step_states.shape))
```

```python
import jax
import jax.numpy as jnp
import numpy as np
from jax import lax
from jax.experimental import pallas as pl
from jax.experimental.pallas import tpu as pltpu
from jax.sharding import Mesh
from jax.sharding import PartitionSpec as P

D = 2048
epsilon = 1e-06
KV = ("z8", "zp", "y")
DP_KV = ("dp", "z8", "zp", "y")
NEAR = ("zp", "y")
f32 = jnp.float32
bf16 = jnp.bfloat16

WO, QKV, SMALL, TOK, WIDE = 0, 512, 2048, 2176, 2304
VMEM = pl.BlockSpec(memory_space=pltpu.VMEM)
SMEM = pl.BlockSpec(memory_space=pltpu.SMEM)


def iota(shape, dim):
    return lax.broadcasted_iota(jnp.int32, shape, dim)


def dot(a, b, ca, cb):
    return lax.dot_general(a, b, (((ca,), (cb,)), ((), ())), preferred_element_type=f32)


def pack_kernel(tok_ref, gain_ref, q_ref, k_ref, v_ref, beta_ref, decay_ref, wo_ref, out_ref):
    eye = iota((32, 32), 0) == iota((32, 32), 1)
    gain = jnp.sum(jnp.where(eye, gain_ref[...], 0.0), axis=1, keepdims=True)
    raw = jnp.concatenate([tok_ref[t] for t in range(4)], axis=1)
    scaled = (raw.astype(f32) * gain).astype(bf16)
    source, dest = iota((512, 512), 0), iota((512, 512), 1)
    group, rho = dest // 64, dest % 64
    wanted = (rho % 4) * 128 + (rho // 8) * 16 + group * 2 + (rho % 8) // 4
    pick = (source == wanted).astype(f32).astype(bf16)
    both = dot(jnp.concatenate([scaled, raw], axis=0), pick, 1, 0)
    head, lane = iota((8, 128), 0), iota((8, 128), 1)
    put_beta = ((lane == head) | (lane == head + 16)).astype(f32).astype(bf16)
    put_decay = ((lane == head + 8) | (lane == head + 24)).astype(f32).astype(bf16)
    small = dot(beta_ref[...], put_beta, 0, 0) + dot(decay_ref[...], put_decay, 0, 0)
    small = small.astype(bf16)
    low = iota((32, 128), 1) < 64
    for r in range(8):
        s = both[:32, 128 * (r // 2) : 128 * (r // 2) + 128]
        w = both[32:, 128 * (r // 2) : 128 * (r // 2) + 128]
        if r % 2 == 0:
            tile = jnp.where(low, s, pltpu.roll(w, 64, 1))
        else:
            tile = jnp.where(low, pltpu.roll(s, 64, 1), w)
        out_ref[r, :, WO:QKV] = wo_ref[...]
        out_ref[r, :, QKV : QKV + 512] = q_ref[...]
        out_ref[r, :, QKV + 512 : QKV + 1024] = k_ref[...]
        out_ref[r, :, QKV + 1024 : SMALL] = v_ref[...]
        out_ref[r, :, SMALL:TOK] = small
        out_ref[r, :, TOK:] = tile.astype(bf16)


def project_kernel(x_ref, out_ref):
    x = x_ref[...].reshape(256, WIDE)
    cols = x[:, TOK:]
    raw = cols.astype(f32)
    square = raw * raw
    high = square.astype(bf16)
    rest = (square - high.astype(f32)).astype(bf16)
    lane = iota((256, 128), 1)
    ones = ((lane == 32) | (lane == 33)).astype(f32).astype(bf16)
    sums = dot(high, ones, 0, 0) + dot(rest, ones, 0, 0)
    main = dot(cols, x[:, QKV:SMALL], 0, 0)
    out_ref[:, : SMALL - QKV] = main[:64].astype(bf16)
    tail = dot(cols, x[:, SMALL:TOK], 0, 0)[:64] + sums[64:]
    first = tail.astype(bf16).astype(f32)
    lane = iota((64, 128), 1)
    keep = (lane < 16) | (lane == 32)
    out_ref[:, SMALL - QKV :] = jnp.where(keep, first, tail - first).astype(bf16)


def delta_kernel(
    accepted_ref, c_ref, prior_ref, rate_ref, extra_ref, gain_ref, states_ref, rows_ref, aux, nrows
):
    c = c_ref[...].astype(f32)
    s = c[0:8]
    for z in range(1, 8):
        s = s + c[8 * z : 8 * z + 8]
    tile = s[:, 1536:]
    total = tile[:, 32:33] + tile[:, 33:34]
    inverse = lax.rsqrt(total / D + epsilon)
    logits = jnp.transpose((tile + pltpu.roll(tile, 112, 1)) * inverse)
    aux[...] = jnp.zeros((8, 128), f32)
    aux[0:4, 0:8] = extra_ref[0]
    aux[4:8, 0:8] = extra_ref[1]
    aux[:, 8:16] = jnp.broadcast_to(rate_ref[...], (8, 8))
    side = jnp.transpose(aux[...])
    beta = jax.nn.sigmoid(logits[0:8])
    fade = jnp.exp(-side[8:16] * jax.nn.softplus(logits[8:16]) + side[0:8])

    sub, lane = iota((8, 128), 0), iota((8, 128), 1)
    masks = [sub == 2 * p + lane // 64 for p in range(4)]
    gain = jnp.concatenate([gain_ref[...], gain_ref[...]], axis=1)

    def silu_of(at):
        u = s[:, at : at + 512] * inverse
        return u / (1.0 + jnp.exp(-u))

    parts = [silu_of(0), silu_of(512), silu_of(1024)]

    def by_heads(values, row):
        m = jnp.zeros((8, 128), f32)
        for p in range(4):
            piece = jnp.broadcast_to(values[row : row + 1, 128 * p : 128 * p + 128], (8, 128))
            m = jnp.where(masks[p], piece, m)
        return m + pltpu.roll(m, 64, 1)

    def unit(values):
        return values * lax.rsqrt(0.5 * jnp.sum(values * values, axis=1, keepdims=True) + epsilon)

    def spread(values, i):
        return jnp.take_along_axis(values, lane // 64 + 2 * i, axis=1, mode="promise_in_bounds")

    for j in range(2):
        start = accepted_ref[j] - 1
        state = [prior_ref[j, start, :, 128 * i : 128 * i + 128] for i in range(32)]
        for t in range(4):
            row = 4 * j + t
            q = unit(by_heads(parts[0], row)) * 0.125
            k = unit(by_heads(parts[1], row))
            v = by_heads(parts[2], row)
            a = jnp.broadcast_to(fade[:, row : row + 1], (8, 128))
            b = jnp.broadcast_to(beta[:, row : row + 1], (8, 128))
            kx = [spread(k, i) for i in range(32)]
            sums = [kx[i] * state[i] for i in range(4)]
            for i in range(4, 32):
                sums[i % 4] = sums[i % 4] + kx[i] * state[i]
            u = (sums[0] + sums[1]) + (sums[2] + sums[3])
            u = u + pltpu.roll(u, 64, 1)
            w = b * (v - a * u)
            sums = [None] * 4
            for i in range(32):
                state[i] = a * state[i] + kx[i] * w
                states_ref[j, t, :, 128 * i : 128 * i + 128] = state[i]
                term = spread(q, i) * state[i]
                sums[i % 4] = term if i < 4 else sums[i % 4] + term
            o = (sums[0] + sums[1]) + (sums[2] + sums[3])
            o = o + pltpu.roll(o, 64, 1)
            mean = jnp.sum(o * o, axis=1, keepdims=True) / 128
            n = o * lax.rsqrt(mean + epsilon) * gain
            for p in range(4):
                nrows[row : row + 1, 128 * p : 128 * p + 128] = jnp.sum(
                    jnp.where(masks[p], n, 0.0), axis=0, keepdims=True
                )
    rows = nrows[...]
    rows_ref[...] = jnp.concatenate([rows] * 8, axis=0).astype(bf16)


def mix_kernel(x_ref, rows_ref, out_ref):
    w = x_ref[:, :, WO:QKV].reshape(256, 512)
    out = dot(w, rows_ref[...], 1, 1).astype(bf16)
    for r in range(8):
        out_ref[2 * r] = out[32 * r : 32 * r + 32]
        out_ref[2 * r + 1] = out[32 * r : 32 * r + 32]


def place_kernel(x_ref, back_ref, out_ref):
    whole = jnp.zeros((32, 512), f32)
    for r in range(8):
        both = (x_ref[2 * r].astype(f32) + x_ref[2 * r + 1].astype(f32)).astype(bf16)
        whole = whole + dot(both, back_ref[64 * r : 64 * r + 64, :], 1, 0)
    for t in range(4):
        out_ref[t] = whole[:, 128 * t : 128 * t + 128].astype(bf16)


def back_table():
    dest = np.arange(512)
    group, rho = dest // 64, dest % 64
    wanted = (rho % 4) * 128 + (rho // 8) * 16 + group * 2 + (rho % 8) // 4
    return (wanted[:, None] == np.arange(512)[None, :]).astype(jnp.bfloat16)


def call(kernel, shapes, args, specs=None, scratch=(), name=None):
    one = not isinstance(shapes, tuple)
    return pl.pallas_call(
        kernel,
        out_shape=shapes,
        in_specs=specs or [VMEM] * len(args),
        out_specs=VMEM if one else tuple([VMEM] * len(shapes)),
        scratch_shapes=scratch,
        name=name,
    )(*args)


def shape(dims, dtype):
    return jax.ShapeDtypeStruct(dims, dtype)


def per_device(
    tokens,
    input_norm_gain,
    query_projection,
    key_projection,
    value_projection,
    write_strength_weight,
    decay_projection,
    head_decay_rate,
    token_extra_decay,
    accepted,
    prior_step_states,
    output_norm_gain,
    output_projection,
):
    def swap(x, axes):
        return lax.all_to_all(x, axes, 0, 0, tiled=True)

    packed = call(
        pack_kernel,
        shape((8, 32, WIDE), bf16),
        (
            jnp.transpose(tokens, (1, 2, 0)),
            input_norm_gain[None, :],
            query_projection,
            key_projection,
            value_projection,
            write_strength_weight.T,
            decay_projection.T,
            output_projection.T,
        ),
        name="pack",
    )
    near = swap(packed, NEAR)
    part = call(project_kernel, shape((64, SMALL + 128 - QKV), bf16), (near,), name="project")
    arrived = swap(part.reshape(8, 8, part.shape[1]), "z8").reshape(part.shape)
    states, rows = call(
        delta_kernel,
        (shape(prior_step_states.shape, f32), shape((64, 512), bf16)),
        (
            accepted,
            arrived,
            prior_step_states,
            head_decay_rate[None, :],
            token_extra_decay,
            output_norm_gain[None, :],
        ),
        specs=[SMEM] + [VMEM] * 5,
        scratch=[pltpu.VMEM((8, 128), f32), pltpu.VMEM((8, 512), f32)],
        name="delta",
    )
    all_rows = swap(rows.reshape(8, 8, 512), "z8").reshape(64, 512)
    columns = call(mix_kernel, shape((16, 32, 64), bf16), (near, all_rows), name="mix")
    back = swap(columns, ("zp", "y", "tp"))
    mixed = call(
        place_kernel, shape((4, 32, 128), bf16), (back, jnp.asarray(back_table())), name="place"
    )
    return (jnp.transpose(mixed, (2, 0, 1)), states)


def solution(mesh):
    split = Mesh(
        mesh.devices.reshape(mesh.shape["dp"], 8, 2, 4, mesh.shape["tp"]),
        ("dp", "z8", "zp", "y", "tp"),
    )
    in_specs = (
        P("dp", None, KV),
        P(KV),
        P(KV, "tp"),
        P(KV, "tp"),
        P(KV, "tp"),
        P(KV, "tp"),
        P(KV, "tp"),
        P("tp"),
        P(DP_KV, None, "tp"),
        P(DP_KV),
        P(DP_KV, None, "tp", None),
        P(),
        P("tp", KV),
    )
    out_specs = (P("dp", None, KV), P(DP_KV, None, "tp", None))
    return jax.shard_map(
        per_device, mesh=split, in_specs=in_specs, out_specs=out_specs, check_vma=False
    )
```

```python
import jax
import jax.numpy as jnp
import numpy as np
from jax import lax
from jax.experimental import pallas as pl
from jax.experimental.pallas import tpu as pltpu
from jax.sharding import Mesh
from jax.sharding import PartitionSpec as P

D = 2048
epsilon = 1e-06
KV = ("z8", "zp", "y")
DP_KV = ("dp", "z8", "zp", "y")
NEAR = ("zp", "y")
f32 = jnp.float32
bf16 = jnp.bfloat16

WO, QKV, SMALL, TOK, WIDE = 0, 512, 2048, 2176, 2304
VMEM = pl.BlockSpec(memory_space=pltpu.VMEM)
SMEM = pl.BlockSpec(memory_space=pltpu.SMEM)


def iota(shape, dim):
    return lax.broadcasted_iota(jnp.int32, shape, dim)


def dot(a, b, ca, cb):
    return lax.dot_general(a, b, (((ca,), (cb,)), ((), ())), preferred_element_type=f32)


def pack_kernel(tok_ref, gain_ref, q_ref, k_ref, v_ref, beta_ref, decay_ref, wo_ref, out_ref):
    eye = iota((32, 32), 0) == iota((32, 32), 1)
    gain = jnp.sum(jnp.where(eye, gain_ref[...], 0.0), axis=1, keepdims=True)
    raw = jnp.concatenate([tok_ref[t] for t in range(4)], axis=1)
    scaled = (raw.astype(f32) * gain).astype(bf16)
    source, dest = iota((512, 512), 0), iota((512, 512), 1)
    group, rho = dest // 64, dest % 64
    wanted = (rho % 4) * 128 + (rho // 8) * 16 + group * 2 + (rho % 8) // 4
    pick = (source == wanted).astype(f32).astype(bf16)
    both = dot(jnp.concatenate([scaled, raw], axis=0), pick, 1, 0)
    head, lane = iota((8, 128), 0), iota((8, 128), 1)
    put_beta = ((lane == head) | (lane == head + 16)).astype(f32).astype(bf16)
    put_decay = ((lane == head + 8) | (lane == head + 24)).astype(f32).astype(bf16)
    small = dot(beta_ref[...], put_beta, 0, 0) + dot(decay_ref[...], put_decay, 0, 0)
    small = small.astype(bf16)
    low = iota((32, 128), 1) < 64
    for r in range(8):
        s = both[:32, 128 * (r // 2) : 128 * (r // 2) + 128]
        w = both[32:, 128 * (r // 2) : 128 * (r // 2) + 128]
        if r % 2 == 0:
            tile = jnp.where(low, s, pltpu.roll(w, 64, 1))
        else:
            tile = jnp.where(low, pltpu.roll(s, 64, 1), w)
        out_ref[r, :, WO:QKV] = wo_ref[...]
        out_ref[r, :, QKV : QKV + 512] = q_ref[...]
        out_ref[r, :, QKV + 512 : QKV + 1024] = k_ref[...]
        out_ref[r, :, QKV + 1024 : SMALL] = v_ref[...]
        out_ref[r, :, SMALL:TOK] = small
        out_ref[r, :, TOK:] = tile.astype(bf16)


def project_kernel(x_ref, out_ref):
    x = x_ref[...].reshape(256, WIDE)
    cols = x[:, TOK:]
    raw = cols.astype(f32)
    square = raw * raw
    high = square.astype(bf16)
    rest = (square - high.astype(f32)).astype(bf16)
    lane = iota((256, 128), 1)
    ones = ((lane == 32) | (lane == 33)).astype(f32).astype(bf16)
    sums = dot(high, ones, 0, 0) + dot(rest, ones, 0, 0)
    main = dot(cols, x[:, QKV:SMALL], 0, 0)
    out_ref[:, : SMALL - QKV] = main[:64].astype(bf16)
    tail = dot(cols, x[:, SMALL:TOK], 0, 0)[:64] + sums[64:]
    first = tail.astype(bf16).astype(f32)
    lane = iota((64, 128), 1)
    keep = (lane < 16) | (lane == 32)
    out_ref[:, SMALL - QKV :] = jnp.where(keep, first, tail - first).astype(bf16)


def delta_kernel(
    accepted_ref, c_ref, prior_ref, rate_ref, extra_ref, gain_ref, out_ref, rows_ref,
    aux, nrows, states_ref, sems
):
    c = c_ref[...].astype(f32)
    s = c[0:8]
    for z in range(1, 8):
        s = s + c[8 * z : 8 * z + 8]
    tile = s[:, 1536:]
    total = tile[:, 32:33] + tile[:, 33:34]
    inverse = lax.rsqrt(total / D + epsilon)
    logits = jnp.transpose((tile + pltpu.roll(tile, 112, 1)) * inverse)
    aux[...] = jnp.zeros((8, 128), f32)
    aux[0:4, 0:8] = extra_ref[0]
    aux[4:8, 0:8] = extra_ref[1]
    aux[:, 8:16] = jnp.broadcast_to(rate_ref[...], (8, 8))
    side = jnp.transpose(aux[...])
    beta = jax.nn.sigmoid(logits[0:8])
    fade = jnp.exp(-side[8:16] * jax.nn.softplus(logits[8:16]) + side[0:8])

    sub, lane = iota((8, 128), 0), iota((8, 128), 1)
    masks = [sub == 2 * p + lane // 64 for p in range(4)]
    gain = jnp.concatenate([gain_ref[...], gain_ref[...]], axis=1)

    def silu_of(at):
        u = s[:, at : at + 512] * inverse
        return u / (1.0 + jnp.exp(-u))

    parts = [silu_of(0), silu_of(512), silu_of(1024)]

    def by_heads(values, row):
        m = jnp.zeros((8, 128), f32)
        for p in range(4):
            piece = jnp.broadcast_to(values[row : row + 1, 128 * p : 128 * p + 128], (8, 128))
            m = jnp.where(masks[p], piece, m)
        return m + pltpu.roll(m, 64, 1)

    def unit(values):
        return values * lax.rsqrt(0.5 * jnp.sum(values * values, axis=1, keepdims=True) + epsilon)

    def spread(values, i):
        return jnp.take_along_axis(values, lane // 64 + 2 * i, axis=1, mode="promise_in_bounds")

    copies = []
    for j in range(2):
        start = accepted_ref[j] - 1
        state = [prior_ref[j, start, :, 128 * i : 128 * i + 128] for i in range(32)]
        for t in range(4):
            row = 4 * j + t
            q = unit(by_heads(parts[0], row)) * 0.125
            k = unit(by_heads(parts[1], row))
            v = by_heads(parts[2], row)
            a = jnp.broadcast_to(fade[:, row : row + 1], (8, 128))
            b = jnp.broadcast_to(beta[:, row : row + 1], (8, 128))
            kx = [spread(k, i) for i in range(32)]
            sums = [kx[i] * state[i] for i in range(4)]
            for i in range(4, 32):
                sums[i % 4] = sums[i % 4] + kx[i] * state[i]
            u = (sums[0] + sums[1]) + (sums[2] + sums[3])
            u = u + pltpu.roll(u, 64, 1)
            w = b * (v - a * u)
            sums = [None] * 4
            for i in range(32):
                state[i] = a * state[i] + kx[i] * w
                states_ref[j, t, :, 128 * i : 128 * i + 128] = state[i]
                term = spread(q, i) * state[i]
                sums[i % 4] = term if i < 4 else sums[i % 4] + term
            copies.append(
                pltpu.make_async_copy(states_ref.at[j, t], out_ref.at[j, t], sems.at[row])
            )
            copies[-1].start()
            o = (sums[0] + sums[1]) + (sums[2] + sums[3])
            o = o + pltpu.roll(o, 64, 1)
            mean = jnp.sum(o * o, axis=1, keepdims=True) / 128
            n = o * lax.rsqrt(mean + epsilon) * gain
            for p in range(4):
                nrows[row : row + 1, 128 * p : 128 * p + 128] = jnp.sum(
                    jnp.where(masks[p], n, 0.0), axis=0, keepdims=True
                )
    rows = nrows[...]
    rows_ref[...] = jnp.concatenate([rows] * 8, axis=0).astype(bf16)
    for copy in copies:
        copy.wait()


def mix_kernel(x_ref, rows_ref, out_ref):
    w = x_ref[:, :, WO:QKV].reshape(256, 512)
    rows = rows_ref[...]
    out = dot(w, jnp.concatenate([rows, rows], axis=0), 1, 1)
    low = iota((16, 128), 1) < 64
    for r in range(8):
        piece = jnp.where(low, out[32 * r : 32 * r + 16], out[32 * r + 16 : 32 * r + 32])
        out_ref[2 * r] = piece.astype(bf16)
        out_ref[2 * r + 1] = piece.astype(bf16)


def place_kernel(x_ref, back_ref, out_ref):
    low = iota((16, 128), 1) < 64
    sums = [x_ref[2 * r].astype(f32) + x_ref[2 * r + 1].astype(f32) for r in range(8)]
    tiles = []
    for p in range(4):
        a, b = sums[2 * p], sums[2 * p + 1]
        top = jnp.where(low, a, pltpu.roll(b, 64, 1))
        end = jnp.where(low, pltpu.roll(a, 64, 1), b)
        tiles.append(jnp.concatenate([top, end], axis=0).astype(bf16))
    whole = dot(jnp.concatenate(tiles, axis=1), back_ref[...], 1, 0).astype(bf16)
    for t in range(4):
        out_ref[t] = whole[:, 128 * t : 128 * t + 128]


def back_table():
    dest = np.arange(512)
    group, rho = dest // 64, dest % 64
    wanted = (rho % 4) * 128 + (rho // 8) * 16 + group * 2 + (rho % 8) // 4
    return (wanted[:, None] == np.arange(512)[None, :]).astype(jnp.bfloat16)


def call(kernel, shapes, args, specs=None, scratch=(), outs=VMEM, name=None):
    if name == "pack":
        args = [pltpu.with_memory_space_constraint(a, pltpu.HBM) for a in args]
    return pl.pallas_call(
        kernel,
        out_shape=shapes,
        in_specs=specs or [VMEM] * len(args),
        out_specs=outs,
        scratch_shapes=scratch,
        compiler_params=pltpu.CompilerParams(vmem_limit_bytes=16 << 20),
        name=name,
    )(*args)


def shape(dims, dtype):
    return jax.ShapeDtypeStruct(dims, dtype)


def per_device(
    tokens,
    input_norm_gain,
    query_projection,
    key_projection,
    value_projection,
    write_strength_weight,
    decay_projection,
    head_decay_rate,
    token_extra_decay,
    accepted,
    prior_step_states,
    output_norm_gain,
    output_projection,
):
    def swap(x, axes):
        return lax.all_to_all(x, axes, 0, 0, tiled=True)

    packed = call(
        pack_kernel,
        shape((8, 32, WIDE), bf16),
        (
            jnp.transpose(tokens, (1, 2, 0)),
            input_norm_gain[None, :],
            query_projection,
            key_projection,
            value_projection,
            write_strength_weight.T,
            decay_projection.T,
            output_projection.T,
        ),
        name="pack",
    )
    near = swap(packed, NEAR)
    part = call(project_kernel, shape((64, SMALL + 128 - QKV), bf16), (near,), name="project")
    arrived = swap(part.reshape(8, 8, part.shape[1]), "z8").reshape(part.shape)
    states, rows = call(
        delta_kernel,
        (shape(prior_step_states.shape, f32), shape((64, 512), bf16)),
        (
            accepted,
            arrived,
            prior_step_states,
            head_decay_rate[None, :],
            token_extra_decay,
            output_norm_gain[None, :],
        ),
        specs=[SMEM] + [VMEM] * 5,
        scratch=[
            pltpu.VMEM((8, 128), f32),
            pltpu.VMEM((8, 512), f32),
            pltpu.VMEM((2, 4, 8, 4096), f32),
            pltpu.SemaphoreType.DMA((8,)),
        ],
        outs=(pl.BlockSpec(memory_space=pltpu.HBM), VMEM),
        name="delta",
    )
    all_rows = swap(rows.reshape(8, 8, 512), "z8").reshape(64, 512)
    columns = call(mix_kernel, shape((16, 16, 128), bf16), (near, all_rows), name="mix")
    back = swap(columns, ("zp", "y", "tp"))
    mixed = call(
        place_kernel, shape((4, 32, 128), bf16), (back, jnp.asarray(back_table())), name="place"
    )
    return (jnp.transpose(mixed, (2, 0, 1)), states)


def solution(mesh):
    split = Mesh(
        mesh.devices.reshape(mesh.shape["dp"], 8, 2, 4, mesh.shape["tp"]),
        ("dp", "z8", "zp", "y", "tp"),
    )
    in_specs = (
        P("dp", None, KV),
        P(KV),
        P(KV, "tp"),
        P(KV, "tp"),
        P(KV, "tp"),
        P(KV, "tp"),
        P(KV, "tp"),
        P("tp"),
        P(DP_KV, None, "tp"),
        P(DP_KV),
        P(DP_KV, None, "tp", None),
        P(),
        P("tp", KV),
    )
    out_specs = (P("dp", None, KV), P(DP_KV, None, "tp", None))
    return jax.shard_map(
        per_device, mesh=split, in_specs=in_specs, out_specs=out_specs, check_vma=False
    )
```

```python
import jax
import jax.numpy as jnp
import numpy as np
from jax import lax
from jax.experimental import pallas as pl
from jax.experimental.pallas import tpu as pltpu
from jax.sharding import Mesh
from jax.sharding import PartitionSpec as P

D = 2048
epsilon = 1e-06
KV = ("z8", "zp", "y")
DP_KV = ("dp", "z8", "zp", "y")
NEAR = ("zp", "y")
f32 = jnp.float32
bf16 = jnp.bfloat16

WO, QKV, SMALL, WIDE = 0, 512, 2048, 2176
VMEM = pl.BlockSpec(memory_space=pltpu.VMEM)
SMEM = pl.BlockSpec(memory_space=pltpu.SMEM)
HBM = pl.BlockSpec(memory_space=pltpu.HBM)


def iota(shape, dim):
    return lax.broadcasted_iota(jnp.int32, shape, dim)


def dot(a, b, ca, cb):
    return lax.dot_general(a, b, (((ca,), (cb,)), ((), ())), preferred_element_type=f32)


def pack_kernel(*refs):
    hbm, out_ref, held, sems = refs[:8], refs[8], refs[9:17], refs[17]
    copies = [pltpu.make_async_copy(hbm[n], held[n], sems.at[n]) for n in range(8)]
    for copy in copies:
        copy.start()
    tok_ref, gain_ref, q_ref, k_ref, v_ref, beta_ref, decay_ref, wo_ref = held
    source, dest = iota((512, 512), 0), iota((1, 512), 1)
    group, rho = dest // 64, dest % 64
    wanted = (rho % 4) * 128 + (rho // 8) * 16 + group * 2 + (rho % 8) // 4
    pick = (source == wanted).astype(f32).astype(bf16)
    eye = iota((32, 32), 0) == iota((32, 32), 1)
    head, lane = iota((8, 128), 0), iota((8, 128), 1)
    put_beta = ((lane == head) | (lane == head + 16)).astype(f32).astype(bf16)
    put_decay = ((lane == head + 8) | (lane == head + 24)).astype(f32).astype(bf16)
    copies[0].wait()
    copies[1].wait()
    gain = jnp.sum(jnp.where(eye, gain_ref[...], 0.0), axis=1, keepdims=True)
    raw = jnp.concatenate([tok_ref[t] for t in range(4)], axis=1).astype(f32)
    scaled = raw * gain
    squares = jnp.sum(raw * raw, axis=0, keepdims=True)
    high = squares.astype(bf16).astype(f32)
    sub = iota((16, 512), 0)
    extra = jnp.where(sub < 2, high, jnp.where(sub < 4, squares - high, 0.0))
    moved = dot(jnp.concatenate([scaled, extra], axis=0).astype(bf16), pick, 1, 0)
    copies[5].wait()
    copies[6].wait()
    small = dot(beta_ref[...], put_beta, 0, 0) + dot(decay_ref[...], put_decay, 0, 0)
    lane = iota((8, 128), 1)
    even = iota((8, 128), 0) % 2 == 0
    for n in (2, 3, 4, 7):
        copies[n].wait()
    for r in range(8):
        at = slice(128 * (r // 2), 128 * (r // 2) + 128)
        sums = moved[32:40, at]
        if r % 2 == 0:
            cols = pltpu.roll(moved[:32, at], 64, 1)
            sums = jnp.where(even, pltpu.roll(sums, 32, 1), sums)
        else:
            cols = moved[:32, at]
            sums = jnp.where(even, pltpu.roll(sums, 96, 1), pltpu.roll(sums, 64, 1))
        groups = []
        for g in range(4):
            right = jnp.where(lane < 64, sums if g == 0 else 0.0, cols[8 * g : 8 * g + 8])
            groups.append(jnp.where(lane < 32, small[8 * g : 8 * g + 8], right))
        tile = jnp.concatenate(groups, axis=0)
        out_ref[r, :, WO:QKV] = wo_ref[...]
        out_ref[r, :, QKV : QKV + 512] = q_ref[...]
        out_ref[r, :, QKV + 512 : QKV + 1024] = k_ref[...]
        out_ref[r, :, QKV + 1024 : SMALL] = v_ref[...]
        out_ref[r, :, SMALL:] = tile.astype(bf16)


def project_kernel(x_ref, out_ref):
    x = x_ref[...].reshape(256, WIDE)
    cols = x[:, SMALL:]
    main = dot(cols, x[:, QKV:SMALL], 0, 0)
    out_ref[:, : SMALL - QKV] = main[64:].astype(bf16)
    sums = jnp.zeros((8, 128), f32)
    for r in range(8):
        sums = sums + cols[32 * r : 32 * r + 16].astype(f32)[0:8]
    sub, lane = iota((32, 128), 0), iota((32, 128), 1)
    halves = []
    for n in range(2):
        row = sums[n : n + 1] + sums[n + 2 : n + 3]
        halves.append(jnp.sum(jnp.where(lane == sub + 32, row, 0.0), axis=1, keepdims=True))
    total = jnp.concatenate(halves, axis=0)
    lane = iota((64, 128), 1)
    tail = jnp.where(lane < 32, dot(cols, cols, 0, 0)[64:], jnp.where(lane < 34, total, 0.0))
    first = tail.astype(bf16).astype(f32)
    keep = (lane < 16) | (lane == 32)
    out_ref[:, SMALL - QKV :] = jnp.where(keep, first, tail - first).astype(bf16)


def delta_kernel(
    accepted_ref, c_ref, prior_ref, rate_ref, extra_ref, gain_ref, out_ref, rows_ref,
    aux, nrows, states_ref, kept, sems
):
    c = c_ref[...].astype(f32)
    s = (c[0:8] + c[8:16]) + (c[16:24] + c[24:32])
    s = s + ((c[32:40] + c[40:48]) + (c[48:56] + c[56:64]))
    tile = s[:, 1536:]
    total = tile[:, 32:33] + tile[:, 33:34]
    inverse = lax.rsqrt(total / D + epsilon)
    logits = jnp.transpose((tile + pltpu.roll(tile, 112, 1)) * inverse)
    aux[...] = jnp.zeros((8, 128), f32)
    aux[0:4, 0:8] = extra_ref[0]
    aux[4:8, 0:8] = extra_ref[1]
    aux[:, 8:16] = jnp.broadcast_to(rate_ref[...], (8, 8))
    side = jnp.transpose(aux[...])
    beta = jax.nn.sigmoid(logits[0:8])
    fade = jnp.exp(-side[8:16] * jax.nn.softplus(logits[8:16]) + side[0:8])

    sub, lane = iota((8, 128), 0), iota((8, 128), 1)
    masks = [sub == 2 * p + lane // 64 for p in range(4)]
    gain = jnp.concatenate([gain_ref[...], gain_ref[...]], axis=1)

    def silu_of(at):
        u = s[:, at : at + 512] * inverse
        return u / (1.0 + jnp.exp(-u))

    parts = [silu_of(0), silu_of(512), silu_of(1024)]

    def by_heads(values, row):
        m = jnp.zeros((8, 128), f32)
        for p in range(4):
            piece = jnp.broadcast_to(values[row : row + 1, 128 * p : 128 * p + 128], (8, 128))
            m = jnp.where(masks[p], piece, m)
        return m + pltpu.roll(m, 64, 1)

    def half_sum(values):
        return 0.5 * jnp.sum(values, axis=1, keepdims=True)

    def unit(values):
        return values * lax.rsqrt(half_sum(values * values) + epsilon)

    ROWS = range(8)
    q = [unit(by_heads(parts[0], row)) * 0.125 for row in ROWS]
    k = [unit(by_heads(parts[1], row)) for row in ROWS]
    v = [by_heads(parts[2], row) for row in ROWS]
    a = [jnp.broadcast_to(fade[:, row : row + 1], (8, 128)) for row in ROWS]
    b = [jnp.broadcast_to(beta[:, row : row + 1], (8, 128)) for row in ROWS]

    starts = [accepted_ref[0] - 1, accepted_ref[1] - 1]
    ks, qs = [None] * 8, [None] * 8
    for i in range(32):
        index = lane // 64 + 2 * i
        at = slice(128 * i, 128 * i + 128)
        for j in range(2):
            start = prior_ref[j, starts[j], :, at]
            for row in range(4 * j, 4 * j + 4):
                kx = jnp.take_along_axis(k[row], index, axis=1, mode="promise_in_bounds")
                qx = jnp.take_along_axis(q[row], index, axis=1, mode="promise_in_bounds")
                kept[row, :, at] = kx
                ks[row] = kx * start if i == 0 else ks[row] + kx * start
                qs[row] = qx * start if i == 0 else qs[row] + qx * start

    def fold(values):
        return values + pltpu.roll(values, 64, 1)

    ks = [fold(values) for values in ks]
    qs = [fold(values) for values in qs]
    w, o = [None] * 8, [None] * 8
    for j in range(2):
        base = 4 * j
        grown = None
        for t in range(4):
            row = base + t
            carried = ks[row] if t == 0 else grown * ks[row]
            for e in range(t):
                reach = half_sum(k[row] * k[base + e])
                for m in range(e + 1, t):
                    reach = reach * a[base + m]
                carried = carried + reach * w[base + e]
            w[row] = b[row] * (v[row] - a[row] * carried)
            grown = a[row] if t == 0 else grown * a[row]
            out = grown * qs[row] + half_sum(q[row] * k[row]) * w[row]
            for e in range(t):
                reach = half_sum(q[row] * k[base + e])
                for m in range(e + 1, t + 1):
                    reach = reach * a[base + m]
                out = out + reach * w[base + e]
            o[row] = out

    copies = []
    for j in range(2):
        for i in range(32):
            at = slice(128 * i, 128 * i + 128)
            state = prior_ref[j, starts[j], :, at]
            for t in range(4):
                row = 4 * j + t
                state = a[row] * state + kept[row, :, at] * w[row]
                states_ref[j, t, :, at] = state
        copies.append(pltpu.make_async_copy(states_ref.at[j], out_ref.at[j], sems.at[j]))
        copies[-1].start()

    for row in ROWS:
        mean = half_sum(o[row] * o[row]) / 64
        n = o[row] * lax.rsqrt(mean + epsilon) * gain
        for p in range(4):
            nrows[row : row + 1, 128 * p : 128 * p + 128] = jnp.sum(
                jnp.where(masks[p], n, 0.0), axis=0, keepdims=True
            )
    rows = nrows[...]
    rows_ref[...] = jnp.concatenate([rows] * 8, axis=0).astype(bf16)
    for copy in copies:
        copy.wait()


def mix_kernel(x_ref, rows_ref, out_ref):
    w = x_ref[:, :, WO:QKV].reshape(256, 512)
    rows = rows_ref[...]
    out = dot(w, jnp.concatenate([rows, rows], axis=0), 1, 1)
    low = iota((16, 128), 1) < 64
    for r in range(8):
        piece = jnp.where(low, out[32 * r : 32 * r + 16], out[32 * r + 16 : 32 * r + 32])
        out_ref[2 * r] = piece.astype(bf16)
        out_ref[2 * r + 1] = piece.astype(bf16)


def place_kernel(x_ref, back_ref, out_ref):
    low = iota((16, 128), 1) < 64
    sums = [x_ref[2 * r].astype(f32) + x_ref[2 * r + 1].astype(f32) for r in range(8)]
    tiles = []
    for p in range(4):
        a, b = sums[2 * p], sums[2 * p + 1]
        top = jnp.where(low, a, pltpu.roll(b, 64, 1))
        end = jnp.where(low, pltpu.roll(a, 64, 1), b)
        tiles.append(jnp.concatenate([top, end], axis=0).astype(bf16))
    whole = dot(jnp.concatenate(tiles, axis=1), back_ref[...], 1, 0).astype(bf16)
    for t in range(4):
        out_ref[t] = whole[:, 128 * t : 128 * t + 128]


def back_table():
    dest = np.arange(512)
    group, rho = dest // 64, dest % 64
    wanted = (rho % 4) * 128 + (rho // 8) * 16 + group * 2 + (rho % 8) // 4
    return (wanted[:, None] == np.arange(512)[None, :]).astype(jnp.bfloat16)


def call(kernel, shapes, args, specs=None, scratch=(), outs=VMEM, name=None):
    if name == "pack":
        args = [pltpu.with_memory_space_constraint(a, pltpu.HBM) for a in args]
    return pl.pallas_call(
        kernel,
        out_shape=shapes,
        in_specs=specs or [VMEM] * len(args),
        out_specs=outs,
        scratch_shapes=scratch,
        compiler_params=pltpu.CompilerParams(vmem_limit_bytes=16 << 20),
        name=name,
    )(*args)


def shape(dims, dtype):
    return jax.ShapeDtypeStruct(dims, dtype)


def per_device(
    tokens,
    input_norm_gain,
    query_projection,
    key_projection,
    value_projection,
    write_strength_weight,
    decay_projection,
    head_decay_rate,
    token_extra_decay,
    accepted,
    prior_step_states,
    output_norm_gain,
    output_projection,
):
    def swap(x, axes):
        return lax.all_to_all(x, axes, 0, 0, tiled=True)

    packed = call(
        pack_kernel,
        shape((8, 32, WIDE), bf16),
        (
            jnp.transpose(tokens, (1, 2, 0)),
            input_norm_gain[None, :],
            query_projection,
            key_projection,
            value_projection,
            write_strength_weight.T,
            decay_projection.T,
            output_projection.T,
        ),
        specs=[HBM] * 8,
        scratch=[
            pltpu.VMEM((4, 32, 128), bf16),
            pltpu.VMEM((1, 32), f32),
            pltpu.VMEM((32, 512), bf16),
            pltpu.VMEM((32, 512), bf16),
            pltpu.VMEM((32, 512), bf16),
            pltpu.VMEM((8, 32), bf16),
            pltpu.VMEM((8, 32), bf16),
            pltpu.VMEM((32, 512), bf16),
            pltpu.SemaphoreType.DMA((8,)),
        ],
        name="pack",
    )
    near = swap(packed, NEAR)
    part = call(project_kernel, shape((64, WIDE - QKV), bf16), (near,), name="project")
    arrived = swap(part.reshape(8, 8, part.shape[1]), "z8").reshape(part.shape)
    states, rows = call(
        delta_kernel,
        (shape(prior_step_states.shape, f32), shape((64, 512), bf16)),
        (
            accepted,
            arrived,
            prior_step_states,
            head_decay_rate[None, :],
            token_extra_decay,
            output_norm_gain[None, :],
        ),
        specs=[SMEM] + [VMEM] * 5,
        scratch=[
            pltpu.VMEM((8, 128), f32),
            pltpu.VMEM((8, 512), f32),
            pltpu.VMEM((2, 4, 8, 4096), f32),
            pltpu.VMEM((8, 8, 4096), f32),
            pltpu.SemaphoreType.DMA((2,)),
        ],
        outs=(HBM, VMEM),
        name="delta",
    )
    all_rows = swap(rows.reshape(8, 8, 512), "z8").reshape(64, 512)
    columns = call(mix_kernel, shape((16, 16, 128), bf16), (near, all_rows), name="mix")
    back = swap(columns, ("zp", "y", "tp"))
    mixed = call(
        place_kernel, shape((4, 32, 128), bf16), (back, jnp.asarray(back_table())), name="place"
    )
    return (jnp.transpose(mixed, (2, 0, 1)), states)


def solution(mesh):
    split = Mesh(
        mesh.devices.reshape(mesh.shape["dp"], 8, 2, 4, mesh.shape["tp"]),
        ("dp", "z8", "zp", "y", "tp"),
    )
    in_specs = (
        P("dp", None, KV),
        P(KV),
        P(KV, "tp"),
        P(KV, "tp"),
        P(KV, "tp"),
        P(KV, "tp"),
        P(KV, "tp"),
        P("tp"),
        P(DP_KV, None, "tp"),
        P(DP_KV),
        P(DP_KV, None, "tp", None),
        P(),
        P("tp", KV),
    )
    out_specs = (P("dp", None, KV), P(DP_KV, None, "tp", None))
    return jax.shard_map(
        per_device, mesh=split, in_specs=in_specs, out_specs=out_specs, check_vma=False
    )
```

```python
import jax
import jax.numpy as jnp
import numpy as np
from jax import lax
from jax.experimental import pallas as pl
from jax.experimental.pallas import tpu as pltpu
from jax.sharding import Mesh
from jax.sharding import PartitionSpec as P

D = 2048
epsilon = 1e-06
KV = ("z8", "zp", "y")
DP_KV = ("dp", "z8", "zp", "y")
NEAR = ("zp", "y")
f32 = jnp.float32
bf16 = jnp.bfloat16

WO, QKV, SMALL, WIDE = 0, 512, 2048, 2176
VMEM = pl.BlockSpec(memory_space=pltpu.VMEM)
SMEM = pl.BlockSpec(memory_space=pltpu.SMEM)
HBM = pl.BlockSpec(memory_space=pltpu.HBM)


def iota(shape, dim):
    return lax.broadcasted_iota(jnp.int32, shape, dim)


def dot(a, b, ca, cb):
    return lax.dot_general(a, b, (((ca,), (cb,)), ((), ())), preferred_element_type=f32)


def pack_kernel(*refs):
    hbm, out_ref, held, sems = refs[:8], refs[8], refs[9:17], refs[17]
    copies = [pltpu.make_async_copy(hbm[n], held[n], sems.at[n]) for n in range(8)]
    for copy in copies:
        copy.start()
    tok_ref, gain_ref, q_ref, k_ref, v_ref, beta_ref, decay_ref, wo_ref = held
    source, dest = iota((512, 512), 0), iota((1, 512), 1)
    group, rho = dest // 64, dest % 64
    wanted = (rho % 4) * 128 + (rho // 8) * 16 + group * 2 + (rho % 8) // 4
    pick = (source == wanted).astype(f32).astype(bf16)
    eye = iota((32, 32), 0) == iota((32, 32), 1)
    head, lane = iota((8, 128), 0), iota((8, 128), 1)
    put_beta = ((lane == head) | (lane == head + 16)).astype(f32).astype(bf16)
    put_decay = ((lane == head + 8) | (lane == head + 24)).astype(f32).astype(bf16)
    copies[0].wait()
    copies[1].wait()
    gain = jnp.sum(jnp.where(eye, gain_ref[...], 0.0), axis=1, keepdims=True)
    raw = jnp.concatenate([tok_ref[t] for t in range(4)], axis=1).astype(f32)
    scaled = raw * gain
    squares = jnp.sum(raw * raw, axis=0, keepdims=True)
    high = squares.astype(bf16).astype(f32)
    sub = iota((16, 512), 0)
    extra = jnp.where(sub < 2, high, jnp.where(sub < 4, squares - high, 0.0))
    moved = dot(jnp.concatenate([scaled, extra], axis=0).astype(bf16), pick, 1, 0)
    copies[5].wait()
    copies[6].wait()
    small = dot(beta_ref[...], put_beta, 0, 0) + dot(decay_ref[...], put_decay, 0, 0)
    lane = iota((8, 128), 1)
    even = iota((8, 128), 0) % 2 == 0
    for n in (2, 3, 4, 7):
        copies[n].wait()
    for r in range(8):
        at = slice(128 * (r // 2), 128 * (r // 2) + 128)
        sums = moved[32:40, at]
        if r % 2 == 0:
            cols = pltpu.roll(moved[:32, at], 64, 1)
            sums = jnp.where(even, pltpu.roll(sums, 32, 1), sums)
        else:
            cols = moved[:32, at]
            sums = jnp.where(even, pltpu.roll(sums, 96, 1), pltpu.roll(sums, 64, 1))
        groups = []
        for g in range(4):
            right = jnp.where(lane < 64, sums if g == 0 else 0.0, cols[8 * g : 8 * g + 8])
            groups.append(jnp.where(lane < 32, small[8 * g : 8 * g + 8], right))
        tile = jnp.concatenate(groups, axis=0)
        out_ref[r, :, WO:QKV] = wo_ref[...]
        out_ref[r, :, QKV : QKV + 512] = q_ref[...]
        out_ref[r, :, QKV + 512 : QKV + 1024] = k_ref[...]
        out_ref[r, :, QKV + 1024 : SMALL] = v_ref[...]
        out_ref[r, :, SMALL:] = tile.astype(bf16)


def project_kernel(x_ref, out_ref):
    x = x_ref[...].reshape(256, WIDE)
    cols = x[:, SMALL:]
    main = dot(cols, x[:, QKV:SMALL], 0, 0)
    out_ref[:, : SMALL - QKV] = main[64:].astype(bf16)
    sums = jnp.zeros((8, 128), f32)
    for r in range(8):
        sums = sums + cols[32 * r : 32 * r + 16].astype(f32)[0:8]
    sub, lane = iota((32, 128), 0), iota((32, 128), 1)
    halves = []
    for n in range(2):
        row = sums[n : n + 1] + sums[n + 2 : n + 3]
        halves.append(jnp.sum(jnp.where(lane == sub + 32, row, 0.0), axis=1, keepdims=True))
    total = jnp.concatenate(halves, axis=0)
    lane = iota((64, 128), 1)
    tail = jnp.where(lane < 32, dot(cols, cols, 0, 0)[64:], jnp.where(lane < 34, total, 0.0))
    first = tail.astype(bf16).astype(f32)
    keep = (lane < 16) | (lane == 32)
    out_ref[:, SMALL - QKV :] = jnp.where(keep, first, tail - first).astype(bf16)


def delta_kernel(
    accepted_ref, c_ref, prior_ref, rate_ref, extra_ref, gain_ref, states_ref, rows_ref,
    aux, nrows, kept
):
    c = c_ref[...].astype(f32)
    s = (c[0:8] + c[8:16]) + (c[16:24] + c[24:32])
    s = s + ((c[32:40] + c[40:48]) + (c[48:56] + c[56:64]))
    tile = s[:, 1536:]
    total = tile[:, 32:33] + tile[:, 33:34]
    inverse = lax.rsqrt(total / D + epsilon)
    logits = jnp.transpose((tile + pltpu.roll(tile, 112, 1)) * inverse)
    aux[...] = jnp.zeros((8, 128), f32)
    aux[0:4, 0:8] = extra_ref[0]
    aux[4:8, 0:8] = extra_ref[1]
    aux[:, 8:16] = jnp.broadcast_to(rate_ref[...], (8, 8))
    side = jnp.transpose(aux[...])
    beta = jax.nn.sigmoid(logits[0:8])
    fade = jnp.exp(-side[8:16] * jax.nn.softplus(logits[8:16]) + side[0:8])

    sub, lane = iota((8, 128), 0), iota((8, 128), 1)
    masks = [sub == 2 * p + lane // 64 for p in range(4)]
    gain = jnp.concatenate([gain_ref[...], gain_ref[...]], axis=1)

    def silu_of(at):
        u = s[:, at : at + 512] * inverse
        return u / (1.0 + jnp.exp(-u))

    parts = [silu_of(0), silu_of(512), silu_of(1024)]

    def by_heads(values, row):
        m = jnp.zeros((8, 128), f32)
        for p in range(4):
            piece = jnp.broadcast_to(values[row : row + 1, 128 * p : 128 * p + 128], (8, 128))
            m = jnp.where(masks[p], piece, m)
        return m + pltpu.roll(m, 64, 1)

    def half_sum(values):
        return 0.5 * jnp.sum(values, axis=1, keepdims=True)

    def unit(values):
        return values * lax.rsqrt(half_sum(values * values) + epsilon)

    ROWS = range(8)
    q = [unit(by_heads(parts[0], row)) * 0.125 for row in ROWS]
    k = [unit(by_heads(parts[1], row)) for row in ROWS]
    v = [by_heads(parts[2], row) for row in ROWS]
    a = [jnp.broadcast_to(fade[:, row : row + 1], (8, 128)) for row in ROWS]
    b = [jnp.broadcast_to(beta[:, row : row + 1], (8, 128)) for row in ROWS]

    starts = [accepted_ref[0] - 1, accepted_ref[1] - 1]
    ks, qs = [None] * 8, [None] * 8
    for i in range(32):
        index = lane // 64 + 2 * i
        at = slice(128 * i, 128 * i + 128)
        for j in range(2):
            start = prior_ref[j, starts[j], :, at]
            for row in range(4 * j, 4 * j + 4):
                kx = jnp.take_along_axis(k[row], index, axis=1, mode="promise_in_bounds")
                qx = jnp.take_along_axis(q[row], index, axis=1, mode="promise_in_bounds")
                kept[row, :, at] = kx
                ks[row] = kx * start if i == 0 else ks[row] + kx * start
                qs[row] = qx * start if i == 0 else qs[row] + qx * start

    def fold(values):
        return values + pltpu.roll(values, 64, 1)

    ks = [fold(values) for values in ks]
    qs = [fold(values) for values in qs]
    w, o = [None] * 8, [None] * 8
    for j in range(2):
        base = 4 * j
        grown = None
        for t in range(4):
            row = base + t
            carried = ks[row] if t == 0 else grown * ks[row]
            for e in range(t):
                reach = half_sum(k[row] * k[base + e])
                for m in range(e + 1, t):
                    reach = reach * a[base + m]
                carried = carried + reach * w[base + e]
            w[row] = b[row] * (v[row] - a[row] * carried)
            grown = a[row] if t == 0 else grown * a[row]
            out = grown * qs[row] + half_sum(q[row] * k[row]) * w[row]
            for e in range(t):
                reach = half_sum(q[row] * k[base + e])
                for m in range(e + 1, t + 1):
                    reach = reach * a[base + m]
                out = out + reach * w[base + e]
            o[row] = out

    for j in range(2):
        for i in range(32):
            at = slice(128 * i, 128 * i + 128)
            state = prior_ref[j, starts[j], :, at]
            for t in range(4):
                row = 4 * j + t
                state = a[row] * state + kept[row, :, at] * w[row]
                states_ref[j, t, :, at] = state

    for row in ROWS:
        mean = half_sum(o[row] * o[row]) / 64
        n = o[row] * lax.rsqrt(mean + epsilon) * gain
        for p in range(4):
            nrows[row : row + 1, 128 * p : 128 * p + 128] = jnp.sum(
                jnp.where(masks[p], n, 0.0), axis=0, keepdims=True
            )
    rows = nrows[...]
    rows_ref[...] = jnp.concatenate([rows] * 8, axis=0).astype(bf16)


def mix_kernel(x_ref, rows_ref, out_ref):
    w = x_ref[:, :, WO:QKV].reshape(256, 512)
    rows = rows_ref[...]
    out = dot(w, jnp.concatenate([rows, rows], axis=0), 1, 1)
    low = iota((16, 128), 1) < 64
    for r in range(8):
        piece = jnp.where(low, out[32 * r : 32 * r + 16], out[32 * r + 16 : 32 * r + 32])
        out_ref[2 * r] = piece.astype(bf16)
        out_ref[2 * r + 1] = piece.astype(bf16)


def place_kernel(x_ref, back_ref, states_ref, out_ref, kept_ref, sem):
    copy = pltpu.make_async_copy(states_ref, kept_ref, sem)
    copy.start()
    low = iota((16, 128), 1) < 64
    sums = [x_ref[2 * r].astype(f32) + x_ref[2 * r + 1].astype(f32) for r in range(8)]
    tiles = []
    for p in range(4):
        a, b = sums[2 * p], sums[2 * p + 1]
        top = jnp.where(low, a, pltpu.roll(b, 64, 1))
        end = jnp.where(low, pltpu.roll(a, 64, 1), b)
        tiles.append(jnp.concatenate([top, end], axis=0).astype(bf16))
    whole = dot(jnp.concatenate(tiles, axis=1), back_ref[...], 1, 0).astype(bf16)
    for t in range(4):
        out_ref[t] = whole[:, 128 * t : 128 * t + 128]
    copy.wait()


def back_table():
    dest = np.arange(512)
    group, rho = dest // 64, dest % 64
    wanted = (rho % 4) * 128 + (rho // 8) * 16 + group * 2 + (rho % 8) // 4
    return (wanted[:, None] == np.arange(512)[None, :]).astype(jnp.bfloat16)


def call(kernel, shapes, args, specs=None, scratch=(), outs=VMEM, name=None):
    if name == "pack":
        args = [pltpu.with_memory_space_constraint(a, pltpu.HBM) for a in args]
    return pl.pallas_call(
        kernel,
        out_shape=shapes,
        in_specs=specs or [VMEM] * len(args),
        out_specs=outs,
        scratch_shapes=scratch,
        compiler_params=pltpu.CompilerParams(vmem_limit_bytes=16 << 20),
        name=name,
    )(*args)


def shape(dims, dtype):
    return jax.ShapeDtypeStruct(dims, dtype)


def per_device(
    tokens,
    input_norm_gain,
    query_projection,
    key_projection,
    value_projection,
    write_strength_weight,
    decay_projection,
    head_decay_rate,
    token_extra_decay,
    accepted,
    prior_step_states,
    output_norm_gain,
    output_projection,
):
    def swap(x, axes):
        return lax.all_to_all(x, axes, 0, 0, tiled=True)

    packed = call(
        pack_kernel,
        shape((8, 32, WIDE), bf16),
        (
            jnp.transpose(tokens, (1, 2, 0)),
            input_norm_gain[None, :],
            query_projection,
            key_projection,
            value_projection,
            write_strength_weight.T,
            decay_projection.T,
            output_projection.T,
        ),
        specs=[HBM] * 8,
        scratch=[
            pltpu.VMEM((4, 32, 128), bf16),
            pltpu.VMEM((1, 32), f32),
            pltpu.VMEM((32, 512), bf16),
            pltpu.VMEM((32, 512), bf16),
            pltpu.VMEM((32, 512), bf16),
            pltpu.VMEM((8, 32), bf16),
            pltpu.VMEM((8, 32), bf16),
            pltpu.VMEM((32, 512), bf16),
            pltpu.SemaphoreType.DMA((8,)),
        ],
        name="pack",
    )
    near = swap(packed, NEAR)
    part = call(project_kernel, shape((64, WIDE - QKV), bf16), (near,), name="project")
    arrived = swap(part.reshape(8, 8, part.shape[1]), "z8").reshape(part.shape)
    states, rows = call(
        delta_kernel,
        (shape(prior_step_states.shape, f32), shape((64, 512), bf16)),
        (
            accepted,
            arrived,
            prior_step_states,
            head_decay_rate[None, :],
            token_extra_decay,
            output_norm_gain[None, :],
        ),
        specs=[SMEM] + [VMEM] * 5,
        scratch=[
            pltpu.VMEM((8, 128), f32),
            pltpu.VMEM((8, 512), f32),
            pltpu.VMEM((8, 8, 4096), f32),
        ],
        outs=(VMEM, VMEM),
        name="delta",
    )
    all_rows = swap(rows.reshape(8, 8, 512), "z8").reshape(64, 512)
    columns = call(mix_kernel, shape((16, 16, 128), bf16), (near, all_rows), name="mix")
    back = swap(columns, ("zp", "y", "tp"))
    mixed, kept = call(
        place_kernel,
        (shape((4, 32, 128), bf16), shape(states.shape, f32)),
        (back, jnp.asarray(back_table()), states),
        scratch=[pltpu.SemaphoreType.DMA],
        outs=(VMEM, HBM),
        name="place",
    )
    return (jnp.transpose(mixed, (2, 0, 1)), kept)


def solution(mesh):
    split = Mesh(
        mesh.devices.reshape(mesh.shape["dp"], 8, 2, 4, mesh.shape["tp"]),
        ("dp", "z8", "zp", "y", "tp"),
    )
    in_specs = (
        P("dp", None, KV),
        P(KV),
        P(KV, "tp"),
        P(KV, "tp"),
        P(KV, "tp"),
        P(KV, "tp"),
        P(KV, "tp"),
        P("tp"),
        P(DP_KV, None, "tp"),
        P(DP_KV),
        P(DP_KV, None, "tp", None),
        P(),
        P("tp", KV),
    )
    out_specs = (P("dp", None, KV), P(DP_KV, None, "tp", None))
    return jax.shard_map(
        per_device, mesh=split, in_specs=in_specs, out_specs=out_specs, check_vma=False
    )
```

```python
import jax
import jax.numpy as jnp
import numpy as np
from jax import lax
from jax.experimental import pallas as pl
from jax.experimental.pallas import tpu as pltpu
from jax.sharding import Mesh
from jax.sharding import PartitionSpec as P

D = 2048
epsilon = 1e-06
KV = ("z8", "zp", "y")
DP_KV = ("dp", "z8", "zp", "y")
NEAR = ("zp", "y")
f32 = jnp.float32
bf16 = jnp.bfloat16

WO, QKV, SMALL, WIDE = 0, 512, 2048, 2176
VMEM = pl.BlockSpec(memory_space=pltpu.VMEM)
SMEM = pl.BlockSpec(memory_space=pltpu.SMEM)
HBM = pl.BlockSpec(memory_space=pltpu.HBM)


def iota(shape, dim):
    return lax.broadcasted_iota(jnp.int32, shape, dim)


def dot(a, b, ca, cb):
    return lax.dot_general(a, b, (((ca,), (cb,)), ((), ())), preferred_element_type=f32)


def pack_kernel(*refs):
    hbm, out_ref, held, sems = refs[:8], refs[8], refs[9:17], refs[17]
    copies = [pltpu.make_async_copy(hbm[n], held[n], sems.at[n]) for n in range(8)]
    for copy in copies:
        copy.start()
    tok_ref, gain_ref, q_ref, k_ref, v_ref, beta_ref, decay_ref, wo_ref = held
    source, dest = iota((512, 512), 0), iota((1, 512), 1)
    group, rho = dest // 64, dest % 64
    wanted = (rho % 4) * 128 + (rho // 8) * 16 + group * 2 + (rho % 8) // 4
    pick = (source == wanted).astype(f32).astype(bf16)
    eye = iota((32, 32), 0) == iota((32, 32), 1)
    head, lane = iota((8, 128), 0), iota((8, 128), 1)
    put_beta = ((lane == head) | (lane == head + 16)).astype(f32).astype(bf16)
    put_decay = ((lane == head + 8) | (lane == head + 24)).astype(f32).astype(bf16)
    for copy in copies:
        copy.wait()
    gain = jnp.sum(jnp.where(eye, gain_ref[...], 0.0), axis=1, keepdims=True)
    raw = jnp.concatenate([tok_ref[t] for t in range(4)], axis=1).astype(f32)
    scaled = raw * gain
    squares = jnp.sum(raw * raw, axis=0, keepdims=True)
    high = squares.astype(bf16).astype(f32)
    sub = iota((16, 512), 0)
    extra = jnp.where(sub < 2, high, jnp.where(sub < 4, squares - high, 0.0))
    moved = dot(jnp.concatenate([scaled, extra], axis=0).astype(bf16), pick, 1, 0)
    small = dot(beta_ref[...], put_beta, 0, 0) + dot(decay_ref[...], put_decay, 0, 0)
    lane = iota((8, 128), 1)
    even = iota((8, 128), 0) % 2 == 0
    for r in range(8):
        at = slice(128 * (r // 2), 128 * (r // 2) + 128)
        sums = moved[32:40, at]
        if r % 2 == 0:
            cols = pltpu.roll(moved[:32, at], 64, 1)
            sums = jnp.where(even, pltpu.roll(sums, 32, 1), sums)
        else:
            cols = moved[:32, at]
            sums = jnp.where(even, pltpu.roll(sums, 96, 1), pltpu.roll(sums, 64, 1))
        groups = []
        for g in range(4):
            right = jnp.where(lane < 64, sums if g == 0 else 0.0, cols[8 * g : 8 * g + 8])
            groups.append(jnp.where(lane < 32, small[8 * g : 8 * g + 8], right))
        tile = jnp.concatenate(groups, axis=0)
        out_ref[r, :, WO:QKV] = wo_ref[...]
        out_ref[r, :, QKV : QKV + 512] = q_ref[...]
        out_ref[r, :, QKV + 512 : QKV + 1024] = k_ref[...]
        out_ref[r, :, QKV + 1024 : SMALL] = v_ref[...]
        out_ref[r, :, SMALL:] = tile.astype(bf16)


def project_kernel(x_ref, out_ref):
    x = x_ref[...].reshape(256, WIDE)
    cols = x[:, SMALL:]
    main = dot(cols, x[:, QKV:SMALL], 0, 0)
    out_ref[:, : SMALL - QKV] = main[64:].astype(bf16)
    sums = jnp.zeros((8, 128), f32)
    for r in range(8):
        sums = sums + cols[32 * r : 32 * r + 16].astype(f32)[0:8]
    sub, lane = iota((32, 128), 0), iota((32, 128), 1)
    halves = []
    for n in range(2):
        row = sums[n : n + 1] + sums[n + 2 : n + 3]
        halves.append(jnp.sum(jnp.where(lane == sub + 32, row, 0.0), axis=1, keepdims=True))
    total = jnp.concatenate(halves, axis=0)
    lane = iota((64, 128), 1)
    tail = jnp.where(lane < 32, dot(cols, cols, 0, 0)[64:], jnp.where(lane < 34, total, 0.0))
    first = tail.astype(bf16).astype(f32)
    keep = (lane < 16) | (lane == 32)
    out_ref[:, SMALL - QKV :] = jnp.where(keep, first, tail - first).astype(bf16)


def delta_kernel(
    accepted_ref, c_ref, prior_ref, rate_ref, extra_ref, gain_ref, states_ref, rows_ref,
    aux, nrows, kept
):
    c = c_ref[...].astype(f32)
    s = (c[0:8] + c[8:16]) + (c[16:24] + c[24:32])
    s = s + ((c[32:40] + c[40:48]) + (c[48:56] + c[56:64]))
    tile = s[:, 1536:]
    total = tile[:, 32:33] + tile[:, 33:34]
    inverse = lax.rsqrt(total / D + epsilon)
    logits = jnp.transpose((tile + pltpu.roll(tile, 112, 1)) * inverse)
    aux[...] = jnp.zeros((8, 128), f32)
    aux[0:4, 0:8] = extra_ref[0]
    aux[4:8, 0:8] = extra_ref[1]
    aux[:, 8:16] = jnp.broadcast_to(rate_ref[...], (8, 8))
    side = jnp.transpose(aux[...])
    beta = jax.nn.sigmoid(logits[0:8])
    fade = jnp.exp(-side[8:16] * jax.nn.softplus(logits[8:16]) + side[0:8])

    sub, lane = iota((8, 128), 0), iota((8, 128), 1)
    masks = [sub == 2 * p + lane // 64 for p in range(4)]
    gain = jnp.concatenate([gain_ref[...], gain_ref[...]], axis=1)

    def silu_of(at):
        u = s[:, at : at + 512] * inverse
        return u / (1.0 + jnp.exp(-u))

    parts = [silu_of(0), silu_of(512), silu_of(1024)]

    def by_heads(values, row):
        m = jnp.zeros((8, 128), f32)
        for p in range(4):
            piece = jnp.broadcast_to(values[row : row + 1, 128 * p : 128 * p + 128], (8, 128))
            m = jnp.where(masks[p], piece, m)
        return m + pltpu.roll(m, 64, 1)

    def half_sum(values):
        return 0.5 * jnp.sum(values, axis=1, keepdims=True)

    def unit(values):
        return values * lax.rsqrt(half_sum(values * values) + epsilon)

    ROWS = range(8)
    q = [unit(by_heads(parts[0], row)) * 0.125 for row in ROWS]
    k = [unit(by_heads(parts[1], row)) for row in ROWS]
    v = [by_heads(parts[2], row) for row in ROWS]
    a = [jnp.broadcast_to(fade[:, row : row + 1], (8, 128)) for row in ROWS]
    b = [jnp.broadcast_to(beta[:, row : row + 1], (8, 128)) for row in ROWS]

    starts = [accepted_ref[0] - 1, accepted_ref[1] - 1]
    ks, qs = [None] * 8, [None] * 8
    for i in range(32):
        index = lane // 64 + 2 * i
        at = slice(128 * i, 128 * i + 128)
        for j in range(2):
            start = prior_ref[j, starts[j], :, at]
            for row in range(4 * j, 4 * j + 4):
                kx = jnp.take_along_axis(k[row], index, axis=1, mode="promise_in_bounds")
                qx = jnp.take_along_axis(q[row], index, axis=1, mode="promise_in_bounds")
                kept[row, :, at] = kx
                ks[row] = kx * start if i == 0 else ks[row] + kx * start
                qs[row] = qx * start if i == 0 else qs[row] + qx * start

    def fold(values):
        return values + pltpu.roll(values, 64, 1)

    ks = [fold(values) for values in ks]
    qs = [fold(values) for values in qs]
    w, o = [None] * 8, [None] * 8
    for j in range(2):
        base = 4 * j
        grown = None
        for t in range(4):
            row = base + t
            carried = ks[row] if t == 0 else grown * ks[row]
            for e in range(t):
                reach = half_sum(k[row] * k[base + e])
                for m in range(e + 1, t):
                    reach = reach * a[base + m]
                carried = carried + reach * w[base + e]
            w[row] = b[row] * (v[row] - a[row] * carried)
            grown = a[row] if t == 0 else grown * a[row]
            out = grown * qs[row] + half_sum(q[row] * k[row]) * w[row]
            for e in range(t):
                reach = half_sum(q[row] * k[base + e])
                for m in range(e + 1, t + 1):
                    reach = reach * a[base + m]
                out = out + reach * w[base + e]
            o[row] = out

    for j in range(2):
        for i in range(32):
            at = slice(128 * i, 128 * i + 128)
            state = prior_ref[j, starts[j], :, at]
            for t in range(4):
                row = 4 * j + t
                state = a[row] * state + kept[row, :, at] * w[row]
                states_ref[j, t, :, at] = state

    for row in ROWS:
        mean = half_sum(o[row] * o[row]) / 64
        n = o[row] * lax.rsqrt(mean + epsilon) * gain
        for p in range(4):
            nrows[row : row + 1, 128 * p : 128 * p + 128] = jnp.sum(
                jnp.where(masks[p], n, 0.0), axis=0, keepdims=True
            )
    rows = nrows[...]
    rows_ref[...] = jnp.concatenate([rows] * 8, axis=0).astype(bf16)


def mix_kernel(x_ref, rows_ref, out_ref):
    w = x_ref[:, :, WO:QKV].reshape(256, 512)
    rows = rows_ref[...]
    out = dot(w, jnp.concatenate([rows, rows], axis=0), 1, 1)
    low = iota((16, 128), 1) < 64
    for r in range(8):
        piece = jnp.where(low, out[32 * r : 32 * r + 16], out[32 * r + 16 : 32 * r + 32])
        out_ref[2 * r] = piece.astype(bf16)
        out_ref[2 * r + 1] = piece.astype(bf16)


def place_kernel(x_ref, back_ref, states_ref, out_ref, kept_ref, sem):
    copies = [
        pltpu.make_async_copy(states_ref.at[n // 4, n % 4], kept_ref.at[n // 4, n % 4], sem.at[n])
        for n in range(8)
    ]
    for copy in copies:
        copy.start()
    low = iota((16, 128), 1) < 64
    sums = [x_ref[2 * r].astype(f32) + x_ref[2 * r + 1].astype(f32) for r in range(8)]
    tiles = []
    for p in range(4):
        a, b = sums[2 * p], sums[2 * p + 1]
        top = jnp.where(low, a, pltpu.roll(b, 64, 1))
        end = jnp.where(low, pltpu.roll(a, 64, 1), b)
        tiles.append(jnp.concatenate([top, end], axis=0).astype(bf16))
    whole = dot(jnp.concatenate(tiles, axis=1), back_ref[...], 1, 0).astype(bf16)
    for t in range(4):
        out_ref[t] = whole[:, 128 * t : 128 * t + 128]
    for copy in copies:
        copy.wait()


def back_table():
    dest = np.arange(512)
    group, rho = dest // 64, dest % 64
    wanted = (rho % 4) * 128 + (rho // 8) * 16 + group * 2 + (rho % 8) // 4
    return (wanted[:, None] == np.arange(512)[None, :]).astype(jnp.bfloat16)


def call(kernel, shapes, args, specs=None, scratch=(), outs=VMEM, name=None):
    if name == "pack":
        args = [pltpu.with_memory_space_constraint(a, pltpu.HBM) for a in args]
    return pl.pallas_call(
        kernel,
        out_shape=shapes,
        in_specs=specs or [VMEM] * len(args),
        out_specs=outs,
        scratch_shapes=scratch,
        compiler_params=pltpu.CompilerParams(vmem_limit_bytes=16 << 20),
        name=name,
    )(*args)


def shape(dims, dtype):
    return jax.ShapeDtypeStruct(dims, dtype)


def per_device(
    tokens,
    input_norm_gain,
    query_projection,
    key_projection,
    value_projection,
    write_strength_weight,
    decay_projection,
    head_decay_rate,
    token_extra_decay,
    accepted,
    prior_step_states,
    output_norm_gain,
    output_projection,
):
    def swap(x, axes):
        return lax.all_to_all(x, axes, 0, 0, tiled=True)

    packed = call(
        pack_kernel,
        shape((8, 32, WIDE), bf16),
        (
            jnp.transpose(tokens, (1, 2, 0)),
            input_norm_gain[None, :],
            query_projection,
            key_projection,
            value_projection,
            write_strength_weight.T,
            decay_projection.T,
            output_projection.T,
        ),
        specs=[HBM] * 8,
        scratch=[
            pltpu.VMEM((4, 32, 128), bf16),
            pltpu.VMEM((1, 32), f32),
            pltpu.VMEM((32, 512), bf16),
            pltpu.VMEM((32, 512), bf16),
            pltpu.VMEM((32, 512), bf16),
            pltpu.VMEM((8, 32), bf16),
            pltpu.VMEM((8, 32), bf16),
            pltpu.VMEM((32, 512), bf16),
            pltpu.SemaphoreType.DMA((8,)),
        ],
        name="pack",
    )
    near = swap(packed, NEAR)
    part = call(project_kernel, shape((64, WIDE - QKV), bf16), (near,), name="project")
    arrived = swap(part.reshape(8, 8, part.shape[1]), "z8").reshape(part.shape)
    states, rows = call(
        delta_kernel,
        (shape(prior_step_states.shape, f32), shape((64, 512), bf16)),
        (
            accepted,
            arrived,
            prior_step_states,
            head_decay_rate[None, :],
            token_extra_decay,
            output_norm_gain[None, :],
        ),
        specs=[SMEM] + [VMEM] * 5,
        scratch=[
            pltpu.VMEM((8, 128), f32),
            pltpu.VMEM((8, 512), f32),
            pltpu.VMEM((8, 8, 4096), f32),
        ],
        outs=(VMEM, VMEM),
        name="delta",
    )
    all_rows = swap(rows.reshape(8, 8, 512), "z8").reshape(64, 512)
    columns = call(mix_kernel, shape((16, 16, 128), bf16), (near, all_rows), name="mix")
    back = swap(columns, ("zp", "y", "tp"))
    mixed, kept = call(
        place_kernel,
        (shape((4, 32, 128), bf16), shape(states.shape, f32)),
        (back, jnp.asarray(back_table()), states),
        scratch=[pltpu.SemaphoreType.DMA((8,))],
        outs=(VMEM, HBM),
        name="place",
    )
    return (jnp.transpose(mixed, (2, 0, 1)), kept)


def solution(mesh):
    split = Mesh(
        mesh.devices.reshape(mesh.shape["dp"], 8, 2, 4, mesh.shape["tp"]),
        ("dp", "z8", "zp", "y", "tp"),
    )
    in_specs = (
        P("dp", None, KV),
        P(KV),
        P(KV, "tp"),
        P(KV, "tp"),
        P(KV, "tp"),
        P(KV, "tp"),
        P(KV, "tp"),
        P("tp"),
        P(DP_KV, None, "tp"),
        P(DP_KV),
        P(DP_KV, None, "tp", None),
        P(),
        P("tp", KV),
    )
    out_specs = (P("dp", None, KV), P(DP_KV, None, "tp", None))
    return jax.shard_map(
        per_device, mesh=split, in_specs=in_specs, out_specs=out_specs, check_vma=False
    )
```

```python
import jax
import jax.numpy as jnp
import numpy as np
from jax import lax
from jax.experimental import pallas as pl
from jax.experimental.pallas import tpu as pltpu
from jax.sharding import Mesh
from jax.sharding import PartitionSpec as P

D = 2048
epsilon = 1e-06
KV = ("z8", "zp", "y")
DP_KV = ("dp", "z8", "zp", "y")
NEAR = ("zp", "y")
f32 = jnp.float32
bf16 = jnp.bfloat16

WO, QKV, SMALL, WIDE = 0, 512, 2048, 2176
VMEM = pl.BlockSpec(memory_space=pltpu.VMEM)
SMEM = pl.BlockSpec(memory_space=pltpu.SMEM)
HBM = pl.BlockSpec(memory_space=pltpu.HBM)


def iota(shape, dim):
    return lax.broadcasted_iota(jnp.int32, shape, dim)


def dot(a, b, ca, cb):
    return lax.dot_general(a, b, (((ca,), (cb,)), ((), ())), preferred_element_type=f32)


def pack_kernel(*refs):
    hbm, out_ref, held, sems = refs[:8], refs[8], refs[9:17], refs[17]
    copies = [pltpu.make_async_copy(hbm[n], held[n], sems.at[n]) for n in range(8)]
    for copy in copies:
        copy.start()
    tok_ref, gain_ref, q_ref, k_ref, v_ref, beta_ref, decay_ref, wo_ref = held
    source, dest = iota((512, 512), 0), iota((1, 512), 1)
    group, rho = dest // 64, dest % 64
    wanted = (rho % 4) * 128 + (rho // 8) * 16 + group * 2 + (rho % 8) // 4
    pick = (source == wanted).astype(f32).astype(bf16)
    eye = iota((32, 32), 0) == iota((32, 32), 1)
    head, lane = iota((8, 128), 0), iota((8, 128), 1)
    put_beta = ((lane == head) | (lane == head + 16)).astype(f32).astype(bf16)
    put_decay = ((lane == head + 8) | (lane == head + 24)).astype(f32).astype(bf16)
    for copy in copies:
        copy.wait()
    gain = jnp.sum(jnp.where(eye, gain_ref[...], 0.0), axis=1, keepdims=True)
    raw = jnp.concatenate([tok_ref[t] for t in range(4)], axis=1).astype(f32)
    scaled = raw * gain
    squares = jnp.sum(raw * raw, axis=0, keepdims=True)
    high = squares.astype(bf16).astype(f32)
    sub = iota((16, 512), 0)
    extra = jnp.where(sub < 2, high, jnp.where(sub < 4, squares - high, 0.0))
    moved = dot(jnp.concatenate([scaled, extra], axis=0).astype(bf16), pick, 1, 0)
    small = dot(beta_ref[...], put_beta, 0, 0) + dot(decay_ref[...], put_decay, 0, 0)
    lane = iota((8, 128), 1)
    even = iota((8, 128), 0) % 2 == 0
    for r in range(8):
        at = slice(128 * (r // 2), 128 * (r // 2) + 128)
        sums = moved[32:40, at]
        if r % 2 == 0:
            cols = pltpu.roll(moved[:32, at], 64, 1)
            sums = jnp.where(even, pltpu.roll(sums, 32, 1), sums)
        else:
            cols = moved[:32, at]
            sums = jnp.where(even, pltpu.roll(sums, 96, 1), pltpu.roll(sums, 64, 1))
        groups = []
        for g in range(4):
            right = jnp.where(lane < 64, sums if g == 0 else 0.0, cols[8 * g : 8 * g + 8])
            groups.append(jnp.where(lane < 32, small[8 * g : 8 * g + 8], right))
        tile = jnp.concatenate(groups, axis=0)
        out_ref[r, :, WO:QKV] = wo_ref[...]
        out_ref[r, :, QKV : QKV + 512] = q_ref[...]
        out_ref[r, :, QKV + 512 : QKV + 1024] = k_ref[...]
        out_ref[r, :, QKV + 1024 : SMALL] = v_ref[...]
        out_ref[r, :, SMALL:] = tile.astype(bf16)


def project_kernel(x_ref, out_ref):
    x = x_ref[...].reshape(256, WIDE)
    cols = x[:, SMALL:]
    main = dot(cols, x[:, QKV:SMALL], 0, 0)
    out_ref[:, : SMALL - QKV] = main[64:].astype(bf16)
    sums = jnp.zeros((8, 128), f32)
    for r in range(8):
        sums = sums + cols[32 * r : 32 * r + 16].astype(f32)[0:8]
    sub, lane = iota((32, 128), 0), iota((32, 128), 1)
    halves = []
    for n in range(2):
        row = sums[n : n + 1] + sums[n + 2 : n + 3]
        halves.append(jnp.sum(jnp.where(lane == sub + 32, row, 0.0), axis=1, keepdims=True))
    total = jnp.concatenate(halves, axis=0)
    lane = iota((64, 128), 1)
    tail = jnp.where(lane < 32, dot(cols, cols, 0, 0)[64:], jnp.where(lane < 34, total, 0.0))
    first = tail.astype(bf16).astype(f32)
    keep = (lane < 16) | (lane == 32)
    out_ref[:, SMALL - QKV :] = jnp.where(keep, first, tail - first).astype(bf16)


def delta_kernel(
    accepted_ref, c_ref, prior_ref, rate_ref, extra_ref, gain_ref, out_ref, late_ref, rows_ref,
    aux, nrows, kept, begin, early_ref, sems
):
    c = c_ref[...].astype(f32)
    s = (c[0:8] + c[8:16]) + (c[16:24] + c[24:32])
    s = s + ((c[32:40] + c[40:48]) + (c[48:56] + c[56:64]))
    tile = s[:, 1536:]
    total = tile[:, 32:33] + tile[:, 33:34]
    inverse = lax.rsqrt(total / D + epsilon)
    logits = jnp.transpose((tile + pltpu.roll(tile, 112, 1)) * inverse)
    aux[...] = jnp.zeros((8, 128), f32)
    aux[0:4, 0:8] = extra_ref[0]
    aux[4:8, 0:8] = extra_ref[1]
    aux[:, 8:16] = jnp.broadcast_to(rate_ref[...], (8, 8))
    side = jnp.transpose(aux[...])
    beta = jax.nn.sigmoid(logits[0:8])
    fade = jnp.exp(-side[8:16] * jax.nn.softplus(logits[8:16]) + side[0:8])

    sub, lane = iota((8, 128), 0), iota((8, 128), 1)
    masks = [sub == 2 * p + lane // 64 for p in range(4)]
    gain = jnp.concatenate([gain_ref[...], gain_ref[...]], axis=1)

    def silu_of(at):
        u = s[:, at : at + 512] * inverse
        return u / (1.0 + jnp.exp(-u))

    parts = [silu_of(0), silu_of(512), silu_of(1024)]

    def by_heads(values, row):
        m = jnp.zeros((8, 128), f32)
        for p in range(4):
            piece = jnp.broadcast_to(values[row : row + 1, 128 * p : 128 * p + 128], (8, 128))
            m = jnp.where(masks[p], piece, m)
        return m + pltpu.roll(m, 64, 1)

    def half_sum(values):
        return 0.5 * jnp.sum(values, axis=1, keepdims=True)

    def norm(values):
        return lax.rsqrt(half_sum(values * values) + epsilon)

    ROWS = range(8)
    q = [by_heads(parts[0], row) for row in ROWS]
    k = [by_heads(parts[1], row) for row in ROWS]
    v = [by_heads(parts[2], row) for row in ROWS]
    q_norm = [norm(values) * 0.125 for values in q]
    k_norm = [norm(values) for values in k]
    a = [jnp.broadcast_to(fade[:, row : row + 1], (8, 128)) for row in ROWS]
    b = [jnp.broadcast_to(beta[:, row : row + 1], (8, 128)) for row in ROWS]

    is_step = []
    for j in range(2):
        taken = jnp.broadcast_to(accepted_ref[0:1, j : j + 1], (8, 128))
        is_step.append([taken == n + 1 for n in range(3)])
    ks, qs = [None] * 8, [None] * 8
    for i in range(32):
        index = lane // 64 + 2 * i
        at = slice(128 * i, 128 * i + 128)
        for j in range(2):
            start = prior_ref[j, 3, :, at]
            for n in range(3):
                start = jnp.where(is_step[j][n], prior_ref[j, n, :, at], start)
            begin[j, :, at] = start
            for row in range(4 * j, 4 * j + 4):
                kx = jnp.take_along_axis(k[row], index, axis=1, mode="promise_in_bounds")
                qx = jnp.take_along_axis(q[row], index, axis=1, mode="promise_in_bounds")
                kept[row, :, at] = kx
                ks[row] = kx * start if i == 0 else ks[row] + kx * start
                qs[row] = qx * start if i == 0 else qs[row] + qx * start

    def fold(values):
        return values + pltpu.roll(values, 64, 1)

    copies = []
    for j in range(2):
        w, kw = [None] * 4, [None] * 4
        grown = None
        for t in range(4):
            row = 4 * j + t
            read = k_norm[row] * fold(ks[row])
            carried = read if t == 0 else grown * read
            for e in range(t):
                reach = half_sum(k[row] * k[4 * j + e]) * k_norm[row]
                for m in range(e + 1, t):
                    reach = reach * a[4 * j + m]
                carried = carried + reach * kw[e]
            w[t] = b[row] * (v[row] - a[row] * carried)
            kw[t] = k_norm[row] * w[t]
            grown = a[row] if t == 0 else grown * a[row]
            out = grown * (q_norm[row] * fold(qs[row]))
            for e in range(t + 1):
                reach = half_sum(q[row] * k[4 * j + e]) * q_norm[row]
                for m in range(e + 1, t + 1):
                    reach = reach * a[4 * j + m]
                out = out + reach * kw[e]
            mean = half_sum(out * out) / 64
            n = out * lax.rsqrt(mean + epsilon) * gain
            for p in range(4):
                nrows[row : row + 1, 128 * p : 128 * p + 128] = jnp.sum(
                    jnp.where(masks[p], n, 0.0), axis=0, keepdims=True
                )
        states_ref = early_ref if j == 0 else late_ref
        for i in range(32):
            at = slice(128 * i, 128 * i + 128)
            state = begin[j, :, at]
            for t in range(4):
                row = 4 * j + t
                state = a[row] * state + kept[row, :, at] * kw[t]
                states_ref[t, :, at] = state
        if j == 0:
            for t in range(4):
                copies.append(
                    pltpu.make_async_copy(early_ref.at[t], out_ref.at[0, t], sems.at[t])
                )
                copies[-1].start()
    rows = nrows[...]
    rows_ref[...] = jnp.concatenate([rows] * 8, axis=0).astype(bf16)
    for copy in copies:
        copy.wait()


def mix_kernel(x_ref, rows_ref, out_ref):
    w = x_ref[:, :, WO:QKV].reshape(256, 512)
    rows = rows_ref[...]
    out = dot(w, jnp.concatenate([rows, rows], axis=0), 1, 1)
    low = iota((16, 128), 1) < 64
    for r in range(8):
        piece = jnp.where(low, out[32 * r : 32 * r + 16], out[32 * r + 16 : 32 * r + 32])
        out_ref[2 * r] = piece.astype(bf16)
        out_ref[2 * r + 1] = piece.astype(bf16)


def place_kernel(x_ref, back_ref, late_ref, begun_ref, out_ref, whole_ref, sems):
    copies = [
        pltpu.make_async_copy(late_ref.at[t], whole_ref.at[1, t], sems.at[t]) for t in range(4)
    ]
    for copy in copies:
        copy.start()
    low = iota((16, 128), 1) < 64
    sums = [x_ref[2 * r].astype(f32) + x_ref[2 * r + 1].astype(f32) for r in range(8)]
    tiles = []
    for p in range(4):
        a, b = sums[2 * p], sums[2 * p + 1]
        top = jnp.where(low, a, pltpu.roll(b, 64, 1))
        end = jnp.where(low, pltpu.roll(a, 64, 1), b)
        tiles.append(jnp.concatenate([top, end], axis=0).astype(bf16))
    whole = dot(jnp.concatenate(tiles, axis=1), back_ref[...], 1, 0).astype(bf16)
    for t in range(4):
        out_ref[t] = whole[:, 128 * t : 128 * t + 128]
    for copy in copies:
        copy.wait()


def back_table():
    dest = np.arange(512)
    group, rho = dest // 64, dest % 64
    wanted = (rho % 4) * 128 + (rho // 8) * 16 + group * 2 + (rho % 8) // 4
    return (wanted[:, None] == np.arange(512)[None, :]).astype(jnp.bfloat16)


def call(kernel, shapes, args, specs=None, scratch=(), outs=VMEM, name=None, aliases=None):
    if name == "pack":
        args = [pltpu.with_memory_space_constraint(a, pltpu.HBM) for a in args]
    return pl.pallas_call(
        kernel,
        out_shape=shapes,
        in_specs=specs or [VMEM] * len(args),
        out_specs=outs,
        scratch_shapes=scratch,
        compiler_params=pltpu.CompilerParams(vmem_limit_bytes=16 << 20),
        input_output_aliases=aliases or {},
        name=name,
    )(*args)


def shape(dims, dtype):
    return jax.ShapeDtypeStruct(dims, dtype)


def per_device(
    tokens,
    input_norm_gain,
    query_projection,
    key_projection,
    value_projection,
    write_strength_weight,
    decay_projection,
    head_decay_rate,
    token_extra_decay,
    accepted,
    prior_step_states,
    output_norm_gain,
    output_projection,
):
    def swap(x, axes):
        return lax.all_to_all(x, axes, 0, 0, tiled=True)

    packed = call(
        pack_kernel,
        shape((8, 32, WIDE), bf16),
        (
            jnp.transpose(tokens, (1, 2, 0)),
            input_norm_gain[None, :],
            query_projection,
            key_projection,
            value_projection,
            write_strength_weight.T,
            decay_projection.T,
            output_projection.T,
        ),
        specs=[HBM] * 8,
        scratch=[
            pltpu.VMEM((4, 32, 128), bf16),
            pltpu.VMEM((1, 32), f32),
            pltpu.VMEM((32, 512), bf16),
            pltpu.VMEM((32, 512), bf16),
            pltpu.VMEM((32, 512), bf16),
            pltpu.VMEM((8, 32), bf16),
            pltpu.VMEM((8, 32), bf16),
            pltpu.VMEM((32, 512), bf16),
            pltpu.SemaphoreType.DMA((8,)),
        ],
        name="pack",
    )
    near = swap(packed, NEAR)
    part = call(project_kernel, shape((64, WIDE - QKV), bf16), (near,), name="project")
    arrived = swap(part.reshape(8, 8, part.shape[1]), "z8").reshape(part.shape)
    begun, late, rows = call(
        delta_kernel,
        (
            shape(prior_step_states.shape, f32),
            shape(prior_step_states.shape[1:], f32),
            shape((64, 512), bf16),
        ),
        (
            accepted[None, :],
            arrived,
            prior_step_states,
            head_decay_rate[None, :],
            token_extra_decay,
            output_norm_gain[None, :],
        ),
        scratch=[
            pltpu.VMEM((8, 128), f32),
            pltpu.VMEM((8, 512), f32),
            pltpu.VMEM((8, 8, 4096), f32),
            pltpu.VMEM((2, 8, 4096), f32),
            pltpu.VMEM((4, 8, 4096), f32),
            pltpu.SemaphoreType.DMA((4,)),
        ],
        outs=(HBM, VMEM, VMEM),
        name="delta",
    )
    all_rows = swap(rows.reshape(8, 8, 512), "z8").reshape(64, 512)
    columns = call(mix_kernel, shape((16, 16, 128), bf16), (near, all_rows), name="mix")
    back = swap(columns, ("zp", "y", "tp"))
    mixed, whole = call(
        place_kernel,
        (shape((4, 32, 128), bf16), shape(begun.shape, f32)),
        (back, jnp.asarray(back_table()), late, begun),
        specs=[VMEM, VMEM, VMEM, HBM],
        scratch=[pltpu.SemaphoreType.DMA((4,))],
        outs=(VMEM, HBM),
        aliases={3: 1},
        name="place",
    )
    return (jnp.transpose(mixed, (2, 0, 1)), whole)


def solution(mesh):
    split = Mesh(
        mesh.devices.reshape(mesh.shape["dp"], 8, 2, 4, mesh.shape["tp"]),
        ("dp", "z8", "zp", "y", "tp"),
    )
    in_specs = (
        P("dp", None, KV),
        P(KV),
        P(KV, "tp"),
        P(KV, "tp"),
        P(KV, "tp"),
        P(KV, "tp"),
        P(KV, "tp"),
        P("tp"),
        P(DP_KV, None, "tp"),
        P(DP_KV),
        P(DP_KV, None, "tp", None),
        P(),
        P("tp", KV),
    )
    out_specs = (P("dp", None, KV), P(DP_KV, None, "tp", None))
    return jax.shard_map(
        per_device, mesh=split, in_specs=in_specs, out_specs=out_specs, check_vma=False
    )
```

```python
import jax
import jax.numpy as jnp
import numpy as np
from jax import lax
from jax.experimental import pallas as pl
from jax.experimental.pallas import tpu as pltpu
from jax.sharding import Mesh
from jax.sharding import PartitionSpec as P

D = 2048
epsilon = 1e-06
KV = ("z8", "zp", "y")
DP_KV = ("dp", "z8", "zp", "y")
NEAR = ("zp", "y")
f32 = jnp.float32
bf16 = jnp.bfloat16

WO, QKV, SMALL, WIDE = 0, 512, 2048, 2176
VMEM = pl.BlockSpec(memory_space=pltpu.VMEM)
SMEM = pl.BlockSpec(memory_space=pltpu.SMEM)
HBM = pl.BlockSpec(memory_space=pltpu.HBM)


def iota(shape, dim):
    return lax.broadcasted_iota(jnp.int32, shape, dim)


def dot(a, b, ca, cb):
    return lax.dot_general(a, b, (((ca,), (cb,)), ((), ())), preferred_element_type=f32)


def pack_kernel(*refs):
    hbm, out_ref, held, sems = refs[:8], refs[8], refs[9:17], refs[17]
    copies = [pltpu.make_async_copy(hbm[n], held[n], sems.at[n]) for n in range(8)]
    for copy in copies:
        copy.start()
    tok_ref, gain_ref, q_ref, k_ref, v_ref, beta_ref, decay_ref, wo_ref = held
    source, dest = iota((512, 512), 0), iota((1, 512), 1)
    group, rho = dest // 64, dest % 64
    wanted = (rho % 4) * 128 + (rho // 8) * 16 + group * 2 + (rho % 8) // 4
    pick = (source == wanted).astype(f32).astype(bf16)
    eye = iota((32, 32), 0) == iota((32, 32), 1)
    head, lane = iota((8, 128), 0), iota((8, 128), 1)
    put_beta = ((lane == head) | (lane == head + 16)).astype(f32).astype(bf16)
    put_decay = ((lane == head + 8) | (lane == head + 24)).astype(f32).astype(bf16)
    for copy in copies:
        copy.wait()
    gain = jnp.sum(jnp.where(eye, gain_ref[...], 0.0), axis=1, keepdims=True)
    raw = jnp.concatenate([tok_ref[t] for t in range(4)], axis=1).astype(f32)
    scaled = raw * gain
    squares = jnp.sum(raw * raw, axis=0, keepdims=True)
    high = squares.astype(bf16).astype(f32)
    sub = iota((16, 512), 0)
    extra = jnp.where(sub < 2, high, jnp.where(sub < 4, squares - high, 0.0))
    moved = dot(jnp.concatenate([scaled, extra], axis=0).astype(bf16), pick, 1, 0)
    small = dot(beta_ref[...], put_beta, 0, 0) + dot(decay_ref[...], put_decay, 0, 0)
    lane = iota((8, 128), 1)
    even = iota((8, 128), 0) % 2 == 0
    for r in range(8):
        at = slice(128 * (r // 2), 128 * (r // 2) + 128)
        sums = moved[32:40, at]
        if r % 2 == 0:
            cols = pltpu.roll(moved[:32, at], 64, 1)
            sums = jnp.where(even, pltpu.roll(sums, 32, 1), sums)
        else:
            cols = moved[:32, at]
            sums = jnp.where(even, pltpu.roll(sums, 96, 1), pltpu.roll(sums, 64, 1))
        groups = []
        for g in range(4):
            right = jnp.where(lane < 64, sums if g == 0 else 0.0, cols[8 * g : 8 * g + 8])
            groups.append(jnp.where(lane < 32, small[8 * g : 8 * g + 8], right))
        tile = jnp.concatenate(groups, axis=0)
        out_ref[r, :, WO:QKV] = wo_ref[...]
        out_ref[r, :, QKV : QKV + 512] = q_ref[...]
        out_ref[r, :, QKV + 512 : QKV + 1024] = k_ref[...]
        out_ref[r, :, QKV + 1024 : SMALL] = v_ref[...]
        out_ref[r, :, SMALL:] = tile.astype(bf16)


def project_kernel(x_ref, out_ref):
    x = x_ref[...].reshape(256, WIDE)
    cols = x[:, SMALL:]
    main = dot(cols, x[:, QKV:SMALL], 0, 0)
    out_ref[:, : SMALL - QKV] = main[64:].astype(bf16)
    sums = jnp.zeros((8, 128), f32)
    for r in range(8):
        sums = sums + cols[32 * r : 32 * r + 16].astype(f32)[0:8]
    sub, lane = iota((32, 128), 0), iota((32, 128), 1)
    halves = []
    for n in range(2):
        row = sums[n : n + 1] + sums[n + 2 : n + 3]
        halves.append(jnp.sum(jnp.where(lane == sub + 32, row, 0.0), axis=1, keepdims=True))
    total = jnp.concatenate(halves, axis=0)
    lane = iota((64, 128), 1)
    tail = jnp.where(lane < 32, dot(cols, cols, 0, 0)[64:], jnp.where(lane < 34, total, 0.0))
    first = tail.astype(bf16).astype(f32)
    keep = (lane < 16) | (lane == 32)
    out_ref[:, SMALL - QKV :] = jnp.where(keep, first, tail - first).astype(bf16)


def delta_kernel(
    accepted_ref, c_ref, prior_ref, rate_ref, extra_ref, gain_ref, states_ref, rows_ref,
    aux, nrows, kept
):
    c = c_ref[...].astype(f32)
    s = (c[0:8] + c[8:16]) + (c[16:24] + c[24:32])
    s = s + ((c[32:40] + c[40:48]) + (c[48:56] + c[56:64]))
    tile = s[:, 1536:]
    total = tile[:, 32:33] + tile[:, 33:34]
    inverse = lax.rsqrt(total / D + epsilon)
    logits = jnp.transpose((tile + pltpu.roll(tile, 112, 1)) * inverse)
    aux[...] = jnp.zeros((8, 128), f32)
    aux[0:4, 0:8] = extra_ref[0]
    aux[4:8, 0:8] = extra_ref[1]
    aux[:, 8:16] = jnp.broadcast_to(rate_ref[...], (8, 8))
    side = jnp.transpose(aux[...])
    beta = jax.nn.sigmoid(logits[0:8])
    fade = jnp.exp(-side[8:16] * jax.nn.softplus(logits[8:16]) + side[0:8])

    sub, lane = iota((8, 128), 0), iota((8, 128), 1)
    masks = [sub == 2 * p + lane // 64 for p in range(4)]
    gain = jnp.concatenate([gain_ref[...], gain_ref[...]], axis=1)

    def silu_of(at):
        u = s[:, at : at + 512] * inverse
        return u / (1.0 + jnp.exp(-u))

    parts = [silu_of(0), silu_of(512), silu_of(1024)]

    def by_heads(values, row):
        m = jnp.zeros((8, 128), f32)
        for p in range(4):
            piece = jnp.broadcast_to(values[row : row + 1, 128 * p : 128 * p + 128], (8, 128))
            m = jnp.where(masks[p], piece, m)
        return m + pltpu.roll(m, 64, 1)

    def half_sum(values):
        return 0.5 * jnp.sum(values, axis=1, keepdims=True)

    def unit(values):
        return values * lax.rsqrt(half_sum(values * values) + epsilon)

    ROWS = range(8)
    q = [unit(by_heads(parts[0], row)) * 0.125 for row in ROWS]
    k = [unit(by_heads(parts[1], row)) for row in ROWS]
    v = [by_heads(parts[2], row) for row in ROWS]
    a = [jnp.broadcast_to(fade[:, row : row + 1], (8, 128)) for row in ROWS]
    b = [jnp.broadcast_to(beta[:, row : row + 1], (8, 128)) for row in ROWS]

    starts = [accepted_ref[0] - 1, accepted_ref[1] - 1]
    ks, qs = [None] * 8, [None] * 8
    for i in range(32):
        index = lane // 64 + 2 * i
        at = slice(128 * i, 128 * i + 128)
        for j in range(2):
            start = prior_ref[j, starts[j], :, at]
            for row in range(4 * j, 4 * j + 4):
                kx = jnp.take_along_axis(k[row], index, axis=1, mode="promise_in_bounds")
                qx = jnp.take_along_axis(q[row], index, axis=1, mode="promise_in_bounds")
                kept[row, :, at] = kx
                ks[row] = kx * start if i == 0 else ks[row] + kx * start
                qs[row] = qx * start if i == 0 else qs[row] + qx * start

    def fold(values):
        return values + pltpu.roll(values, 64, 1)

    ks = [fold(values) for values in ks]
    qs = [fold(values) for values in qs]
    w, o = [None] * 8, [None] * 8
    for j in range(2):
        base = 4 * j
        grown = None
        for t in range(4):
            row = base + t
            carried = ks[row] if t == 0 else grown * ks[row]
            for e in range(t):
                reach = half_sum(k[row] * k[base + e])
                for m in range(e + 1, t):
                    reach = reach * a[base + m]
                carried = carried + reach * w[base + e]
            w[row] = b[row] * (v[row] - a[row] * carried)
            grown = a[row] if t == 0 else grown * a[row]
            out = grown * qs[row] + half_sum(q[row] * k[row]) * w[row]
            for e in range(t):
                reach = half_sum(q[row] * k[base + e])
                for m in range(e + 1, t + 1):
                    reach = reach * a[base + m]
                out = out + reach * w[base + e]
            o[row] = out

    for j in range(2):
        for i in range(32):
            at = slice(128 * i, 128 * i + 128)
            state = prior_ref[j, starts[j], :, at]
            for t in range(4):
                row = 4 * j + t
                state = a[row] * state + kept[row, :, at] * w[row]
                states_ref[j, t, :, at] = state

    for row in ROWS:
        mean = half_sum(o[row] * o[row]) / 64
        n = o[row] * lax.rsqrt(mean + epsilon) * gain
        for p in range(4):
            nrows[row : row + 1, 128 * p : 128 * p + 128] = jnp.sum(
                jnp.where(masks[p], n, 0.0), axis=0, keepdims=True
            )
    rows = nrows[...]
    rows_ref[...] = jnp.concatenate([rows] * 8, axis=0).astype(bf16)


def mix_kernel(x_ref, rows_ref, out_ref):
    w = x_ref[:, :, WO:QKV].reshape(256, 512)
    rows = rows_ref[...]
    out = dot(w, jnp.concatenate([rows, rows], axis=0), 1, 1)
    low = iota((16, 128), 1) < 64
    for r in range(8):
        piece = jnp.where(low, out[32 * r : 32 * r + 16], out[32 * r + 16 : 32 * r + 32])
        out_ref[2 * r] = piece.astype(bf16)
        out_ref[2 * r + 1] = piece.astype(bf16)


def place_kernel(x_ref, back_ref, out_ref):
    low = iota((16, 128), 1) < 64
    sums = [x_ref[2 * r].astype(f32) + x_ref[2 * r + 1].astype(f32) for r in range(8)]
    tiles = []
    for p in range(4):
        a, b = sums[2 * p], sums[2 * p + 1]
        top = jnp.where(low, a, pltpu.roll(b, 64, 1))
        end = jnp.where(low, pltpu.roll(a, 64, 1), b)
        tiles.append(jnp.concatenate([top, end], axis=0).astype(bf16))
    whole = dot(jnp.concatenate(tiles, axis=1), back_ref[...], 1, 0).astype(bf16)
    for t in range(4):
        out_ref[t] = whole[:, 128 * t : 128 * t + 128]


def back_table():
    dest = np.arange(512)
    group, rho = dest // 64, dest % 64
    wanted = (rho % 4) * 128 + (rho // 8) * 16 + group * 2 + (rho % 8) // 4
    return (wanted[:, None] == np.arange(512)[None, :]).astype(jnp.bfloat16)


def call(kernel, shapes, args, specs=None, scratch=(), outs=VMEM, name=None, aliases=None):
    if name == "pack":
        args = [pltpu.with_memory_space_constraint(a, pltpu.HBM) for a in args]
    return pl.pallas_call(
        kernel,
        out_shape=shapes,
        in_specs=specs or [VMEM] * len(args),
        out_specs=outs,
        scratch_shapes=scratch,
        compiler_params=pltpu.CompilerParams(vmem_limit_bytes=16 << 20),
        input_output_aliases=aliases or {},
        name=name,
    )(*args)


def shape(dims, dtype):
    return jax.ShapeDtypeStruct(dims, dtype)


def per_device(
    tokens,
    input_norm_gain,
    query_projection,
    key_projection,
    value_projection,
    write_strength_weight,
    decay_projection,
    head_decay_rate,
    token_extra_decay,
    accepted,
    prior_step_states,
    output_norm_gain,
    output_projection,
):
    def swap(x, axes):
        return lax.all_to_all(x, axes, 0, 0, tiled=True)

    packed = call(
        pack_kernel,
        shape((8, 32, WIDE), bf16),
        (
            jnp.transpose(tokens, (1, 2, 0)),
            input_norm_gain[None, :],
            query_projection,
            key_projection,
            value_projection,
            write_strength_weight.T,
            decay_projection.T,
            output_projection.T,
        ),
        specs=[HBM] * 8,
        scratch=[
            pltpu.VMEM((4, 32, 128), bf16),
            pltpu.VMEM((1, 32), f32),
            pltpu.VMEM((32, 512), bf16),
            pltpu.VMEM((32, 512), bf16),
            pltpu.VMEM((32, 512), bf16),
            pltpu.VMEM((8, 32), bf16),
            pltpu.VMEM((8, 32), bf16),
            pltpu.VMEM((32, 512), bf16),
            pltpu.SemaphoreType.DMA((8,)),
        ],
        name="pack",
    )
    near = swap(packed, NEAR)
    part = call(project_kernel, shape((64, WIDE - QKV), bf16), (near,), name="project")
    arrived = swap(part.reshape(8, 8, part.shape[1]), "z8").reshape(part.shape)
    states, rows = call(
        delta_kernel,
        (pltpu.VMEM(prior_step_states.shape, f32), shape((64, 512), bf16)),
        (
            accepted,
            arrived,
            prior_step_states,
            head_decay_rate[None, :],
            token_extra_decay,
            output_norm_gain[None, :],
        ),
        specs=[SMEM] + [VMEM] * 5,
        scratch=[
            pltpu.VMEM((8, 128), f32),
            pltpu.VMEM((8, 512), f32),
            pltpu.VMEM((8, 8, 4096), f32),
        ],
        outs=(VMEM, VMEM),
        name="delta",
    )
    all_rows = swap(rows.reshape(8, 8, 512), "z8").reshape(64, 512)
    columns = call(mix_kernel, shape((16, 16, 128), bf16), (near, all_rows), name="mix")
    back = swap(columns, ("zp", "y", "tp"))
    mixed = call(
        place_kernel, shape((4, 32, 128), bf16), (back, jnp.asarray(back_table())), name="place"
    )
    return (jnp.transpose(mixed, (2, 0, 1)), states)


def solution(mesh):
    split = Mesh(
        mesh.devices.reshape(mesh.shape["dp"], 8, 2, 4, mesh.shape["tp"]),
        ("dp", "z8", "zp", "y", "tp"),
    )
    in_specs = (
        P("dp", None, KV),
        P(KV),
        P(KV, "tp"),
        P(KV, "tp"),
        P(KV, "tp"),
        P(KV, "tp"),
        P(KV, "tp"),
        P("tp"),
        P(DP_KV, None, "tp"),
        P(DP_KV),
        P(DP_KV, None, "tp", None),
        P(),
        P("tp", KV),
    )
    out_specs = (P("dp", None, KV), P(DP_KV, None, "tp", None))
    return jax.shard_map(
        per_device, mesh=split, in_specs=in_specs, out_specs=out_specs, check_vma=False
    )
```

```python
import functools

import jax
import jax.numpy as jnp
import numpy as np
from jax import lax
from jax.experimental import pallas as pl
from jax.experimental.pallas import tpu as pltpu
from jax.sharding import Mesh
from jax.sharding import PartitionSpec as P

D = 2048
epsilon = 1e-06
KV = ("z8", "zp", "y")
DP_KV = ("dp", "z8", "zp", "y")
NEAR = ("zp", "y")
f32 = jnp.float32
bf16 = jnp.bfloat16

QKV, SMALL, WO, WIDE = 0, 1536, 1664, 2176
VMEM = pl.BlockSpec(memory_space=pltpu.VMEM)
SMEM = pl.BlockSpec(memory_space=pltpu.SMEM)
HBM = pl.BlockSpec(memory_space=pltpu.HBM)


def iota(shape, dim):
    return lax.broadcasted_iota(jnp.int32, shape, dim)


def dot(a, b, ca, cb):
    return lax.dot_general(a, b, (((ca,), (cb,)), ((), ())), preferred_element_type=f32)


def pack_kernel(*refs, late):
    hbm, out_ref, held, sems = refs[:8], refs[8], refs[-9:-1], refs[-1]
    copies = [pltpu.make_async_copy(hbm[n], held[n], sems.at[n]) for n in range(8)]
    for copy in copies:
        copy.start()
    tok_ref, gain_ref, q_ref, k_ref, v_ref, beta_ref, decay_ref, wo_ref = held
    source, dest = iota((512, 512), 0), iota((1, 512), 1)
    group, rho = dest // 64, dest % 64
    wanted = (rho % 4) * 128 + (rho // 8) * 16 + group * 2 + (rho % 8) // 4
    pick = (source == wanted).astype(f32).astype(bf16)
    eye = iota((32, 32), 0) == iota((32, 32), 1)
    head, lane = iota((8, 128), 0), iota((8, 128), 1)
    put_beta = ((lane == head) | (lane == head + 16)).astype(f32).astype(bf16)
    put_decay = ((lane == head + 8) | (lane == head + 24)).astype(f32).astype(bf16)
    for copy in copies:
        copy.wait()
    gain = jnp.sum(jnp.where(eye, gain_ref[...], 0.0), axis=1, keepdims=True)
    raw = jnp.concatenate([tok_ref[t] for t in range(4)], axis=1).astype(f32)
    scaled = raw * gain
    squares = jnp.sum(raw * raw, axis=0, keepdims=True)
    high = squares.astype(bf16).astype(f32)
    sub = iota((16, 512), 0)
    extra = jnp.where(sub < 2, high, jnp.where(sub < 4, squares - high, 0.0))
    moved = dot(jnp.concatenate([scaled, extra], axis=0).astype(bf16), pick, 1, 0)
    small = dot(beta_ref[...], put_beta, 0, 0) + dot(decay_ref[...], put_decay, 0, 0)
    lane = iota((8, 128), 1)
    even = iota((8, 128), 0) % 2 == 0
    for r in range(8):
        at = slice(128 * (r // 2), 128 * (r // 2) + 128)
        sums = moved[32:40, at]
        if r % 2 == 0:
            cols = pltpu.roll(moved[:32, at], 64, 1)
            sums = jnp.where(even, pltpu.roll(sums, 32, 1), sums)
        else:
            cols = moved[:32, at]
            sums = jnp.where(even, pltpu.roll(sums, 96, 1), pltpu.roll(sums, 64, 1))
        groups = []
        for g in range(4):
            right = jnp.where(lane < 64, sums if g == 0 else 0.0, cols[8 * g : 8 * g + 8])
            groups.append(jnp.where(lane < 32, small[8 * g : 8 * g + 8], right))
        tile = jnp.concatenate(groups, axis=0)
        if late:
            refs[9][r] = wo_ref[...]
        else:
            out_ref[r, :, WO:] = wo_ref[...]
        out_ref[r, :, QKV : QKV + 512] = q_ref[...]
        out_ref[r, :, QKV + 512 : QKV + 1024] = k_ref[...]
        out_ref[r, :, QKV + 1024 : SMALL] = v_ref[...]
        out_ref[r, :, SMALL:WO] = tile.astype(bf16)


def project_kernel(x_ref, out_ref, *wo_refs):
    for wo_ref in wo_refs:
        wo_ref[...] = x_ref[:, :, WO:]
    x = x_ref[:, :, :WO].reshape(256, WO)
    cols = x[:, SMALL:]
    main = dot(cols, x[:, QKV:SMALL], 0, 0)
    out_ref[:, : SMALL - QKV] = main[64:].astype(bf16)
    sums = jnp.zeros((8, 128), f32)
    for r in range(8):
        sums = sums + cols[32 * r : 32 * r + 16].astype(f32)[0:8]
    sub, lane = iota((32, 128), 0), iota((32, 128), 1)
    halves = []
    for n in range(2):
        row = sums[n : n + 1] + sums[n + 2 : n + 3]
        halves.append(jnp.sum(jnp.where(lane == sub + 32, row, 0.0), axis=1, keepdims=True))
    total = jnp.concatenate(halves, axis=0)
    lane = iota((64, 128), 1)
    tail = jnp.where(lane < 32, dot(cols, cols, 0, 0)[64:], jnp.where(lane < 34, total, 0.0))
    first = tail.astype(bf16).astype(f32)
    keep = (lane < 16) | (lane == 32)
    out_ref[:, SMALL - QKV :] = jnp.where(keep, first, tail - first).astype(bf16)


def delta_kernel(
    accepted_ref, c_ref, prior_ref, rate_ref, extra_ref, gain_ref, states_ref, rows_ref,
    aux, nrows, kept
):
    c = c_ref[...].astype(f32)
    s = (c[0:8] + c[8:16]) + (c[16:24] + c[24:32])
    s = s + ((c[32:40] + c[40:48]) + (c[48:56] + c[56:64]))
    tile = s[:, 1536:]
    total = tile[:, 32:33] + tile[:, 33:34]
    inverse = lax.rsqrt(total / D + epsilon)
    logits = jnp.transpose((tile + pltpu.roll(tile, 112, 1)) * inverse)
    aux[...] = jnp.zeros((8, 128), f32)
    aux[0:4, 0:8] = extra_ref[0]
    aux[4:8, 0:8] = extra_ref[1]
    aux[:, 8:16] = jnp.broadcast_to(rate_ref[...], (8, 8))
    side = jnp.transpose(aux[...])
    beta = jax.nn.sigmoid(logits[0:8])
    fade = jnp.exp(-side[8:16] * jax.nn.softplus(logits[8:16]) + side[0:8])

    sub, lane = iota((8, 128), 0), iota((8, 128), 1)
    masks = [sub == 2 * p + lane // 64 for p in range(4)]
    gain = jnp.concatenate([gain_ref[...], gain_ref[...]], axis=1)

    def silu_of(at):
        u = s[:, at : at + 512] * inverse
        return u / (1.0 + jnp.exp(-u))

    parts = [silu_of(0), silu_of(512), silu_of(1024)]

    def by_heads(values, row):
        m = jnp.zeros((8, 128), f32)
        for p in range(4):
            piece = jnp.broadcast_to(values[row : row + 1, 128 * p : 128 * p + 128], (8, 128))
            m = jnp.where(masks[p], piece, m)
        return m + pltpu.roll(m, 64, 1)

    def half_sum(values):
        return 0.5 * jnp.sum(values, axis=1, keepdims=True)

    def unit(values):
        return values * lax.rsqrt(half_sum(values * values) + epsilon)

    ROWS = range(8)
    q = [unit(by_heads(parts[0], row)) * 0.125 for row in ROWS]
    k = [unit(by_heads(parts[1], row)) for row in ROWS]
    v = [by_heads(parts[2], row) for row in ROWS]
    a = [jnp.broadcast_to(fade[:, row : row + 1], (8, 128)) for row in ROWS]
    b = [jnp.broadcast_to(beta[:, row : row + 1], (8, 128)) for row in ROWS]

    starts = [accepted_ref[0] - 1, accepted_ref[1] - 1]
    ks, qs = [None] * 8, [None] * 8
    for i in range(32):
        index = lane // 64 + 2 * i
        at = slice(128 * i, 128 * i + 128)
        for j in range(2):
            start = prior_ref[j, starts[j], :, at]
            for row in range(4 * j, 4 * j + 4):
                kx = jnp.take_along_axis(k[row], index, axis=1, mode="promise_in_bounds")
                qx = jnp.take_along_axis(q[row], index, axis=1, mode="promise_in_bounds")
                kept[row, :, at] = kx
                ks[row] = kx * start if i == 0 else ks[row] + kx * start
                qs[row] = qx * start if i == 0 else qs[row] + qx * start

    def fold(values):
        return values + pltpu.roll(values, 64, 1)

    ks = [fold(values) for values in ks]
    qs = [fold(values) for values in qs]
    w, o = [None] * 8, [None] * 8
    for j in range(2):
        base = 4 * j
        grown = None
        for t in range(4):
            row = base + t
            carried = ks[row] if t == 0 else grown * ks[row]
            for e in range(t):
                reach = half_sum(k[row] * k[base + e])
                for m in range(e + 1, t):
                    reach = reach * a[base + m]
                carried = carried + reach * w[base + e]
            w[row] = b[row] * (v[row] - a[row] * carried)
            grown = a[row] if t == 0 else grown * a[row]
            out = grown * qs[row] + half_sum(q[row] * k[row]) * w[row]
            for e in range(t):
                reach = half_sum(q[row] * k[base + e])
                for m in range(e + 1, t + 1):
                    reach = reach * a[base + m]
                out = out + reach * w[base + e]
            o[row] = out

    for j in range(2):
        for i in range(32):
            at = slice(128 * i, 128 * i + 128)
            state = prior_ref[j, starts[j], :, at]
            for t in range(4):
                row = 4 * j + t
                state = a[row] * state + kept[row, :, at] * w[row]
                states_ref[j, t, :, at] = state

    for row in ROWS:
        mean = half_sum(o[row] * o[row]) / 64
        n = o[row] * lax.rsqrt(mean + epsilon) * gain
        for p in range(4):
            nrows[row : row + 1, 128 * p : 128 * p + 128] = jnp.sum(
                jnp.where(masks[p], n, 0.0), axis=0, keepdims=True
            )
    rows = nrows[...]
    rows_ref[...] = jnp.concatenate([rows] * 8, axis=0).astype(bf16)


def mix_kernel(x_ref, rows_ref, out_ref):
    w = x_ref[...].reshape(256, 512)
    rows = rows_ref[...]
    out = dot(w, jnp.concatenate([rows, rows], axis=0), 1, 1)
    low = iota((16, 128), 1) < 64
    for r in range(8):
        piece = jnp.where(low, out[32 * r : 32 * r + 16], out[32 * r + 16 : 32 * r + 32])
        out_ref[2 * r] = piece.astype(bf16)
        out_ref[2 * r + 1] = piece.astype(bf16)


def place_kernel(x_ref, back_ref, states_ref, out_ref, kept_ref, sem):
    copies = [
        pltpu.make_async_copy(states_ref.at[n // 4, n % 4], kept_ref.at[n // 4, n % 4], sem.at[n])
        for n in range(8)
    ]
    for copy in copies:
        copy.start()
    low = iota((16, 128), 1) < 64
    sums = [x_ref[2 * r].astype(f32) + x_ref[2 * r + 1].astype(f32) for r in range(8)]
    tiles = []
    for p in range(4):
        a, b = sums[2 * p], sums[2 * p + 1]
        top = jnp.where(low, a, pltpu.roll(b, 64, 1))
        end = jnp.where(low, pltpu.roll(a, 64, 1), b)
        tiles.append(jnp.concatenate([top, end], axis=0).astype(bf16))
    whole = dot(jnp.concatenate(tiles, axis=1), back_ref[...], 1, 0).astype(bf16)
    for t in range(4):
        out_ref[t] = whole[:, 128 * t : 128 * t + 128]
    for copy in copies:
        copy.wait()


def back_table():
    dest = np.arange(512)
    group, rho = dest // 64, dest % 64
    wanted = (rho % 4) * 128 + (rho // 8) * 16 + group * 2 + (rho % 8) // 4
    return (wanted[:, None] == np.arange(512)[None, :]).astype(jnp.bfloat16)


def call(kernel, shapes, args, specs=None, scratch=(), outs=VMEM, name=None):
    if name == "pack":
        args = [pltpu.with_memory_space_constraint(a, pltpu.HBM) for a in args]
    return pl.pallas_call(
        kernel,
        out_shape=shapes,
        in_specs=specs or [VMEM] * len(args),
        out_specs=outs,
        scratch_shapes=scratch,
        compiler_params=pltpu.CompilerParams(vmem_limit_bytes=16 << 20),
        name=name,
    )(*args)


def shape(dims, dtype):
    return jax.ShapeDtypeStruct(dims, dtype)


def per_device(
    tokens,
    input_norm_gain,
    query_projection,
    key_projection,
    value_projection,
    write_strength_weight,
    decay_projection,
    head_decay_rate,
    token_extra_decay,
    accepted,
    prior_step_states,
    output_norm_gain,
    output_projection,
):
    def swap(x, axes):
        return lax.all_to_all(x, axes, 0, 0, tiled=True)

    part_shape, wo_shape = shape((64, WO), bf16), shape((8, 32, 512), bf16)

    def pack(late, args):
        sizes = (shape((8, 32, WO), bf16), wo_shape) if late else shape((8, 32, WIDE), bf16)
        return call(
            functools.partial(pack_kernel, late=late),
            sizes,
            args,
            specs=[HBM] * 8,
            scratch=[
                pltpu.VMEM((4, 32, 128), bf16),
                pltpu.VMEM((1, 32), f32),
                pltpu.VMEM((32, 512), bf16),
                pltpu.VMEM((32, 512), bf16),
                pltpu.VMEM((32, 512), bf16),
                pltpu.VMEM((8, 32), bf16),
                pltpu.VMEM((8, 32), bf16),
                pltpu.VMEM((32, 512), bf16),
                pltpu.SemaphoreType.DMA((8,)),
            ],
            outs=(VMEM, VMEM) if late else VMEM,
            name="pack",
        )

    def start_late(*args):
        packed, own = pack(True, args)
        return call(project_kernel, part_shape, (swap(packed, NEAR),), name="project"), own

    def start_early(*args):
        near = swap(pack(False, args), NEAR)
        return call(
            project_kernel, (part_shape, wo_shape), (near,), outs=(VMEM, VMEM), name="project"
        )

    def mix(weights, rows):
        return call(mix_kernel, shape((16, 16, 128), bf16), (weights, rows), name="mix")

    pair = lax.axis_index("z8")
    late = (pair >= 4) & (pair <= 6)
    part, weights = lax.cond(
        late,
        start_late,
        start_early,
        jnp.transpose(tokens, (1, 2, 0)),
        input_norm_gain[None, :],
        query_projection,
        key_projection,
        value_projection,
        write_strength_weight.T,
        decay_projection.T,
        output_projection.T,
    )
    arrived = swap(part.reshape(8, 8, part.shape[1]), "z8").reshape(part.shape)
    states, rows = call(
        delta_kernel,
        (shape(prior_step_states.shape, f32), shape((64, 512), bf16)),
        (
            accepted,
            arrived,
            prior_step_states,
            head_decay_rate[None, :],
            token_extra_decay,
            output_norm_gain[None, :],
        ),
        specs=[SMEM] + [VMEM] * 5,
        scratch=[
            pltpu.VMEM((8, 128), f32),
            pltpu.VMEM((8, 512), f32),
            pltpu.VMEM((8, 8, 4096), f32),
        ],
        outs=(VMEM, VMEM),
        name="delta",
    )
    all_rows = swap(rows.reshape(8, 8, 512), "z8").reshape(64, 512)
    columns = lax.cond(
        late, lambda w, r: mix(swap(w, NEAR), r), lambda w, r: mix(w, r), weights, all_rows
    )
    back = swap(columns, ("zp", "y", "tp"))
    mixed, kept = call(
        place_kernel,
        (shape((4, 32, 128), bf16), shape(states.shape, f32)),
        (back, jnp.asarray(back_table()), states),
        scratch=[pltpu.SemaphoreType.DMA((8,))],
        outs=(VMEM, HBM),
        name="place",
    )
    return (jnp.transpose(mixed, (2, 0, 1)), kept)


def solution(mesh):
    split = Mesh(
        mesh.devices.reshape(mesh.shape["dp"], 8, 2, 4, mesh.shape["tp"]),
        ("dp", "z8", "zp", "y", "tp"),
    )
    in_specs = (
        P("dp", None, KV),
        P(KV),
        P(KV, "tp"),
        P(KV, "tp"),
        P(KV, "tp"),
        P(KV, "tp"),
        P(KV, "tp"),
        P("tp"),
        P(DP_KV, None, "tp"),
        P(DP_KV),
        P(DP_KV, None, "tp", None),
        P(),
        P("tp", KV),
    )
    out_specs = (P("dp", None, KV), P(DP_KV, None, "tp", None))
    return jax.shard_map(
        per_device, mesh=split, in_specs=in_specs, out_specs=out_specs, check_vma=False
    )
```

```python
import functools

import jax
import jax.numpy as jnp
import numpy as np
from jax import lax
from jax.experimental import pallas as pl
from jax.experimental.pallas import tpu as pltpu
from jax.sharding import Mesh
from jax.sharding import PartitionSpec as P

D = 2048
epsilon = 1e-06
KV = ("z8", "zp", "y")
DP_KV = ("dp", "z8", "zp", "y")
NEAR = ("zp", "y")
f32 = jnp.float32
bf16 = jnp.bfloat16

QKV, SMALL, WO, WIDE = 0, 1536, 1664, 2176
VMEM = pl.BlockSpec(memory_space=pltpu.VMEM)
SMEM = pl.BlockSpec(memory_space=pltpu.SMEM)
HBM = pl.BlockSpec(memory_space=pltpu.HBM)


def iota(shape, dim):
    return lax.broadcasted_iota(jnp.int32, shape, dim)


def dot(a, b, ca, cb):
    return lax.dot_general(a, b, (((ca,), (cb,)), ((), ())), preferred_element_type=f32)


def pack_kernel(*refs, late):
    hbm, out_ref, held, sems = refs[:8], refs[8], refs[-9:-1], refs[-1]
    copies = [pltpu.make_async_copy(hbm[n], held[n], sems.at[n]) for n in range(8)]
    for copy in copies:
        copy.start()
    tok_ref, gain_ref, q_ref, k_ref, v_ref, beta_ref, decay_ref, wo_ref = held
    source, dest = iota((512, 512), 0), iota((1, 512), 1)
    group, rho = dest // 64, dest % 64
    wanted = (rho % 4) * 128 + (rho // 8) * 16 + group * 2 + (rho % 8) // 4
    pick = (source == wanted).astype(f32).astype(bf16)
    eye = iota((32, 32), 0) == iota((32, 32), 1)
    head, lane = iota((8, 128), 0), iota((8, 128), 1)
    put_beta = ((lane == head) | (lane == head + 16)).astype(f32).astype(bf16)
    put_decay = ((lane == head + 8) | (lane == head + 24)).astype(f32).astype(bf16)
    for copy in copies:
        copy.wait()
    gain = jnp.sum(jnp.where(eye, gain_ref[...], 0.0), axis=1, keepdims=True)
    raw = dot(jnp.concatenate([tok_ref[t] for t in range(4)], axis=1), pick, 1, 0)
    scaled = raw * gain
    squares = jnp.sum(raw * raw, axis=0, keepdims=True)
    high = squares.astype(bf16).astype(f32)
    sub = iota((8, 512), 0)
    extra = jnp.where(sub < 2, high, jnp.where(sub < 4, squares - high, 0.0))
    small = dot(beta_ref[...], put_beta, 0, 0) + dot(decay_ref[...], put_decay, 0, 0)
    lane = iota((8, 128), 1)
    even = iota((8, 128), 0) % 2 == 0
    for r in range(8):
        at = slice(128 * (r // 2), 128 * (r // 2) + 128)
        sums = extra[:, at]
        if r % 2 == 0:
            cols = pltpu.roll(scaled[:, at], 64, 1)
            sums = jnp.where(even, pltpu.roll(sums, 32, 1), sums)
        else:
            cols = scaled[:, at]
            sums = jnp.where(even, pltpu.roll(sums, 96, 1), pltpu.roll(sums, 64, 1))
        groups = []
        for g in range(4):
            right = jnp.where(lane < 64, sums if g == 0 else 0.0, cols[8 * g : 8 * g + 8])
            groups.append(jnp.where(lane < 32, small[8 * g : 8 * g + 8], right))
        tile = jnp.concatenate(groups, axis=0)
        if late:
            refs[9][r] = wo_ref[...]
        else:
            out_ref[r, :, WO:] = wo_ref[...]
        out_ref[r, :, QKV : QKV + 512] = q_ref[...]
        out_ref[r, :, QKV + 512 : QKV + 1024] = k_ref[...]
        out_ref[r, :, QKV + 1024 : SMALL] = v_ref[...]
        out_ref[r, :, SMALL:WO] = tile.astype(bf16)


def project_kernel(x_ref, out_ref, *wo_refs):
    for wo_ref in wo_refs:
        wo_ref[...] = x_ref[:, :, WO:]
    x = x_ref[:, :, :WO].reshape(256, WO)
    cols = x[:, SMALL:]
    main = dot(cols, x[:, QKV:SMALL], 0, 0)
    out_ref[:, : SMALL - QKV] = main[64:].astype(bf16)
    sums = jnp.zeros((8, 128), f32)
    for r in range(8):
        sums = sums + cols[32 * r : 32 * r + 16].astype(f32)[0:8]
    sub, lane = iota((32, 128), 0), iota((32, 128), 1)
    halves = []
    for n in range(2):
        row = sums[n : n + 1] + sums[n + 2 : n + 3]
        halves.append(jnp.sum(jnp.where(lane == sub + 32, row, 0.0), axis=1, keepdims=True))
    total = jnp.concatenate(halves, axis=0)
    lane = iota((64, 128), 1)
    tail = jnp.where(lane < 32, dot(cols, cols, 0, 0)[64:], jnp.where(lane < 34, total, 0.0))
    first = tail.astype(bf16).astype(f32)
    keep = (lane < 16) | (lane == 32)
    out_ref[:, SMALL - QKV :] = jnp.where(keep, first, tail - first).astype(bf16)


def delta_kernel(
    accepted_ref, c_ref, prior_ref, rate_ref, extra_ref, gain_ref, states_ref, rows_ref,
    aux, nrows, spread_ref
):
    c = c_ref[...].astype(f32)
    s = (c[0:8] + c[8:16]) + (c[16:24] + c[24:32])
    s = s + ((c[32:40] + c[40:48]) + (c[48:56] + c[56:64]))
    tile = s[:, 1536:]
    total = tile[:, 32:33] + tile[:, 33:34]
    inverse = lax.rsqrt(total / D + epsilon)
    logits = jnp.transpose((tile + pltpu.roll(tile, 112, 1)) * inverse)
    aux[...] = jnp.zeros((8, 128), f32)
    aux[0:4, 0:8] = extra_ref[0]
    aux[4:8, 0:8] = extra_ref[1]
    aux[:, 8:16] = jnp.broadcast_to(rate_ref[...], (8, 8))
    side = jnp.transpose(aux[...])
    beta = jax.nn.sigmoid(logits[0:8])
    fade = jnp.exp(-side[8:16] * jax.nn.softplus(logits[8:16]) + side[0:8])

    sub, lane = iota((8, 128), 0), iota((8, 128), 1)
    masks = [sub == 2 * p + lane // 64 for p in range(4)]
    gain = jnp.concatenate([gain_ref[...], gain_ref[...]], axis=1)

    def silu_of(at):
        u = s[:, at : at + 512] * inverse
        return u / (1.0 + jnp.exp(-u))

    parts = [silu_of(0), silu_of(512), silu_of(1024)]

    def by_heads(values, row):
        m = jnp.zeros((8, 128), f32)
        for p in range(4):
            piece = jnp.broadcast_to(values[row : row + 1, 128 * p : 128 * p + 128], (8, 128))
            m = jnp.where(masks[p], piece, m)
        return m + pltpu.roll(m, 64, 1)

    def half_sum(values):
        return 0.5 * jnp.sum(values, axis=1, keepdims=True)

    def norm(values):
        return lax.rsqrt(half_sum(values * values) + epsilon)

    ROWS = range(8)
    q = [by_heads(parts[0], row) for row in ROWS]
    k = [by_heads(parts[1], row) for row in ROWS]
    v = [by_heads(parts[2], row) for row in ROWS]
    q_norm = [norm(values) * 0.125 for values in q]
    k_norm = [norm(values) for values in k]
    a = [jnp.broadcast_to(fade[:, row : row + 1], (8, 128)) for row in ROWS]
    b = [jnp.broadcast_to(beta[:, row : row + 1], (8, 128)) for row in ROWS]

    tall = jnp.concatenate(q + k, axis=0)
    first = tall.astype(bf16).astype(f32)
    second = (tall - first).astype(bf16).astype(f32)
    left = iota(tall.shape, 1) < 64
    one = jnp.where(left, first, second).astype(bf16)
    two = jnp.where(left, tall - first - second, 0.0).astype(bf16)
    bit, column = iota((256, 256), 0), iota((256, 256), 1)
    wide = (bit % 64 == column // 64).astype(f32).astype(bf16)
    for n in range(16):
        if n > 0:
            turned = [pltpu.roll(half, 128 - 4 * n, 1) for half in (one, two)]
        else:
            turned = [one, two]
        spread_ref[:, 256 * n : 256 * n + 256] = dot(jnp.concatenate(turned, axis=1), wide, 1, 0)

    starts = [accepted_ref[0] - 1, accepted_ref[1] - 1]
    ks, qs = [None] * 8, [None] * 8
    for i in range(32):
        at = slice(128 * i, 128 * i + 128)
        for j in range(2):
            start = prior_ref[j, starts[j], :, at]
            for row in range(4 * j, 4 * j + 4):
                kx = spread_ref[64 + 8 * row : 72 + 8 * row, at]
                qx = spread_ref[8 * row : 8 * row + 8, at]
                ks[row] = kx * start if i == 0 else ks[row] + kx * start
                qs[row] = qx * start if i == 0 else qs[row] + qx * start

    def fold(values):
        return values + pltpu.roll(values, 64, 1)

    ks = [k_norm[row] * fold(ks[row]) for row in ROWS]
    qs = [q_norm[row] * fold(qs[row]) for row in ROWS]
    kw, o = [None] * 8, [None] * 8
    for j in range(2):
        base = 4 * j
        grown = None
        for t in range(4):
            row = base + t
            carried = ks[row] if t == 0 else grown * ks[row]
            for e in range(t):
                reach = half_sum(k[row] * k[base + e]) * k_norm[row]
                for m in range(e + 1, t):
                    reach = reach * a[base + m]
                carried = carried + reach * kw[base + e]
            kw[row] = k_norm[row] * (b[row] * (v[row] - a[row] * carried))
            grown = a[row] if t == 0 else grown * a[row]
            out = grown * qs[row]
            for e in range(t + 1):
                reach = half_sum(q[row] * k[base + e]) * q_norm[row]
                for m in range(e + 1, t + 1):
                    reach = reach * a[base + m]
                out = out + reach * kw[base + e]
            o[row] = out

    for j in range(2):
        for i in range(32):
            at = slice(128 * i, 128 * i + 128)
            state = prior_ref[j, starts[j], :, at]
            for t in range(4):
                row = 4 * j + t
                state = a[row] * state + spread_ref[64 + 8 * row : 72 + 8 * row, at] * kw[row]
                states_ref[j, t, :, at] = state

    for row in ROWS:
        mean = half_sum(o[row] * o[row]) / 64
        n = o[row] * lax.rsqrt(mean + epsilon) * gain
        for p in range(4):
            nrows[row : row + 1, 128 * p : 128 * p + 128] = jnp.sum(
                jnp.where(masks[p], n, 0.0), axis=0, keepdims=True
            )
    rows = nrows[...]
    rows_ref[...] = jnp.concatenate([rows] * 8, axis=0).astype(bf16)


def mix_kernel(x_ref, rows_ref, out_ref):
    w = x_ref[...].reshape(256, 512)
    rows = rows_ref[...]
    out = dot(w, jnp.concatenate([rows, rows], axis=0), 1, 1)
    low = iota((16, 128), 1) < 64
    for r in range(8):
        piece = jnp.where(low, out[32 * r : 32 * r + 16], out[32 * r + 16 : 32 * r + 32])
        out_ref[2 * r] = piece.astype(bf16)
        out_ref[2 * r + 1] = piece.astype(bf16)


def place_kernel(x_ref, back_ref, states_ref, out_ref, kept_ref, sem):
    copies = [
        pltpu.make_async_copy(states_ref.at[n // 4, n % 4], kept_ref.at[n // 4, n % 4], sem.at[n])
        for n in range(8)
    ]
    for copy in copies:
        copy.start()
    low = iota((16, 128), 1) < 64
    sums = [x_ref[2 * r].astype(f32) + x_ref[2 * r + 1].astype(f32) for r in range(8)]
    tiles = []
    for p in range(4):
        a, b = sums[2 * p], sums[2 * p + 1]
        top = jnp.where(low, a, pltpu.roll(b, 64, 1))
        end = jnp.where(low, pltpu.roll(a, 64, 1), b)
        tiles.append(jnp.concatenate([top, end], axis=0).astype(bf16))
    whole = dot(jnp.concatenate(tiles, axis=1), back_ref[...], 1, 0).astype(bf16)
    for t in range(4):
        out_ref[t] = whole[:, 128 * t : 128 * t + 128]
    for copy in copies:
        copy.wait()


def back_table():
    dest = np.arange(512)
    group, rho = dest // 64, dest % 64
    wanted = (rho % 4) * 128 + (rho // 8) * 16 + group * 2 + (rho % 8) // 4
    return (wanted[:, None] == np.arange(512)[None, :]).astype(jnp.bfloat16)


def call(kernel, shapes, args, specs=None, scratch=(), outs=VMEM, name=None):
    if name == "pack":
        args = [pltpu.with_memory_space_constraint(a, pltpu.HBM) for a in args]
    return pl.pallas_call(
        kernel,
        out_shape=shapes,
        in_specs=specs or [VMEM] * len(args),
        out_specs=outs,
        scratch_shapes=scratch,
        compiler_params=pltpu.CompilerParams(vmem_limit_bytes=16 << 20),
        name=name,
    )(*args)


def shape(dims, dtype):
    return jax.ShapeDtypeStruct(dims, dtype)


def per_device(
    tokens,
    input_norm_gain,
    query_projection,
    key_projection,
    value_projection,
    write_strength_weight,
    decay_projection,
    head_decay_rate,
    token_extra_decay,
    accepted,
    prior_step_states,
    output_norm_gain,
    output_projection,
):
    def swap(x, axes):
        return lax.all_to_all(x, axes, 0, 0, tiled=True)

    part_shape, wo_shape = shape((64, WO), bf16), shape((8, 32, 512), bf16)

    def pack(late, args):
        sizes = (shape((8, 32, WO), bf16), wo_shape) if late else shape((8, 32, WIDE), bf16)
        return call(
            functools.partial(pack_kernel, late=late),
            sizes,
            args,
            specs=[HBM] * 8,
            scratch=[
                pltpu.VMEM((4, 32, 128), bf16),
                pltpu.VMEM((1, 32), f32),
                pltpu.VMEM((32, 512), bf16),
                pltpu.VMEM((32, 512), bf16),
                pltpu.VMEM((32, 512), bf16),
                pltpu.VMEM((8, 32), bf16),
                pltpu.VMEM((8, 32), bf16),
                pltpu.VMEM((32, 512), bf16),
                pltpu.SemaphoreType.DMA((8,)),
            ],
            outs=(VMEM, VMEM) if late else VMEM,
            name="pack",
        )

    def start_late(*args):
        packed, own = pack(True, args)
        return call(project_kernel, part_shape, (swap(packed, NEAR),), name="project"), own

    def start_early(*args):
        near = swap(pack(False, args), NEAR)
        return call(
            project_kernel, (part_shape, wo_shape), (near,), outs=(VMEM, VMEM), name="project"
        )

    def mix(weights, rows):
        return call(mix_kernel, shape((16, 16, 128), bf16), (weights, rows), name="mix")

    pair = lax.axis_index("z8")
    late = (pair >= 4) & (pair <= 6)
    part, weights = lax.cond(
        late,
        start_late,
        start_early,
        jnp.transpose(tokens, (1, 2, 0)),
        input_norm_gain[None, :],
        query_projection,
        key_projection,
        value_projection,
        write_strength_weight.T,
        decay_projection.T,
        output_projection.T,
    )
    arrived = swap(part.reshape(8, 8, part.shape[1]), "z8").reshape(part.shape)
    states, rows = call(
        delta_kernel,
        (shape(prior_step_states.shape, f32), shape((64, 512), bf16)),
        (
            accepted,
            arrived,
            prior_step_states,
            head_decay_rate[None, :],
            token_extra_decay,
            output_norm_gain[None, :],
        ),
        specs=[SMEM] + [VMEM] * 5,
        scratch=[
            pltpu.VMEM((8, 128), f32),
            pltpu.VMEM((8, 512), f32),
            pltpu.VMEM((128, 4096), f32),
        ],
        outs=(VMEM, VMEM),
        name="delta",
    )
    all_rows = swap(rows.reshape(8, 8, 512), "z8").reshape(64, 512)
    columns = lax.cond(
        late, lambda w, r: mix(swap(w, NEAR), r), lambda w, r: mix(w, r), weights, all_rows
    )
    back = swap(columns, ("zp", "y", "tp"))
    mixed, kept = call(
        place_kernel,
        (shape((4, 32, 128), bf16), shape(states.shape, f32)),
        (back, jnp.asarray(back_table()), states),
        scratch=[pltpu.SemaphoreType.DMA((8,))],
        outs=(VMEM, HBM),
        name="place",
    )
    return (jnp.transpose(mixed, (2, 0, 1)), kept)


def solution(mesh):
    split = Mesh(
        mesh.devices.reshape(mesh.shape["dp"], 8, 2, 4, mesh.shape["tp"]),
        ("dp", "z8", "zp", "y", "tp"),
    )
    in_specs = (
        P("dp", None, KV),
        P(KV),
        P(KV, "tp"),
        P(KV, "tp"),
        P(KV, "tp"),
        P(KV, "tp"),
        P(KV, "tp"),
        P("tp"),
        P(DP_KV, None, "tp"),
        P(DP_KV),
        P(DP_KV, None, "tp", None),
        P(),
        P("tp", KV),
    )
    out_specs = (P("dp", None, KV), P(DP_KV, None, "tp", None))
    return jax.shard_map(
        per_device, mesh=split, in_specs=in_specs, out_specs=out_specs, check_vma=False
    )
```

```python
import functools

import jax
import jax.numpy as jnp
import numpy as np
from jax import lax
from jax.experimental import pallas as pl
from jax.experimental.pallas import tpu as pltpu
from jax.sharding import Mesh
from jax.sharding import PartitionSpec as P

D = 2048
epsilon = 1e-06
KV = ("z8", "zp", "y")
DP_KV = ("dp", "z8", "zp", "y")
NEAR = ("zp", "y")
f32 = jnp.float32
bf16 = jnp.bfloat16

QKV, SMALL, WO, WIDE = 0, 1536, 1664, 2176
VMEM = pl.BlockSpec(memory_space=pltpu.VMEM)
SMEM = pl.BlockSpec(memory_space=pltpu.SMEM)
HBM = pl.BlockSpec(memory_space=pltpu.HBM)


def iota(shape, dim):
    return lax.broadcasted_iota(jnp.int32, shape, dim)


def dot(a, b, ca, cb):
    return lax.dot_general(a, b, (((ca,), (cb,)), ((), ())), preferred_element_type=f32)


def pack_kernel(*refs, late):
    hbm, out_ref, held, sems = refs[:8], refs[8], refs[-9:-1], refs[-1]
    copies = [pltpu.make_async_copy(hbm[n], held[n], sems.at[n]) for n in range(8)]
    for copy in copies:
        copy.start()
    tok_ref, gain_ref, q_ref, k_ref, v_ref, beta_ref, decay_ref, wo_ref = held
    source, dest = iota((512, 512), 0), iota((1, 512), 1)
    group, rho = dest // 64, dest % 64
    wanted = (rho % 4) * 128 + (rho // 8) * 16 + group * 2 + (rho % 8) // 4
    pick = (source == wanted).astype(f32).astype(bf16)
    eye = iota((32, 32), 0) == iota((32, 32), 1)
    head, lane = iota((8, 128), 0), iota((8, 128), 1)
    put_beta = ((lane == head) | (lane == head + 16)).astype(f32).astype(bf16)
    put_decay = ((lane == head + 8) | (lane == head + 24)).astype(f32).astype(bf16)
    for copy in copies:
        copy.wait()
    gain = jnp.sum(jnp.where(eye, gain_ref[...], 0.0), axis=1, keepdims=True)
    raw = dot(jnp.concatenate([tok_ref[t] for t in range(4)], axis=1), pick, 1, 0)
    scaled = raw * gain
    squares = jnp.sum(raw * raw, axis=0, keepdims=True)
    high = squares.astype(bf16).astype(f32)
    sub = iota((8, 512), 0)
    extra = jnp.where(sub < 2, high, jnp.where(sub < 4, squares - high, 0.0))
    small = dot(beta_ref[...], put_beta, 0, 0) + dot(decay_ref[...], put_decay, 0, 0)
    lane = iota((8, 128), 1)
    even = iota((8, 128), 0) % 2 == 0
    for r in range(8):
        at = slice(128 * (r // 2), 128 * (r // 2) + 128)
        sums = extra[:, at]
        if r % 2 == 0:
            cols = pltpu.roll(scaled[:, at], 64, 1)
            sums = jnp.where(even, pltpu.roll(sums, 32, 1), sums)
        else:
            cols = scaled[:, at]
            sums = jnp.where(even, pltpu.roll(sums, 96, 1), pltpu.roll(sums, 64, 1))
        groups = []
        for g in range(4):
            right = jnp.where(lane < 64, sums if g == 0 else 0.0, cols[8 * g : 8 * g + 8])
            groups.append(jnp.where(lane < 32, small[8 * g : 8 * g + 8], right))
        tile = jnp.concatenate(groups, axis=0)
        if late:
            refs[9][r] = wo_ref[...]
        else:
            out_ref[r, :, WO:] = wo_ref[...]
        out_ref[r, :, QKV : QKV + 512] = q_ref[...]
        out_ref[r, :, QKV + 512 : QKV + 1024] = k_ref[...]
        out_ref[r, :, QKV + 1024 : SMALL] = v_ref[...]
        out_ref[r, :, SMALL:WO] = tile.astype(bf16)


def project_kernel(x_ref, out_ref, *wo_refs):
    for wo_ref in wo_refs:
        wo_ref[...] = x_ref[:, :, WO:]
    x = x_ref[:, :, :WO].reshape(256, WO)
    cols = x[:, SMALL:]
    main = dot(cols, x[:, QKV:SMALL], 0, 0)
    out_ref[:, : SMALL - QKV] = main[64:].astype(bf16)
    sums = jnp.zeros((8, 128), f32)
    for r in range(8):
        sums = sums + cols[32 * r : 32 * r + 16].astype(f32)[0:8]
    sub, lane = iota((32, 128), 0), iota((32, 128), 1)
    halves = []
    for n in range(2):
        row = sums[n : n + 1] + sums[n + 2 : n + 3]
        halves.append(jnp.sum(jnp.where(lane == sub + 32, row, 0.0), axis=1, keepdims=True))
    total = jnp.concatenate(halves, axis=0)
    lane = iota((64, 128), 1)
    tail = jnp.where(lane < 32, dot(cols, cols, 0, 0)[64:], jnp.where(lane < 34, total, 0.0))
    first = tail.astype(bf16).astype(f32)
    keep = (lane < 16) | (lane == 32)
    out_ref[:, SMALL - QKV :] = jnp.where(keep, first, tail - first).astype(bf16)


def delta_kernel(
    accepted_ref, c_ref, prior_ref, rate_ref, extra_ref, gain_ref, states_ref, rows_ref,
    aux, nrows, spread_ref
):
    c = c_ref[...].astype(f32)
    s = (c[0:8] + c[8:16]) + (c[16:24] + c[24:32])
    s = s + ((c[32:40] + c[40:48]) + (c[48:56] + c[56:64]))
    tile = s[:, 1536:]
    total = tile[:, 32:33] + tile[:, 33:34]
    inverse = lax.rsqrt(total / D + epsilon)
    logits = jnp.transpose((tile + pltpu.roll(tile, 112, 1)) * inverse)
    aux[...] = jnp.zeros((8, 128), f32)
    aux[0:4, 0:8] = extra_ref[0]
    aux[4:8, 0:8] = extra_ref[1]
    aux[:, 8:16] = jnp.broadcast_to(rate_ref[...], (8, 8))
    side = jnp.transpose(aux[...])
    beta = jax.nn.sigmoid(logits[0:8])
    fade = jnp.exp(-side[8:16] * jax.nn.softplus(logits[8:16]) + side[0:8])

    sub, lane = iota((8, 128), 0), iota((8, 128), 1)
    masks = [sub == 2 * p + lane // 64 for p in range(4)]
    gain = jnp.concatenate([gain_ref[...], gain_ref[...]], axis=1)

    def silu_of(at):
        u = s[:, at : at + 512] * inverse
        return u / (1.0 + jnp.exp(-u))

    parts = [silu_of(0), silu_of(512), silu_of(1024)]

    def by_heads(values, row):
        m = jnp.zeros((8, 128), f32)
        for p in range(4):
            piece = jnp.broadcast_to(values[row : row + 1, 128 * p : 128 * p + 128], (8, 128))
            m = jnp.where(masks[p], piece, m)
        return m + pltpu.roll(m, 64, 1)

    def half_sum(values):
        return 0.5 * jnp.sum(values, axis=1, keepdims=True)

    def norm(values):
        return lax.rsqrt(half_sum(values * values) + epsilon)

    ROWS = range(8)
    q = [by_heads(parts[0], row) for row in ROWS]
    k = [by_heads(parts[1], row) for row in ROWS]
    v = [by_heads(parts[2], row) for row in ROWS]
    q_norm = [norm(values) * 0.125 for values in q]
    k_norm = [norm(values) for values in k]
    a = [jnp.broadcast_to(fade[:, row : row + 1], (8, 128)) for row in ROWS]
    b = [jnp.broadcast_to(beta[:, row : row + 1], (8, 128)) for row in ROWS]

    tall = jnp.concatenate(q + k, axis=0)
    first = tall.astype(bf16).astype(f32)
    second = (tall - first).astype(bf16).astype(f32)
    left = iota(tall.shape, 1) < 64
    one = jnp.where(left, first, second).astype(bf16)
    two = jnp.where(left, tall - first - second, 0.0).astype(bf16)
    bit, column = iota((256, 256), 0), iota((256, 256), 1)
    wide = (bit % 64 == column // 64).astype(f32).astype(bf16)
    for n in range(16):
        if n > 0:
            turned = [pltpu.roll(half, 128 - 4 * n, 1) for half in (one, two)]
        else:
            turned = [one, two]
        spread_ref[:, 256 * n : 256 * n + 256] = dot(jnp.concatenate(turned, axis=1), wide, 1, 0)

    starts = [accepted_ref[0] - 1, accepted_ref[1] - 1]
    ks, qs = [None] * 8, [None] * 8
    for i in range(32):
        at = slice(128 * i, 128 * i + 128)
        for j in range(2):
            start = prior_ref[j, starts[j], :, at]
            for row in range(4 * j, 4 * j + 4):
                kx = spread_ref[64 + 8 * row : 72 + 8 * row, at]
                qx = spread_ref[8 * row : 8 * row + 8, at]
                ks[row] = kx * start if i == 0 else ks[row] + kx * start
                qs[row] = qx * start if i == 0 else qs[row] + qx * start

    def fold(values):
        return values + pltpu.roll(values, 64, 1)

    ks = [k_norm[row] * fold(ks[row]) for row in ROWS]
    qs = [q_norm[row] * fold(qs[row]) for row in ROWS]
    kw, o = [None] * 8, [None] * 8
    for j in range(2):
        base = 4 * j
        grown = None
        for t in range(4):
            row = base + t
            carried = ks[row] if t == 0 else grown * ks[row]
            for e in range(t):
                reach = half_sum(k[row] * k[base + e]) * k_norm[row]
                for m in range(e + 1, t):
                    reach = reach * a[base + m]
                carried = carried + reach * kw[base + e]
            kw[row] = k_norm[row] * (b[row] * (v[row] - a[row] * carried))
            grown = a[row] if t == 0 else grown * a[row]
            out = grown * qs[row]
            for e in range(t + 1):
                reach = half_sum(q[row] * k[base + e]) * q_norm[row]
                for m in range(e + 1, t + 1):
                    reach = reach * a[base + m]
                out = out + reach * kw[base + e]
            o[row] = out

    for j in range(2):
        for i in range(32):
            at = slice(128 * i, 128 * i + 128)
            state = prior_ref[j, starts[j], :, at]
            for t in range(4):
                row = 4 * j + t
                state = a[row] * state + spread_ref[64 + 8 * row : 72 + 8 * row, at] * kw[row]
                states_ref[j, t, :, at] = state

    for row in ROWS:
        mean = half_sum(o[row] * o[row]) / 64
        n = o[row] * lax.rsqrt(mean + epsilon) * gain
        for p in range(4):
            nrows[row : row + 1, 128 * p : 128 * p + 128] = jnp.sum(
                jnp.where(masks[p], n, 0.0), axis=0, keepdims=True
            )
    rows = nrows[...]
    rows_ref[...] = jnp.concatenate([rows] * 8, axis=0).astype(bf16)


def mix_kernel(x_ref, rows_ref, out_ref):
    w = x_ref[...].reshape(256, 512)
    rows = rows_ref[...]
    out = dot(w, jnp.concatenate([rows, rows], axis=0), 1, 1)
    low = iota((16, 128), 1) < 64
    for r in range(8):
        piece = jnp.where(low, out[32 * r : 32 * r + 16], out[32 * r + 16 : 32 * r + 32])
        out_ref[2 * r] = piece.astype(bf16)
        out_ref[2 * r + 1] = piece.astype(bf16)


def place_kernel(x_ref, back_ref, states_ref, out_ref, kept_ref, sem):
    copies = [
        pltpu.make_async_copy(states_ref.at[n // 4, n % 4], kept_ref.at[n // 4, n % 4], sem.at[n])
        for n in range(8)
    ]
    for copy in copies:
        copy.start()
    low = iota((16, 128), 1) < 64
    sums = [x_ref[2 * r].astype(f32) + x_ref[2 * r + 1].astype(f32) for r in range(8)]
    tiles = []
    for p in range(4):
        a, b = sums[2 * p], sums[2 * p + 1]
        top = jnp.where(low, a, pltpu.roll(b, 64, 1))
        end = jnp.where(low, pltpu.roll(a, 64, 1), b)
        tiles.append(jnp.concatenate([top, end], axis=0).astype(bf16))
    whole = dot(jnp.concatenate(tiles, axis=1), back_ref[...], 1, 0).astype(bf16)
    for t in range(4):
        out_ref[t] = whole[:, 128 * t : 128 * t + 128]
    for copy in copies:
        copy.wait()


def back_table():
    dest = np.arange(512)
    group, rho = dest // 64, dest % 64
    wanted = (rho % 4) * 128 + (rho // 8) * 16 + group * 2 + (rho % 8) // 4
    return (wanted[:, None] == np.arange(512)[None, :]).astype(jnp.bfloat16)


def call(kernel, shapes, args, specs=None, scratch=(), outs=VMEM, name=None):
    if name == "pack":
        args = [pltpu.with_memory_space_constraint(a, pltpu.HBM) for a in args]
    return pl.pallas_call(
        kernel,
        out_shape=shapes,
        in_specs=specs or [VMEM] * len(args),
        out_specs=outs,
        scratch_shapes=scratch,
        compiler_params=pltpu.CompilerParams(vmem_limit_bytes=16 << 20),
        name=name,
    )(*args)


def shape(dims, dtype):
    return jax.ShapeDtypeStruct(dims, dtype)


def per_device(
    tokens,
    input_norm_gain,
    query_projection,
    key_projection,
    value_projection,
    write_strength_weight,
    decay_projection,
    head_decay_rate,
    token_extra_decay,
    accepted,
    prior_step_states,
    output_norm_gain,
    output_projection,
):
    def swap(x, axes):
        return lax.all_to_all(x, axes, 0, 0, tiled=True)

    part_shape, wo_shape = shape((64, WO), bf16), shape((8, 32, 512), bf16)

    def pack(late, args):
        sizes = (shape((8, 32, WO), bf16), wo_shape) if late else shape((8, 32, WIDE), bf16)
        return call(
            functools.partial(pack_kernel, late=late),
            sizes,
            args,
            specs=[HBM] * 8,
            scratch=[
                pltpu.VMEM((4, 32, 128), bf16),
                pltpu.VMEM((1, 32), f32),
                pltpu.VMEM((32, 512), bf16),
                pltpu.VMEM((32, 512), bf16),
                pltpu.VMEM((32, 512), bf16),
                pltpu.VMEM((8, 32), bf16),
                pltpu.VMEM((8, 32), bf16),
                pltpu.VMEM((32, 512), bf16),
                pltpu.SemaphoreType.DMA((8,)),
            ],
            outs=(VMEM, VMEM) if late else VMEM,
            name="pack",
        )

    def start_late(*args):
        packed, own = pack(True, args)
        return call(project_kernel, part_shape, (swap(packed, NEAR),), name="project"), own

    def start_early(*args):
        near = swap(pack(False, args), NEAR)
        return call(
            project_kernel, (part_shape, wo_shape), (near,), outs=(VMEM, VMEM), name="project"
        )

    def mix(weights, rows):
        return call(mix_kernel, shape((16, 16, 128), bf16), (weights, rows), name="mix")

    pair = lax.axis_index("z8")
    late = pair >= 3
    part, weights = lax.cond(
        late,
        start_late,
        start_early,
        jnp.transpose(tokens, (1, 2, 0)),
        input_norm_gain[None, :],
        query_projection,
        key_projection,
        value_projection,
        write_strength_weight.T,
        decay_projection.T,
        output_projection.T,
    )
    arrived = swap(part.reshape(8, 8, part.shape[1]), "z8").reshape(part.shape)
    states, rows = call(
        delta_kernel,
        (shape(prior_step_states.shape, f32), shape((64, 512), bf16)),
        (
            accepted,
            arrived,
            prior_step_states,
            head_decay_rate[None, :],
            token_extra_decay,
            output_norm_gain[None, :],
        ),
        specs=[SMEM] + [VMEM] * 5,
        scratch=[
            pltpu.VMEM((8, 128), f32),
            pltpu.VMEM((8, 512), f32),
            pltpu.VMEM((128, 4096), f32),
        ],
        outs=(VMEM, VMEM),
        name="delta",
    )
    all_rows = swap(rows.reshape(8, 8, 512), "z8").reshape(64, 512)
    columns = lax.cond(
        late, lambda w, r: mix(swap(w, NEAR), r), lambda w, r: mix(w, r), weights, all_rows
    )
    back = swap(columns, ("zp", "y", "tp"))
    mixed, kept = call(
        place_kernel,
        (shape((4, 32, 128), bf16), shape(states.shape, f32)),
        (back, jnp.asarray(back_table()), states),
        scratch=[pltpu.SemaphoreType.DMA((8,))],
        outs=(VMEM, HBM),
        name="place",
    )
    return (jnp.transpose(mixed, (2, 0, 1)), kept)


def solution(mesh):
    split = Mesh(
        mesh.devices.reshape(mesh.shape["dp"], 8, 2, 4, mesh.shape["tp"]),
        ("dp", "z8", "zp", "y", "tp"),
    )
    in_specs = (
        P("dp", None, KV),
        P(KV),
        P(KV, "tp"),
        P(KV, "tp"),
        P(KV, "tp"),
        P(KV, "tp"),
        P(KV, "tp"),
        P("tp"),
        P(DP_KV, None, "tp"),
        P(DP_KV),
        P(DP_KV, None, "tp", None),
        P(),
        P("tp", KV),
    )
    out_specs = (P("dp", None, KV), P(DP_KV, None, "tp", None))
    return jax.shard_map(
        per_device, mesh=split, in_specs=in_specs, out_specs=out_specs, check_vma=False
    )
```

```python
import functools

import jax
import jax.numpy as jnp
import numpy as np
from jax import lax
from jax.experimental import pallas as pl
from jax.experimental.pallas import tpu as pltpu
from jax.sharding import Mesh
from jax.sharding import PartitionSpec as P

D = 2048
epsilon = 1e-06
KV = ("z8", "zp", "y")
DP_KV = ("dp", "z8", "zp", "y")
NEAR = ("y", "zp")
f32 = jnp.float32
bf16 = jnp.bfloat16

QKV, SMALL, WO, WIDE = 0, 1536, 1664, 2176
VMEM = pl.BlockSpec(memory_space=pltpu.VMEM)
SMEM = pl.BlockSpec(memory_space=pltpu.SMEM)
HBM = pl.BlockSpec(memory_space=pltpu.HBM)


def iota(shape, dim):
    return lax.broadcasted_iota(jnp.int32, shape, dim)


def dot(a, b, ca, cb):
    return lax.dot_general(a, b, (((ca,), (cb,)), ((), ())), preferred_element_type=f32)


def pack_kernel(*refs, late):
    hbm, out_ref, held, sems = refs[:8], refs[8], refs[-9:-1], refs[-1]
    copies = [pltpu.make_async_copy(hbm[n], held[n], sems.at[n]) for n in range(8)]
    for copy in copies:
        copy.start()
    tok_ref, gain_ref, q_ref, k_ref, v_ref, beta_ref, decay_ref, wo_ref = held
    source, dest = iota((512, 512), 0), iota((1, 512), 1)
    group, rho = dest // 64, dest % 64
    group = (group % 2) * 4 + group // 2
    wanted = (rho % 4) * 128 + (rho // 8) * 16 + group * 2 + (rho % 8) // 4
    pick = (source == wanted).astype(f32).astype(bf16)
    eye = iota((32, 32), 0) == iota((32, 32), 1)
    head, lane = iota((8, 128), 0), iota((8, 128), 1)
    put_beta = ((lane == head) | (lane == head + 16)).astype(f32).astype(bf16)
    put_decay = ((lane == head + 8) | (lane == head + 24)).astype(f32).astype(bf16)
    for copy in copies:
        copy.wait()
    gain = jnp.sum(jnp.where(eye, gain_ref[...], 0.0), axis=1, keepdims=True)
    raw = dot(jnp.concatenate([tok_ref[t] for t in range(4)], axis=1), pick, 1, 0)
    scaled = raw * gain
    squares = jnp.sum(raw * raw, axis=0, keepdims=True)
    high = squares.astype(bf16).astype(f32)
    sub = iota((8, 512), 0)
    extra = jnp.where(sub < 2, high, jnp.where(sub < 4, squares - high, 0.0))
    small = dot(beta_ref[...], put_beta, 0, 0) + dot(decay_ref[...], put_decay, 0, 0)
    lane = iota((8, 128), 1)
    even = iota((8, 128), 0) % 2 == 0
    for r in range(8):
        at = slice(128 * (r // 2), 128 * (r // 2) + 128)
        sums = extra[:, at]
        if r % 2 == 0:
            cols = pltpu.roll(scaled[:, at], 64, 1)
            sums = jnp.where(even, pltpu.roll(sums, 32, 1), sums)
        else:
            cols = scaled[:, at]
            sums = jnp.where(even, pltpu.roll(sums, 96, 1), pltpu.roll(sums, 64, 1))
        groups = []
        for g in range(4):
            right = jnp.where(lane < 64, sums if g == 0 else 0.0, cols[8 * g : 8 * g + 8])
            groups.append(jnp.where(lane < 32, small[8 * g : 8 * g + 8], right))
        tile = jnp.concatenate(groups, axis=0)
        if late:
            refs[9][r] = wo_ref[...]
        else:
            out_ref[r, :, WO:] = wo_ref[...]
        out_ref[r, :, QKV : QKV + 512] = q_ref[...]
        out_ref[r, :, QKV + 512 : QKV + 1024] = k_ref[...]
        out_ref[r, :, QKV + 1024 : SMALL] = v_ref[...]
        out_ref[r, :, SMALL:WO] = tile.astype(bf16)


def project_kernel(x_ref, out_ref, *wo_refs):
    for wo_ref in wo_refs:
        wo_ref[...] = x_ref[:, :, WO:]
    x = x_ref[:, :, :WO].reshape(256, WO)
    cols = x[:, SMALL:]
    main = dot(cols, x[:, QKV:SMALL], 0, 0)
    out_ref[:, : SMALL - QKV] = main[64:].astype(bf16)
    sums = jnp.zeros((8, 128), f32)
    for r in range(8):
        sums = sums + cols[32 * r : 32 * r + 16].astype(f32)[0:8]
    sub, lane = iota((32, 128), 0), iota((32, 128), 1)
    halves = []
    for n in range(2):
        row = sums[n : n + 1] + sums[n + 2 : n + 3]
        halves.append(jnp.sum(jnp.where(lane == sub + 32, row, 0.0), axis=1, keepdims=True))
    total = jnp.concatenate(halves, axis=0)
    lane = iota((64, 128), 1)
    tail = jnp.where(lane < 32, dot(cols, cols, 0, 0)[64:], jnp.where(lane < 34, total, 0.0))
    first = tail.astype(bf16).astype(f32)
    keep = (lane < 16) | (lane == 32)
    out_ref[:, SMALL - QKV :] = jnp.where(keep, first, tail - first).astype(bf16)


def delta_kernel(
    accepted_ref, c_ref, prior_ref, rate_ref, extra_ref, gain_ref, states_ref, rows_ref,
    aux, nrows, spread_ref
):
    c = c_ref[...].astype(f32)
    s = (c[0:8] + c[8:16]) + (c[16:24] + c[24:32])
    s = s + ((c[32:40] + c[40:48]) + (c[48:56] + c[56:64]))
    tile = s[:, 1536:]
    total = tile[:, 32:33] + tile[:, 33:34]
    inverse = lax.rsqrt(total / D + epsilon)
    logits = jnp.transpose((tile + pltpu.roll(tile, 112, 1)) * inverse)
    aux[...] = jnp.zeros((8, 128), f32)
    aux[0:4, 0:8] = extra_ref[0]
    aux[4:8, 0:8] = extra_ref[1]
    aux[:, 8:16] = jnp.broadcast_to(rate_ref[...], (8, 8))
    side = jnp.transpose(aux[...])
    beta = jax.nn.sigmoid(logits[0:8])
    fade = jnp.exp(-side[8:16] * jax.nn.softplus(logits[8:16]) + side[0:8])

    sub, lane = iota((8, 128), 0), iota((8, 128), 1)
    masks = [sub == 2 * p + lane // 64 for p in range(4)]
    gain = jnp.concatenate([gain_ref[...], gain_ref[...]], axis=1)

    def silu_of(at):
        u = s[:, at : at + 512] * inverse
        return u / (1.0 + jnp.exp(-u))

    parts = [silu_of(0), silu_of(512), silu_of(1024)]

    def by_heads(values, row):
        m = jnp.zeros((8, 128), f32)
        for p in range(4):
            piece = jnp.broadcast_to(values[row : row + 1, 128 * p : 128 * p + 128], (8, 128))
            m = jnp.where(masks[p], piece, m)
        return m + pltpu.roll(m, 64, 1)

    def half_sum(values):
        return 0.5 * jnp.sum(values, axis=1, keepdims=True)

    def norm(values):
        return lax.rsqrt(half_sum(values * values) + epsilon)

    ROWS = range(8)
    q = [by_heads(parts[0], row) for row in ROWS]
    k = [by_heads(parts[1], row) for row in ROWS]
    v = [by_heads(parts[2], row) for row in ROWS]
    q_norm = [norm(values) * 0.125 for values in q]
    k_norm = [norm(values) for values in k]
    a = [jnp.broadcast_to(fade[:, row : row + 1], (8, 128)) for row in ROWS]
    b = [jnp.broadcast_to(beta[:, row : row + 1], (8, 128)) for row in ROWS]

    tall = jnp.concatenate(q + k, axis=0)
    first = tall.astype(bf16).astype(f32)
    second = (tall - first).astype(bf16).astype(f32)
    left = iota(tall.shape, 1) < 64
    one = jnp.where(left, first, second).astype(bf16)
    two = jnp.where(left, tall - first - second, 0.0).astype(bf16)
    bit, column = iota((256, 256), 0), iota((256, 256), 1)
    wide = (bit % 64 == column // 64).astype(f32).astype(bf16)
    for n in range(16):
        if n > 0:
            turned = [pltpu.roll(half, 128 - 4 * n, 1) for half in (one, two)]
        else:
            turned = [one, two]
        spread_ref[:, 256 * n : 256 * n + 256] = dot(jnp.concatenate(turned, axis=1), wide, 1, 0)

    starts = [accepted_ref[0] - 1, accepted_ref[1] - 1]
    ks, qs = [None] * 8, [None] * 8
    for i in range(32):
        at = slice(128 * i, 128 * i + 128)
        for j in range(2):
            start = prior_ref[j, starts[j], :, at]
            for row in range(4 * j, 4 * j + 4):
                kx = spread_ref[64 + 8 * row : 72 + 8 * row, at]
                qx = spread_ref[8 * row : 8 * row + 8, at]
                ks[row] = kx * start if i == 0 else ks[row] + kx * start
                qs[row] = qx * start if i == 0 else qs[row] + qx * start

    def fold(values):
        return values + pltpu.roll(values, 64, 1)

    ks = [k_norm[row] * fold(ks[row]) for row in ROWS]
    qs = [q_norm[row] * fold(qs[row]) for row in ROWS]
    kw, o = [None] * 8, [None] * 8
    for j in range(2):
        base = 4 * j
        grown = None
        for t in range(4):
            row = base + t
            carried = ks[row] if t == 0 else grown * ks[row]
            for e in range(t):
                reach = half_sum(k[row] * k[base + e]) * k_norm[row]
                for m in range(e + 1, t):
                    reach = reach * a[base + m]
                carried = carried + reach * kw[base + e]
            kw[row] = k_norm[row] * (b[row] * (v[row] - a[row] * carried))
            grown = a[row] if t == 0 else grown * a[row]
            out = grown * qs[row]
            for e in range(t + 1):
                reach = half_sum(q[row] * k[base + e]) * q_norm[row]
                for m in range(e + 1, t + 1):
                    reach = reach * a[base + m]
                out = out + reach * kw[base + e]
            o[row] = out

    for j in range(2):
        for i in range(32):
            at = slice(128 * i, 128 * i + 128)
            state = prior_ref[j, starts[j], :, at]
            for t in range(4):
                row = 4 * j + t
                state = a[row] * state + spread_ref[64 + 8 * row : 72 + 8 * row, at] * kw[row]
                states_ref[j, t, :, at] = state

    for row in ROWS:
        mean = half_sum(o[row] * o[row]) / 64
        n = o[row] * lax.rsqrt(mean + epsilon) * gain
        for p in range(4):
            nrows[row : row + 1, 128 * p : 128 * p + 128] = jnp.sum(
                jnp.where(masks[p], n, 0.0), axis=0, keepdims=True
            )
    rows = nrows[...]
    rows_ref[...] = jnp.concatenate([rows] * 8, axis=0).astype(bf16)


def mix_kernel(x_ref, rows_ref, out_ref):
    w = x_ref[...].reshape(256, 512)
    rows = rows_ref[...]
    out = dot(w, jnp.concatenate([rows, rows], axis=0), 1, 1)
    low = iota((16, 128), 1) < 64
    for r in range(8):
        piece = jnp.where(low, out[32 * r : 32 * r + 16], out[32 * r + 16 : 32 * r + 32])
        out_ref[2 * r] = piece.astype(bf16)
        out_ref[2 * r + 1] = piece.astype(bf16)


def place_kernel(x_ref, back_ref, states_ref, out_ref, kept_ref, sem):
    copies = [
        pltpu.make_async_copy(states_ref.at[n // 4, n % 4], kept_ref.at[n // 4, n % 4], sem.at[n])
        for n in range(8)
    ]
    for copy in copies:
        copy.start()
    low = iota((16, 128), 1) < 64
    sums = [x_ref[2 * r].astype(f32) + x_ref[2 * r + 1].astype(f32) for r in range(8)]
    tiles = []
    for p in range(4):
        a, b = sums[2 * p], sums[2 * p + 1]
        top = jnp.where(low, a, pltpu.roll(b, 64, 1))
        end = jnp.where(low, pltpu.roll(a, 64, 1), b)
        tiles.append(jnp.concatenate([top, end], axis=0).astype(bf16))
    whole = dot(jnp.concatenate(tiles, axis=1), back_ref[...], 1, 0).astype(bf16)
    for t in range(4):
        out_ref[t] = whole[:, 128 * t : 128 * t + 128]
    for copy in copies:
        copy.wait()


def back_table():
    dest = np.arange(512)
    group, rho = dest // 64, dest % 64
    group = (group % 2) * 4 + group // 2
    wanted = (rho % 4) * 128 + (rho // 8) * 16 + group * 2 + (rho % 8) // 4
    return (wanted[:, None] == np.arange(512)[None, :]).astype(jnp.bfloat16)


def call(kernel, shapes, args, specs=None, scratch=(), outs=VMEM, name=None):
    if name == "pack":
        args = [pltpu.with_memory_space_constraint(a, pltpu.HBM) for a in args]
    return pl.pallas_call(
        kernel,
        out_shape=shapes,
        in_specs=specs or [VMEM] * len(args),
        out_specs=outs,
        scratch_shapes=scratch,
        compiler_params=pltpu.CompilerParams(vmem_limit_bytes=16 << 20),
        name=name,
    )(*args)


def shape(dims, dtype):
    return jax.ShapeDtypeStruct(dims, dtype)


def per_device(
    tokens,
    input_norm_gain,
    query_projection,
    key_projection,
    value_projection,
    write_strength_weight,
    decay_projection,
    head_decay_rate,
    token_extra_decay,
    accepted,
    prior_step_states,
    output_norm_gain,
    output_projection,
):
    def swap(x, axes):
        return lax.all_to_all(x, axes, 0, 0, tiled=True)

    part_shape, wo_shape = shape((64, WO), bf16), shape((8, 32, 512), bf16)

    def pack(late, args):
        sizes = (shape((8, 32, WO), bf16), wo_shape) if late else shape((8, 32, WIDE), bf16)
        return call(
            functools.partial(pack_kernel, late=late),
            sizes,
            args,
            specs=[HBM] * 8,
            scratch=[
                pltpu.VMEM((4, 32, 128), bf16),
                pltpu.VMEM((1, 32), f32),
                pltpu.VMEM((32, 512), bf16),
                pltpu.VMEM((32, 512), bf16),
                pltpu.VMEM((32, 512), bf16),
                pltpu.VMEM((8, 32), bf16),
                pltpu.VMEM((8, 32), bf16),
                pltpu.VMEM((32, 512), bf16),
                pltpu.SemaphoreType.DMA((8,)),
            ],
            outs=(VMEM, VMEM) if late else VMEM,
            name="pack",
        )

    def start_late(*args):
        packed, own = pack(True, args)
        return call(project_kernel, part_shape, (swap(packed, NEAR),), name="project"), own

    def start_early(*args):
        near = swap(pack(False, args), NEAR)
        return call(
            project_kernel, (part_shape, wo_shape), (near,), outs=(VMEM, VMEM), name="project"
        )

    def mix(weights, rows):
        return call(mix_kernel, shape((16, 16, 128), bf16), (weights, rows), name="mix")

    pair = lax.axis_index("z8")
    late = (pair >= 4) & (pair <= 6)
    part, weights = lax.cond(
        late,
        start_late,
        start_early,
        jnp.transpose(tokens, (1, 2, 0)),
        input_norm_gain[None, :],
        query_projection,
        key_projection,
        value_projection,
        write_strength_weight.T,
        decay_projection.T,
        output_projection.T,
    )
    arrived = swap(part.reshape(8, 8, part.shape[1]), "z8").reshape(part.shape)
    states, rows = call(
        delta_kernel,
        (shape(prior_step_states.shape, f32), shape((64, 512), bf16)),
        (
            accepted,
            arrived,
            prior_step_states,
            head_decay_rate[None, :],
            token_extra_decay,
            output_norm_gain[None, :],
        ),
        specs=[SMEM] + [VMEM] * 5,
        scratch=[
            pltpu.VMEM((8, 128), f32),
            pltpu.VMEM((8, 512), f32),
            pltpu.VMEM((128, 4096), f32),
        ],
        outs=(VMEM, VMEM),
        name="delta",
    )
    all_rows = swap(rows.reshape(8, 8, 512), "z8").reshape(64, 512)
    columns = lax.cond(
        late, lambda w, r: mix(swap(w, NEAR), r), lambda w, r: mix(w, r), weights, all_rows
    )
    back = swap(columns, ("y", "zp", "tp"))
    mixed, kept = call(
        place_kernel,
        (shape((4, 32, 128), bf16), shape(states.shape, f32)),
        (back, jnp.asarray(back_table()), states),
        scratch=[pltpu.SemaphoreType.DMA((8,))],
        outs=(VMEM, HBM),
        name="place",
    )
    return (jnp.transpose(mixed, (2, 0, 1)), kept)


def solution(mesh):
    split = Mesh(
        mesh.devices.reshape(mesh.shape["dp"], 8, 2, 4, mesh.shape["tp"]),
        ("dp", "z8", "zp", "y", "tp"),
    )
    in_specs = (
        P("dp", None, KV),
        P(KV),
        P(KV, "tp"),
        P(KV, "tp"),
        P(KV, "tp"),
        P(KV, "tp"),
        P(KV, "tp"),
        P("tp"),
        P(DP_KV, None, "tp"),
        P(DP_KV),
        P(DP_KV, None, "tp", None),
        P(),
        P("tp", KV),
    )
    out_specs = (P("dp", None, KV), P(DP_KV, None, "tp", None))
    return jax.shard_map(
        per_device, mesh=split, in_specs=in_specs, out_specs=out_specs, check_vma=False
    )
```

```python
import functools

import jax
import jax.numpy as jnp
import numpy as np
from jax import lax
from jax.experimental import pallas as pl
from jax.experimental.pallas import tpu as pltpu
from jax.sharding import Mesh
from jax.sharding import PartitionSpec as P

D = 2048
epsilon = 1e-06
KV = ("z8", "zp", "y")
DP_KV = ("dp", "z8", "zp", "y")
NEAR = ("y", "zp")
f32 = jnp.float32
bf16 = jnp.bfloat16

QKV, SMALL, WO, WIDE = 0, 1536, 1664, 2176
VMEM = pl.BlockSpec(memory_space=pltpu.VMEM)
SMEM = pl.BlockSpec(memory_space=pltpu.SMEM)
HBM = pl.BlockSpec(memory_space=pltpu.HBM)


def iota(shape, dim):
    return lax.broadcasted_iota(jnp.int32, shape, dim)


def dot(a, b, ca, cb):
    return lax.dot_general(a, b, (((ca,), (cb,)), ((), ())), preferred_element_type=f32)


def pack_kernel(*refs, late):
    hbm, out_ref, held, sems = refs[:8], refs[8], refs[-9:-1], refs[-1]
    copies = [pltpu.make_async_copy(hbm[n], held[n], sems.at[n]) for n in range(8)]
    for copy in copies:
        copy.start()
    tok_ref, gain_ref, q_ref, k_ref, v_ref, beta_ref, decay_ref, wo_ref = held
    source, dest = iota((512, 512), 0), iota((1, 512), 1)
    group, rho = dest // 64, dest % 64
    group = (group % 2) * 4 + group // 2
    wanted = (rho % 4) * 128 + (rho // 8) * 16 + group * 2 + (rho % 8) // 4
    pick = (source == wanted).astype(f32).astype(bf16)
    eye = iota((32, 32), 0) == iota((32, 32), 1)
    head, lane = iota((8, 128), 0), iota((8, 128), 1)
    put_beta = ((lane == head) | (lane == head + 16)).astype(f32).astype(bf16)
    put_decay = ((lane == head + 8) | (lane == head + 24)).astype(f32).astype(bf16)
    for copy in copies:
        copy.wait()
    gain = jnp.sum(jnp.where(eye, gain_ref[...], 0.0), axis=1, keepdims=True)
    raw = dot(jnp.concatenate([tok_ref[t] for t in range(4)], axis=1), pick, 1, 0)
    scaled = raw * gain
    squares = jnp.sum(raw * raw, axis=0, keepdims=True)
    high = squares.astype(bf16).astype(f32)
    sub = iota((8, 512), 0)
    extra = jnp.where(sub < 2, high, jnp.where(sub < 4, squares - high, 0.0))
    small = dot(beta_ref[...], put_beta, 0, 0) + dot(decay_ref[...], put_decay, 0, 0)
    lane = iota((8, 128), 1)
    even = iota((8, 128), 0) % 2 == 0
    for r in range(8):
        at = slice(128 * (r // 2), 128 * (r // 2) + 128)
        sums = extra[:, at]
        if r % 2 == 0:
            cols = pltpu.roll(scaled[:, at], 64, 1)
            sums = jnp.where(even, pltpu.roll(sums, 32, 1), sums)
        else:
            cols = scaled[:, at]
            sums = jnp.where(even, pltpu.roll(sums, 96, 1), pltpu.roll(sums, 64, 1))
        groups = []
        for g in range(4):
            right = jnp.where(lane < 64, sums if g == 0 else 0.0, cols[8 * g : 8 * g + 8])
            groups.append(jnp.where(lane < 32, small[8 * g : 8 * g + 8], right))
        tile = jnp.concatenate(groups, axis=0)
        if late:
            refs[9][r] = wo_ref[...]
        else:
            out_ref[r, :, WO:] = wo_ref[...]
        out_ref[r, :, QKV : QKV + 512] = q_ref[...]
        out_ref[r, :, QKV + 512 : QKV + 1024] = k_ref[...]
        out_ref[r, :, QKV + 1024 : SMALL] = v_ref[...]
        out_ref[r, :, SMALL:WO] = tile.astype(bf16)


def project_kernel(x_ref, out_ref, *wo_refs):
    for wo_ref in wo_refs:
        wo_ref[...] = x_ref[:, :, WO:]
    x = x_ref[:, :, :WO].reshape(256, WO)
    cols = x[:, SMALL:]
    main = dot(cols, x[:, QKV:SMALL], 0, 0)
    out_ref[:, : SMALL - QKV] = main[64:].astype(bf16)
    sums = jnp.zeros((8, 128), f32)
    for r in range(8):
        sums = sums + cols[32 * r : 32 * r + 16].astype(f32)[0:8]
    sub, lane = iota((32, 128), 0), iota((32, 128), 1)
    halves = []
    for n in range(2):
        row = sums[n : n + 1] + sums[n + 2 : n + 3]
        halves.append(jnp.sum(jnp.where(lane == sub + 32, row, 0.0), axis=1, keepdims=True))
    total = jnp.concatenate(halves, axis=0)
    lane = iota((64, 128), 1)
    tail = jnp.where(lane < 32, dot(cols, cols, 0, 0)[64:], jnp.where(lane < 34, total, 0.0))
    first = tail.astype(bf16).astype(f32)
    keep = (lane < 16) | (lane == 32)
    out_ref[:, SMALL - QKV :] = jnp.where(keep, first, tail - first).astype(bf16)


def delta_kernel(
    accepted_ref, c_ref, prior_ref, rate_ref, extra_ref, gain_ref, states_ref, rows_ref,
    aux, nrows, spread_ref
):
    c = c_ref[...].astype(f32)
    s = (c[0:8] + c[8:16]) + (c[16:24] + c[24:32])
    s = s + ((c[32:40] + c[40:48]) + (c[48:56] + c[56:64]))
    tile = s[:, 1536:]
    total = tile[:, 32:33] + tile[:, 33:34]
    inverse = lax.rsqrt(total / D + epsilon)
    logits = jnp.transpose((tile + pltpu.roll(tile, 112, 1)) * inverse)
    aux[...] = jnp.zeros((8, 128), f32)
    aux[0:4, 0:8] = extra_ref[0]
    aux[4:8, 0:8] = extra_ref[1]
    aux[:, 8:16] = jnp.broadcast_to(rate_ref[...], (8, 8))
    side = jnp.transpose(aux[...])
    beta = jax.nn.sigmoid(logits[0:8])
    fade = jnp.exp(-side[8:16] * jax.nn.softplus(logits[8:16]) + side[0:8])

    sub, lane = iota((8, 128), 0), iota((8, 128), 1)
    masks = [sub == 2 * p + lane // 64 for p in range(4)]
    gain = jnp.concatenate([gain_ref[...], gain_ref[...]], axis=1)

    def silu_of(at):
        u = s[:, at : at + 512] * inverse
        return u / (1.0 + jnp.exp(-u))

    parts = [silu_of(0), silu_of(512), silu_of(1024)]

    def by_heads(values, row):
        m = jnp.zeros((8, 128), f32)
        for p in range(4):
            piece = jnp.broadcast_to(values[row : row + 1, 128 * p : 128 * p + 128], (8, 128))
            m = jnp.where(masks[p], piece, m)
        return m + pltpu.roll(m, 64, 1)

    def half_sum(values):
        return 0.5 * jnp.sum(values, axis=1, keepdims=True)

    def norm(values):
        return lax.rsqrt(half_sum(values * values) + epsilon)

    ROWS = range(8)
    q = [by_heads(parts[0], row) for row in ROWS]
    k = [by_heads(parts[1], row) for row in ROWS]
    v = [by_heads(parts[2], row) for row in ROWS]
    q_norm = [norm(values) * 0.125 for values in q]
    k_norm = [norm(values) for values in k]
    a = [jnp.broadcast_to(fade[:, row : row + 1], (8, 128)) for row in ROWS]
    b = [jnp.broadcast_to(beta[:, row : row + 1], (8, 128)) for row in ROWS]

    tall = jnp.concatenate(q + k, axis=0)
    first = tall.astype(bf16).astype(f32)
    second = (tall - first).astype(bf16).astype(f32)
    left = iota(tall.shape, 1) < 64
    one = jnp.where(left, first, second).astype(bf16)
    two = jnp.where(left, tall - first - second, 0.0).astype(bf16)
    bit, column = iota((256, 256), 0), iota((256, 256), 1)
    wide = (bit % 64 == column // 64).astype(f32).astype(bf16)
    for n in range(16):
        if n > 0:
            turned = [pltpu.roll(half, 128 - 4 * n, 1) for half in (one, two)]
        else:
            turned = [one, two]
        spread_ref[:, 256 * n : 256 * n + 256] = dot(jnp.concatenate(turned, axis=1), wide, 1, 0)

    starts = [accepted_ref[0] - 1, accepted_ref[1] - 1]
    ks, qs = [None] * 8, [None] * 8
    for i in range(32):
        at = slice(128 * i, 128 * i + 128)
        for j in range(2):
            start = prior_ref[j, starts[j], :, at]
            for row in range(4 * j, 4 * j + 4):
                kx = spread_ref[64 + 8 * row : 72 + 8 * row, at]
                qx = spread_ref[8 * row : 8 * row + 8, at]
                ks[row] = kx * start if i == 0 else ks[row] + kx * start
                qs[row] = qx * start if i == 0 else qs[row] + qx * start

    def fold(values):
        return values + pltpu.roll(values, 64, 1)

    ks = [k_norm[row] * fold(ks[row]) for row in ROWS]
    qs = [q_norm[row] * fold(qs[row]) for row in ROWS]
    kw, o = [None] * 8, [None] * 8
    for j in range(2):
        base = 4 * j
        grown = None
        for t in range(4):
            row = base + t
            carried = ks[row] if t == 0 else grown * ks[row]
            for e in range(t):
                reach = half_sum(k[row] * k[base + e]) * k_norm[row]
                for m in range(e + 1, t):
                    reach = reach * a[base + m]
                carried = carried + reach * kw[base + e]
            kw[row] = k_norm[row] * (b[row] * (v[row] - a[row] * carried))
            grown = a[row] if t == 0 else grown * a[row]
            out = grown * qs[row]
            for e in range(t + 1):
                reach = half_sum(q[row] * k[base + e]) * q_norm[row]
                for m in range(e + 1, t + 1):
                    reach = reach * a[base + m]
                out = out + reach * kw[base + e]
            o[row] = out

    for j in range(2):
        for i in range(32):
            at = slice(128 * i, 128 * i + 128)
            state = prior_ref[j, starts[j], :, at]
            for t in range(4):
                row = 4 * j + t
                state = a[row] * state + spread_ref[64 + 8 * row : 72 + 8 * row, at] * kw[row]
                states_ref[j, t, :, at] = state

    for row in ROWS:
        mean = half_sum(o[row] * o[row]) / 64
        n = o[row] * lax.rsqrt(mean + epsilon) * gain
        for p in range(4):
            nrows[row : row + 1, 128 * p : 128 * p + 128] = jnp.sum(
                jnp.where(masks[p], n, 0.0), axis=0, keepdims=True
            )
    rows = nrows[...]
    rows_ref[...] = jnp.concatenate([rows] * 8, axis=0).astype(bf16)


def mix_kernel(x_ref, rows_ref, out_ref):
    w = x_ref[...].reshape(256, 512)
    rows = rows_ref[...]
    out = dot(w, jnp.concatenate([rows, rows], axis=0), 1, 1)
    low = iota((16, 128), 1) < 64
    for r in range(8):
        piece = jnp.where(low, out[32 * r : 32 * r + 16], out[32 * r + 16 : 32 * r + 32])
        out_ref[r] = piece.astype(bf16)
        out_ref[8 + r] = piece.astype(bf16)


def place_kernel(x_ref, back_ref, states_ref, out_ref, kept_ref, sem):
    copies = [
        pltpu.make_async_copy(states_ref.at[n], kept_ref.at[n], sem.at[n]) for n in range(2)
    ]
    for copy in copies:
        copy.start()
    low = iota((16, 128), 1) < 64
    sums = [x_ref[r].astype(f32) + x_ref[8 + r].astype(f32) for r in range(8)]
    tiles = []
    for p in range(4):
        a, b = sums[2 * p], sums[2 * p + 1]
        top = jnp.where(low, a, pltpu.roll(b, 64, 1))
        end = jnp.where(low, pltpu.roll(a, 64, 1), b)
        tiles.append(jnp.concatenate([top, end], axis=0).astype(bf16))
    whole = dot(jnp.concatenate(tiles, axis=1), back_ref[...], 1, 0).astype(bf16)
    for t in range(4):
        out_ref[t] = whole[:, 128 * t : 128 * t + 128]
    for copy in copies:
        copy.wait()


def back_table():
    dest = np.arange(512)
    group, rho = dest // 64, dest % 64
    group = (group % 2) * 4 + group // 2
    wanted = (rho % 4) * 128 + (rho // 8) * 16 + group * 2 + (rho % 8) // 4
    return (wanted[:, None] == np.arange(512)[None, :]).astype(jnp.bfloat16)


def call(kernel, shapes, args, specs=None, scratch=(), outs=VMEM, name=None):
    if name == "pack":
        args = [pltpu.with_memory_space_constraint(a, pltpu.HBM) for a in args]
    return pl.pallas_call(
        kernel,
        out_shape=shapes,
        in_specs=specs or [VMEM] * len(args),
        out_specs=outs,
        scratch_shapes=scratch,
        compiler_params=pltpu.CompilerParams(vmem_limit_bytes=16 << 20),
        name=name,
    )(*args)


def shape(dims, dtype):
    return jax.ShapeDtypeStruct(dims, dtype)


def per_device(
    tokens,
    input_norm_gain,
    query_projection,
    key_projection,
    value_projection,
    write_strength_weight,
    decay_projection,
    head_decay_rate,
    token_extra_decay,
    accepted,
    prior_step_states,
    output_norm_gain,
    output_projection,
):
    def swap(x, axes):
        return lax.all_to_all(x, axes, 0, 0, tiled=True)

    part_shape, wo_shape = shape((64, WO), bf16), shape((8, 32, 512), bf16)

    def pack(late, args):
        sizes = (shape((8, 32, WO), bf16), wo_shape) if late else shape((8, 32, WIDE), bf16)
        return call(
            functools.partial(pack_kernel, late=late),
            sizes,
            args,
            specs=[HBM] * 8,
            scratch=[
                pltpu.VMEM((4, 32, 128), bf16),
                pltpu.VMEM((1, 32), f32),
                pltpu.VMEM((32, 512), bf16),
                pltpu.VMEM((32, 512), bf16),
                pltpu.VMEM((32, 512), bf16),
                pltpu.VMEM((8, 32), bf16),
                pltpu.VMEM((8, 32), bf16),
                pltpu.VMEM((32, 512), bf16),
                pltpu.SemaphoreType.DMA((8,)),
            ],
            outs=(VMEM, VMEM) if late else VMEM,
            name="pack",
        )

    def start_late(*args):
        packed, own = pack(True, args)
        return call(project_kernel, part_shape, (swap(packed, NEAR),), name="project"), own

    def start_early(*args):
        near = swap(pack(False, args), NEAR)
        return call(
            project_kernel, (part_shape, wo_shape), (near,), outs=(VMEM, VMEM), name="project"
        )

    def mix(weights, rows):
        return call(mix_kernel, shape((16, 16, 128), bf16), (weights, rows), name="mix")

    pair = lax.axis_index("z8")
    late = (pair >= 4) & (pair <= 6)
    part, weights = lax.cond(
        late,
        start_late,
        start_early,
        jnp.transpose(tokens, (1, 2, 0)),
        input_norm_gain[None, :],
        query_projection,
        key_projection,
        value_projection,
        write_strength_weight.T,
        decay_projection.T,
        output_projection.T,
    )
    arrived = swap(part.reshape(8, 8, part.shape[1]), "z8").reshape(part.shape)
    states, rows = call(
        delta_kernel,
        (shape(prior_step_states.shape, f32), shape((64, 512), bf16)),
        (
            accepted,
            arrived,
            prior_step_states,
            head_decay_rate[None, :],
            token_extra_decay,
            output_norm_gain[None, :],
        ),
        specs=[SMEM] + [VMEM] * 5,
        scratch=[
            pltpu.VMEM((8, 128), f32),
            pltpu.VMEM((8, 512), f32),
            pltpu.VMEM((128, 4096), f32),
        ],
        outs=(VMEM, VMEM),
        name="delta",
    )
    all_rows = swap(rows.reshape(8, 8, 512), "z8").reshape(64, 512)
    columns = lax.cond(
        late, lambda w, r: mix(swap(w, NEAR), r), lambda w, r: mix(w, r), weights, all_rows
    )
    back = swap(columns, ("tp", "y", "zp"))
    mixed, kept = call(
        place_kernel,
        (shape((4, 32, 128), bf16), shape(states.shape, f32)),
        (back, jnp.asarray(back_table()), states),
        scratch=[pltpu.SemaphoreType.DMA((2,))],
        outs=(VMEM, HBM),
        name="place",
    )
    return (jnp.transpose(mixed, (2, 0, 1)), kept)


def solution(mesh):
    split = Mesh(
        mesh.devices.reshape(mesh.shape["dp"], 8, 2, 4, mesh.shape["tp"]),
        ("dp", "z8", "zp", "y", "tp"),
    )
    in_specs = (
        P("dp", None, KV),
        P(KV),
        P(KV, "tp"),
        P(KV, "tp"),
        P(KV, "tp"),
        P(KV, "tp"),
        P(KV, "tp"),
        P("tp"),
        P(DP_KV, None, "tp"),
        P(DP_KV),
        P(DP_KV, None, "tp", None),
        P(),
        P("tp", KV),
    )
    out_specs = (P("dp", None, KV), P(DP_KV, None, "tp", None))
    return jax.shard_map(
        per_device, mesh=split, in_specs=in_specs, out_specs=out_specs, check_vma=False
    )
```

```python
import functools

import jax
import jax.numpy as jnp
import numpy as np
from jax import lax
from jax.experimental import pallas as pl
from jax.experimental.pallas import tpu as pltpu
from jax.sharding import Mesh
from jax.sharding import PartitionSpec as P

D = 2048
epsilon = 1e-06
KV = ("z8", "zp", "y")
DP_KV = ("dp", "z8", "zp", "y")
NEAR = ("y", "zp")
f32 = jnp.float32
bf16 = jnp.bfloat16

QKV, SMALL, WO, WIDE = 0, 1536, 1664, 2176
VMEM = pl.BlockSpec(memory_space=pltpu.VMEM)
SMEM = pl.BlockSpec(memory_space=pltpu.SMEM)
HBM = pl.BlockSpec(memory_space=pltpu.HBM)


def iota(shape, dim):
    return lax.broadcasted_iota(jnp.int32, shape, dim)


def dot(a, b, ca, cb):
    return lax.dot_general(a, b, (((ca,), (cb,)), ((), ())), preferred_element_type=f32)


def pack_kernel(*refs, late):
    hbm, out_ref, held, sems = refs[:8], refs[8], refs[-9:-1], refs[-1]
    copies = [pltpu.make_async_copy(hbm[n], held[n], sems.at[n]) for n in range(8)]
    for copy in copies:
        copy.start()
    tok_ref, gain_ref, q_ref, k_ref, v_ref, beta_ref, decay_ref, wo_ref = held
    source, dest = iota((512, 512), 0), iota((1, 512), 1)
    group, rho = dest // 64, dest % 64
    group = (group % 2) * 4 + group // 2
    wanted = (rho % 4) * 128 + (rho // 8) * 16 + group * 2 + (rho % 8) // 4
    pick = (source == wanted).astype(f32).astype(bf16)
    eye = iota((32, 32), 0) == iota((32, 32), 1)
    head, lane = iota((8, 128), 0), iota((8, 128), 1)
    put_beta = ((lane == head) | (lane == head + 16)).astype(f32).astype(bf16)
    put_decay = ((lane == head + 8) | (lane == head + 24)).astype(f32).astype(bf16)
    for copy in copies:
        copy.wait()
    gain = jnp.sum(jnp.where(eye, gain_ref[...], 0.0), axis=1, keepdims=True)
    raw = dot(jnp.concatenate([tok_ref[t] for t in range(4)], axis=1), pick, 1, 0)
    scaled = raw * gain
    squares = jnp.sum(raw * raw, axis=0, keepdims=True)
    high = squares.astype(bf16).astype(f32)
    sub = iota((8, 512), 0)
    extra = jnp.where(sub < 2, high, jnp.where(sub < 4, squares - high, 0.0))
    small = dot(beta_ref[...], put_beta, 0, 0) + dot(decay_ref[...], put_decay, 0, 0)
    lane = iota((8, 128), 1)
    even = iota((8, 128), 0) % 2 == 0
    for r in range(8):
        at = slice(128 * (r // 2), 128 * (r // 2) + 128)
        sums = extra[:, at]
        if r % 2 == 0:
            cols = pltpu.roll(scaled[:, at], 64, 1)
            sums = jnp.where(even, pltpu.roll(sums, 32, 1), sums)
        else:
            cols = scaled[:, at]
            sums = jnp.where(even, pltpu.roll(sums, 96, 1), pltpu.roll(sums, 64, 1))
        groups = []
        for g in range(4):
            right = jnp.where(lane < 64, sums if g == 0 else 0.0, cols[8 * g : 8 * g + 8])
            groups.append(jnp.where(lane < 32, small[8 * g : 8 * g + 8], right))
        tile = jnp.concatenate(groups, axis=0)
        if late:
            refs[9][r] = wo_ref[...]
        else:
            out_ref[r, :, WO:] = wo_ref[...]
        out_ref[r, :, QKV : QKV + 512] = q_ref[...]
        out_ref[r, :, QKV + 512 : QKV + 1024] = k_ref[...]
        out_ref[r, :, QKV + 1024 : SMALL] = v_ref[...]
        out_ref[r, :, SMALL:WO] = tile.astype(bf16)


def project_kernel(x_ref, out_ref, *wo_refs):
    for wo_ref in wo_refs:
        wo_ref[...] = x_ref[:, :, WO:]
    x = x_ref[:, :, :WO].reshape(256, WO)
    cols = x[:, SMALL:]
    main = dot(cols, x[:, QKV:SMALL], 0, 0)
    out_ref[:, : SMALL - QKV] = main[64:].astype(bf16)
    sums = jnp.zeros((8, 128), f32)
    for r in range(8):
        sums = sums + cols[32 * r : 32 * r + 16].astype(f32)[0:8]
    sub, lane = iota((32, 128), 0), iota((32, 128), 1)
    halves = []
    for n in range(2):
        row = sums[n : n + 1] + sums[n + 2 : n + 3]
        halves.append(jnp.sum(jnp.where(lane == sub + 32, row, 0.0), axis=1, keepdims=True))
    total = jnp.concatenate(halves, axis=0)
    lane = iota((64, 128), 1)
    tail = jnp.where(lane < 32, dot(cols, cols, 0, 0)[64:], jnp.where(lane < 34, total, 0.0))
    first = tail.astype(bf16).astype(f32)
    keep = (lane < 16) | (lane == 32)
    out_ref[:, SMALL - QKV :] = jnp.where(keep, first, tail - first).astype(bf16)


def delta_kernel(
    accepted_ref, c_ref, prior_ref, rate_ref, extra_ref, gain_ref, states_ref, rows_ref,
    aux, nrows, spread_ref
):
    c = c_ref[...].astype(f32)
    s = (c[0:8] + c[8:16]) + (c[16:24] + c[24:32])
    s = s + ((c[32:40] + c[40:48]) + (c[48:56] + c[56:64]))
    tile = s[:, 1536:]
    total = tile[:, 32:33] + tile[:, 33:34]
    inverse = lax.rsqrt(total / D + epsilon)
    logits = jnp.transpose((tile + pltpu.roll(tile, 112, 1)) * inverse)
    aux[...] = jnp.zeros((8, 128), f32)
    aux[0:4, 0:8] = extra_ref[0]
    aux[4:8, 0:8] = extra_ref[1]
    aux[:, 8:16] = jnp.broadcast_to(rate_ref[...], (8, 8))
    side = jnp.transpose(aux[...])
    beta = jax.nn.sigmoid(logits[0:8])
    fade = jnp.exp(-side[8:16] * jax.nn.softplus(logits[8:16]) + side[0:8])

    sub, lane = iota((8, 128), 0), iota((8, 128), 1)
    masks = [sub == 2 * p + lane // 64 for p in range(4)]
    gain = jnp.concatenate([gain_ref[...], gain_ref[...]], axis=1)

    def silu_of(at):
        u = s[:, at : at + 512] * inverse
        return u / (1.0 + jnp.exp(-u))

    parts = [silu_of(0), silu_of(512), silu_of(1024)]

    def by_heads(values, row):
        m = jnp.zeros((8, 128), f32)
        for p in range(4):
            piece = jnp.broadcast_to(values[row : row + 1, 128 * p : 128 * p + 128], (8, 128))
            m = jnp.where(masks[p], piece, m)
        return m + pltpu.roll(m, 64, 1)

    def half_sum(values):
        return 0.5 * jnp.sum(values, axis=1, keepdims=True)

    def norm(values):
        return lax.rsqrt(half_sum(values * values) + epsilon)

    ROWS = range(8)
    q = [by_heads(parts[0], row) for row in ROWS]
    k = [by_heads(parts[1], row) for row in ROWS]
    v = [by_heads(parts[2], row) for row in ROWS]
    q_norm = [norm(values) * 0.125 for values in q]
    k_norm = [norm(values) for values in k]
    a = [jnp.broadcast_to(fade[:, row : row + 1], (8, 128)) for row in ROWS]
    b = [jnp.broadcast_to(beta[:, row : row + 1], (8, 128)) for row in ROWS]

    tall = jnp.concatenate(q + k, axis=0)
    first = tall.astype(bf16).astype(f32)
    second = (tall - first).astype(bf16).astype(f32)
    left = iota(tall.shape, 1) < 64
    one = jnp.where(left, first, second).astype(bf16)
    two = jnp.where(left, tall - first - second, 0.0).astype(bf16)
    bit, column = iota((256, 256), 0), iota((256, 256), 1)
    wide = (bit % 64 == column // 64).astype(f32).astype(bf16)
    for n in range(16):
        if n > 0:
            turned = [pltpu.roll(half, 128 - 4 * n, 1) for half in (one, two)]
        else:
            turned = [one, two]
        spread_ref[:, 256 * n : 256 * n + 256] = dot(jnp.concatenate(turned, axis=1), wide, 1, 0)

    starts = [accepted_ref[0] - 1, accepted_ref[1] - 1]
    ks, qs = [None] * 8, [None] * 8
    for i in range(32):
        at = slice(128 * i, 128 * i + 128)
        for j in range(2):
            start = prior_ref[j, starts[j], :, at]
            for row in range(4 * j, 4 * j + 4):
                kx = spread_ref[64 + 8 * row : 72 + 8 * row, at]
                qx = spread_ref[8 * row : 8 * row + 8, at]
                ks[row] = kx * start if i == 0 else ks[row] + kx * start
                qs[row] = qx * start if i == 0 else qs[row] + qx * start

    def fold(values):
        return values + pltpu.roll(values, 64, 1)

    ks = [k_norm[row] * fold(ks[row]) for row in ROWS]
    qs = [q_norm[row] * fold(qs[row]) for row in ROWS]
    kw, o = [None] * 8, [None] * 8
    for j in range(2):
        base = 4 * j
        grown = None
        for t in range(4):
            row = base + t
            carried = ks[row] if t == 0 else grown * ks[row]
            for e in range(t):
                reach = half_sum(k[row] * k[base + e]) * k_norm[row]
                for m in range(e + 1, t):
                    reach = reach * a[base + m]
                carried = carried + reach * kw[base + e]
            kw[row] = k_norm[row] * (b[row] * (v[row] - a[row] * carried))
            grown = a[row] if t == 0 else grown * a[row]
            out = grown * qs[row]
            for e in range(t + 1):
                reach = half_sum(q[row] * k[base + e]) * q_norm[row]
                for m in range(e + 1, t + 1):
                    reach = reach * a[base + m]
                out = out + reach * kw[base + e]
            o[row] = out

    for j in range(2):
        for i in range(32):
            at = slice(128 * i, 128 * i + 128)
            state = prior_ref[j, starts[j], :, at]
            for t in range(4):
                row = 4 * j + t
                state = a[row] * state + spread_ref[64 + 8 * row : 72 + 8 * row, at] * kw[row]
                states_ref[j, t, :, at] = state

    for row in ROWS:
        mean = half_sum(o[row] * o[row]) / 64
        n = o[row] * lax.rsqrt(mean + epsilon) * gain
        for p in range(4):
            nrows[row : row + 1, 128 * p : 128 * p + 128] = jnp.sum(
                jnp.where(masks[p], n, 0.0), axis=0, keepdims=True
            )
    rows = nrows[...]
    rows_ref[...] = jnp.concatenate([rows] * 8, axis=0).astype(bf16)


def mix_kernel(x_ref, rows_ref, out_ref):
    w = x_ref[...].reshape(256, 512)
    rows = rows_ref[...]
    out = dot(w, jnp.concatenate([rows, rows], axis=0), 1, 1)
    low = iota((16, 128), 1) < 64
    for r in range(8):
        piece = jnp.where(low, out[32 * r : 32 * r + 16], out[32 * r + 16 : 32 * r + 32])
        out_ref[r] = piece.astype(bf16)
        out_ref[8 + r] = piece.astype(bf16)


def place_kernel(x_ref, back_ref, states_ref, out_ref, kept_ref, sem):
    copies = [
        pltpu.make_async_copy(states_ref, kept_ref, sem.at[n]) for n in range(1)
    ]
    for copy in copies:
        copy.start()
    low = iota((16, 128), 1) < 64
    sums = [x_ref[r].astype(f32) + x_ref[8 + r].astype(f32) for r in range(8)]
    tiles = []
    for p in range(4):
        a, b = sums[2 * p], sums[2 * p + 1]
        top = jnp.where(low, a, pltpu.roll(b, 64, 1))
        end = jnp.where(low, pltpu.roll(a, 64, 1), b)
        tiles.append(jnp.concatenate([top, end], axis=0).astype(bf16))
    whole = dot(jnp.concatenate(tiles, axis=1), back_ref[...], 1, 0).astype(bf16)
    for t in range(4):
        out_ref[t] = whole[:, 128 * t : 128 * t + 128]
    for copy in copies:
        copy.wait()


def back_table():
    dest = np.arange(512)
    group, rho = dest // 64, dest % 64
    group = (group % 2) * 4 + group // 2
    wanted = (rho % 4) * 128 + (rho // 8) * 16 + group * 2 + (rho % 8) // 4
    return (wanted[:, None] == np.arange(512)[None, :]).astype(jnp.bfloat16)


def call(kernel, shapes, args, specs=None, scratch=(), outs=VMEM, name=None):
    if name == "pack":
        args = [pltpu.with_memory_space_constraint(a, pltpu.HBM) for a in args]
    return pl.pallas_call(
        kernel,
        out_shape=shapes,
        in_specs=specs or [VMEM] * len(args),
        out_specs=outs,
        scratch_shapes=scratch,
        compiler_params=pltpu.CompilerParams(vmem_limit_bytes=16 << 20),
        name=name,
    )(*args)


def shape(dims, dtype):
    return jax.ShapeDtypeStruct(dims, dtype)


def per_device(
    tokens,
    input_norm_gain,
    query_projection,
    key_projection,
    value_projection,
    write_strength_weight,
    decay_projection,
    head_decay_rate,
    token_extra_decay,
    accepted,
    prior_step_states,
    output_norm_gain,
    output_projection,
):
    def swap(x, axes):
        return lax.all_to_all(x, axes, 0, 0, tiled=True)

    part_shape, wo_shape = shape((64, WO), bf16), shape((8, 32, 512), bf16)

    def pack(late, args):
        sizes = (shape((8, 32, WO), bf16), wo_shape) if late else shape((8, 32, WIDE), bf16)
        return call(
            functools.partial(pack_kernel, late=late),
            sizes,
            args,
            specs=[HBM] * 8,
            scratch=[
                pltpu.VMEM((4, 32, 128), bf16),
                pltpu.VMEM((1, 32), f32),
                pltpu.VMEM((32, 512), bf16),
                pltpu.VMEM((32, 512), bf16),
                pltpu.VMEM((32, 512), bf16),
                pltpu.VMEM((8, 32), bf16),
                pltpu.VMEM((8, 32), bf16),
                pltpu.VMEM((32, 512), bf16),
                pltpu.SemaphoreType.DMA((8,)),
            ],
            outs=(VMEM, VMEM) if late else VMEM,
            name="pack",
        )

    def start_late(*args):
        packed, own = pack(True, args)
        return call(project_kernel, part_shape, (swap(packed, NEAR),), name="project"), own

    def start_early(*args):
        near = swap(pack(False, args), NEAR)
        return call(
            project_kernel, (part_shape, wo_shape), (near,), outs=(VMEM, VMEM), name="project"
        )

    def mix(weights, rows):
        return call(mix_kernel, shape((16, 16, 128), bf16), (weights, rows), name="mix")

    pair = lax.axis_index("z8")
    late = (pair >= 4) & (pair <= 6)
    part, weights = lax.cond(
        late,
        start_late,
        start_early,
        jnp.transpose(tokens, (1, 2, 0)),
        input_norm_gain[None, :],
        query_projection,
        key_projection,
        value_projection,
        write_strength_weight.T,
        decay_projection.T,
        output_projection.T,
    )
    arrived = swap(part.reshape(8, 8, part.shape[1]), "z8").reshape(part.shape)
    states, rows = call(
        delta_kernel,
        (shape(prior_step_states.shape, f32), shape((64, 512), bf16)),
        (
            accepted,
            arrived,
            prior_step_states,
            head_decay_rate[None, :],
            token_extra_decay,
            output_norm_gain[None, :],
        ),
        specs=[SMEM] + [VMEM] * 5,
        scratch=[
            pltpu.VMEM((8, 128), f32),
            pltpu.VMEM((8, 512), f32),
            pltpu.VMEM((128, 4096), f32),
        ],
        outs=(VMEM, VMEM),
        name="delta",
    )
    all_rows = swap(rows.reshape(8, 8, 512), "z8").reshape(64, 512)
    columns = lax.cond(
        late, lambda w, r: mix(swap(w, NEAR), r), lambda w, r: mix(w, r), weights, all_rows
    )
    back = swap(columns, ("tp", "y", "zp"))
    mixed, kept = call(
        place_kernel,
        (shape((4, 32, 128), bf16), shape(states.shape, f32)),
        (back, jnp.asarray(back_table()), states),
        scratch=[pltpu.SemaphoreType.DMA((1,))],
        outs=(VMEM, HBM),
        name="place",
    )
    return (jnp.transpose(mixed, (2, 0, 1)), kept)


def solution(mesh):
    split = Mesh(
        mesh.devices.reshape(mesh.shape["dp"], 8, 2, 4, mesh.shape["tp"]),
        ("dp", "z8", "zp", "y", "tp"),
    )
    in_specs = (
        P("dp", None, KV),
        P(KV),
        P(KV, "tp"),
        P(KV, "tp"),
        P(KV, "tp"),
        P(KV, "tp"),
        P(KV, "tp"),
        P("tp"),
        P(DP_KV, None, "tp"),
        P(DP_KV),
        P(DP_KV, None, "tp", None),
        P(),
        P("tp", KV),
    )
    out_specs = (P("dp", None, KV), P(DP_KV, None, "tp", None))
    return jax.shard_map(
        per_device, mesh=split, in_specs=in_specs, out_specs=out_specs, check_vma=False
    )
```
